512 devices in a mesh: kv: 32 (over z, core), tp: 16 (over y, x).
Axes of the slice: x: 4, y: 4, z: 16, core: 2. Of those that a mesh axis runs over, the one named last changes fastest.
Arguments:
- tokens: bfloat16 [256, 4096], P('tp', 'kv'), may hold values from -64 to 64
- first_norm_gain: float32 [4096], P('kv'), may hold values from 0.1 to 1.9
- first_gate_weight: bfloat16 [4096, 10240], P('kv', 'tp'), may hold values from -0.09375 to 0.09375
- first_up_weight: bfloat16 [4096, 10240], P('kv', 'tp'), may hold values from -0.09375 to 0.09375
- first_down_weight: bfloat16 [10240, 4096], P('tp', 'kv'), may hold values from -0.0625 to 0.0625
- mixer_norm_gain: float32 [4096], P('kv'), may hold values from 0.1 to 1.9
- query_weight_matrix: bfloat16 [4096, 2048], P('kv', 'tp'), may hold values from -0.09375 to 0.09375
- key_weight_matrix: bfloat16 [4096, 2048], P('kv', 'tp'), may hold values from -0.09375 to 0.09375
- value_weight_matrix: bfloat16 [4096, 2048], P('kv', 'tp'), may hold values from -0.09375 to 0.09375
- output_gate_weight: bfloat16 [4096, 2048], P('kv', 'tp'), may hold values from -0.09375 to 0.09375
- strength_weight: bfloat16 [4096, 16], replicated, may hold values from -0.375 to 0.375
- decay_weight: bfloat16 [4096, 16], replicated, may hold values from -0.75 to 0.75
- head_decay_speed: float32 [16], P('tp'), may hold values from 0.003 to 0.15
- head_decay_offset: float32 [16], P('tp'), may hold values from -4 to 4
- head_norm_gain: float32 [128], replicated, may hold values from 0.1 to 1.9
- mixer_out_weight: bfloat16 [2048, 4096], P('tp', 'kv'), may hold values from -0.125 to 0.125
- second_norm_gain: float32 [4096], P('kv'), may hold values from 0.1 to 1.9
- second_gate_weight: bfloat16 [4096, 10240], P('kv', 'tp'), may hold values from -0.09375 to 0.09375
- second_up_weight: bfloat16 [4096, 10240], P('kv', 'tp'), may hold values from -0.09375 to 0.09375
- second_down_weight: bfloat16 [10240, 4096], P('tp', 'kv'), may hold values from -0.0625 to 0.0625
- recurrent: float32 [256, 16, 128, 128], P('kv', 'tp'), may hold values from -1.25 to 1.25
- earlier_key_cache: bfloat16 [256, 64, 2048], P('kv', None, 'tp'), may hold values from -6 to 6
- earlier_value_cache: bfloat16 [256, 64, 2048], P('kv', None, 'tp'), may hold values from -6 to 6
- strength_logit_history: float32 [16, 256, 64], P('tp', 'kv'), may hold values from -6 to 6
- decay_input_history: float32 [16, 256, 64], P('tp', 'kv'), may hold values from -8 to 8
- position_decay_extra: float32 [16, 256, 64], P('tp', 'kv'), may hold values from -1 to 0
- lengths: int32 [256], P('kv'), may hold values from 1 to 64, 4096 in all
Outputs:
- layer_output: bfloat16 [256, 4096], P('tp', 'kv')
The draws below stay inside these ranges and needn't reach their ends.
Inputs may be any that keep to these rules, and one draw needn't show every extreme that they name: `lengths`: positions at or beyond a sequence's length in its caches take no part; the new token sits at position length - 1.
All inputs are finite; a program needn't handle non-finite values. No bound on the sum of `lengths` on one device may be relied on, other than what follows from the above.
Results may differ from the reference program's by a relative error of at most 0.008.
Values may be sent and summed in bfloat16 or wider, within the bound.
No kernel may reach another device: no remote copies, remote signals or barrier semaphores. Data moves between devices by JAX's collectives and lax.ppermute only.
A program may use at most 64 MiB of HBM per device.

```python
import math
import jax
import jax.numpy as jnp
import numpy as np
from jax import lax

D = 4096
FF = 10240
HEADS = 16
DK = 128
DV = 128
BLOCK = 64
BATCH = 256


def draw_tokens(key, part):
    base_key, row_key = jax.random.split(jax.random.fold_in(key, 11), 2)
    column = 10.0 ** (jnp.arange(D, dtype=jnp.float32) / D - 0.5)
    half_range = 0.5 * math.log(10.0)
    row_scale = jnp.exp(jax.random.uniform(row_key, (BATCH, 1), jnp.float32, -half_range, half_range))
    base = jnp.clip(jax.random.normal(base_key, (BATCH, D), jnp.float32), -6.0, 6.0)
    return (base * column[None, :] * row_scale).astype(jnp.bfloat16)


def draw_decay_input_history(key, part):
    noise_key = jax.random.fold_in(key, 23)
    offset = 2.0 * jnp.arange(BATCH, dtype=jnp.float32) / BATCH - 1.0
    base = jnp.clip(jax.random.normal(noise_key, (HEADS, BATCH, BLOCK), jnp.float32), -5.0, 5.0)
    return base + offset[None, :, None]


def draw_position_decay_extra(key, part):
    spot_key, size_key = jax.random.split(jax.random.fold_in(key, 37), 2)
    spots = jax.random.randint(spot_key, (HEADS, BATCH, 2), 0, BLOCK)
    position = jnp.arange(BLOCK, dtype=jnp.int32)
    struck = jnp.any(position[None, None, None, :] == spots[..., None], axis=2)
    size = jax.random.uniform(size_key, (HEADS, BATCH, BLOCK), jnp.float32, math.log(0.5), math.log(0.8))
    return jnp.where(struck, size, 0.0)


def level_of(key, shape, cuts, smallest, high):
    def one(dim, blocks):
        heights = jax.random.uniform(jax.random.fold_in(jax.random.fold_in(key, 6), dim), (blocks,), jnp.float32, smallest / len(cuts), high / len(cuts))
        return jnp.repeat(jnp.exp(heights), shape[dim] // blocks).reshape((-1,) + (1,) * (len(shape) - dim - 1))

    level = one(*cuts[0])
    for cut in cuts[1:]:
        level = level * one(*cut)
    return level


def split_up(count, total, bound, slope):
    loads = [(1 << 20) // math.isqrt(rank ** slope) + 1 for rank in range(2, count + 1)]
    surplus, given = total - bound - (count - 1), [1] * (count - 1)
    while surplus > 0:
        candidates = [i for i in range(count - 1) if given[i] < bound]
        mass, left = sum([loads[i] for i in candidates]), surplus
        for i in candidates:
            extra = min(bound - given[i], max(1, left * loads[i] // mass), surplus)
            given[i] = given[i] + extra
            surplus = surplus - extra
    return np.array([bound] + given)


def ragged_sizes(key, number_of, total, limit, lean):
    if number_of == 2:
        one = jax.random.randint(key, (), max(1, total - limit), min(limit, total - 1) + 1)
        return jnp.stack([one, total - one])
    tallies = jnp.asarray(split_up(number_of, total, limit, lean), jnp.int32)
    pairs = (number_of - 1) // 2
    donor, taker = tallies[1:1 + 2 * pairs:2], tallies[2:2 + 2 * pairs:2]
    margin = jnp.minimum(donor - 1, limit - taker)
    shifted = jax.random.randint(jax.random.fold_in(key, 1), (pairs,), 0, 1 << 20) % (margin + 1)
    tallies = tallies.at[1:1 + 2 * pairs:2].set(donor - shifted).at[2:2 + 2 * pairs:2].set(taker + shifted)
    return tallies[jax.random.permutation(jax.random.fold_in(key, 2), number_of)]


def normal_values(key, shape, deviation, bound, cuts=(), held_as=jnp.bfloat16):
    drawn = deviation * jax.random.normal(key, shape, jnp.float32)
    if cuts:
        drawn = drawn * level_of(key, shape, cuts, -0.22, 0.18)
    return jnp.clip(drawn, -bound, bound).astype(held_as)


def setup_inputs(seed: int = 0) -> dict:
    splits = jax.random.split(jax.random.key(seed), 28)
    tokens = draw_tokens(jax.random.fold_in(splits[27], 71), 0)
    first_norm_gain = jnp.clip(1.0 + 0.18 * jax.random.normal(splits[1], (D,), jnp.float32), 0.1, 1.9)
    first_gate_weight = normal_values(splits[2], (D, FF), D ** -0.5, 0.09375, ((0, 32), (1, 16)))
    first_up_weight = normal_values(splits[3], (D, FF), D ** -0.5, 0.09375, ((0, 32), (1, 16)))
    first_down_weight = normal_values(splits[4], (FF, D), FF ** -0.5, 0.0625, ((0, 16), (1, 32)))
    mixer_norm_gain = jnp.clip(1.0 + 0.18 * jax.random.normal(splits[5], (D,), jnp.float32), 0.1, 1.9)
    query_weight_matrix = normal_values(splits[6], (D, HEADS * DK), D ** -0.5, 0.09375, ((0, 32), (1, 16)))
    key_weight_matrix = normal_values(splits[7], (D, HEADS * DK), D ** -0.5, 0.09375, ((0, 32), (1, 16)))
    value_weight_matrix = normal_values(splits[8], (D, HEADS * DV), D ** -0.5, 0.09375, ((0, 32), (1, 16)))
    output_gate_weight = normal_values(splits[9], (D, HEADS * DV), D ** -0.5, 0.09375, ((0, 32), (1, 16)))
    strength_weight = normal_values(splits[10], (D, HEADS), (D // 16) ** -0.5, 0.375)
    decay_weight = normal_values(splits[11], (D, HEADS), (D // 64) ** -0.5, 0.75)
    head_decay_speed = jnp.clip(jnp.exp(math.log(0.15) - 3.912023 * jax.random.uniform(splits[12], (HEADS,), jnp.float32) ** level_of(splits[12], (HEADS,), ((0, 16),), -0.2, 0.2)), 0.003, 0.15)
    head_decay_offset = jnp.clip(jax.random.uniform(splits[13], (HEADS,), jnp.float32, -4.0, 4.0) * level_of(splits[13], (HEADS,), ((0, 16),), -0.4, 0.0), -4.0, 4.0)
    head_norm_gain = jnp.clip(1.0 + 0.18 * jax.random.normal(splits[14], (DV,), jnp.float32), 0.1, 1.9)
    mixer_out_weight = normal_values(splits[15], (HEADS * DV, D), (HEADS * DV) ** -0.5, 0.125, ((0, 16), (1, 32)))
    second_norm_gain = jnp.clip(1.0 + 0.18 * jax.random.normal(splits[16], (D,), jnp.float32), 0.1, 1.9)
    second_gate_weight = normal_values(splits[17], (D, FF), D ** -0.5, 0.09375, ((0, 32), (1, 16)))
    second_up_weight = normal_values(splits[18], (D, FF), D ** -0.5, 0.09375, ((0, 32), (1, 16)))
    second_down_weight = normal_values(splits[19], (FF, D), FF ** -0.5, 0.0625, ((0, 16), (1, 32)))
    recurrent = normal_values(splits[20], (BATCH, HEADS, DK, DV), (DK ** -0.5), 1.25, ((0, 32), (1, 16)), jnp.float32)
    earlier_key_cache = normal_values(splits[21], (BATCH, BLOCK, HEADS * DK), 1.0, 6.0, ((0, 32), (2, 16)))
    earlier_value_cache = normal_values(splits[22], (BATCH, BLOCK, HEADS * DV), 1.0, 6.0, ((0, 32), (2, 16)))
    strength_logit_history = normal_values(splits[23], (HEADS, BATCH, BLOCK), 1.5, 6.0, ((0, 16), (1, 32)), jnp.float32)
    decay_input_history = draw_decay_input_history(jax.random.fold_in(splits[27], 71), 0)
    position_decay_extra = draw_position_decay_extra(jax.random.fold_in(splits[27], 71), 0)
    lengths = ragged_sizes(splits[26], BATCH, BATCH * BLOCK // 4, BLOCK, 2).astype(jnp.int32)
    return dict(tokens=tokens, first_norm_gain=first_norm_gain, first_gate_weight=first_gate_weight, first_up_weight=first_up_weight, first_down_weight=first_down_weight, mixer_norm_gain=mixer_norm_gain, query_weight_matrix=query_weight_matrix, key_weight_matrix=key_weight_matrix, value_weight_matrix=value_weight_matrix, output_gate_weight=output_gate_weight, strength_weight=strength_weight, decay_weight=decay_weight, head_decay_speed=head_decay_speed, head_decay_offset=head_decay_offset, head_norm_gain=head_norm_gain, mixer_out_weight=mixer_out_weight, second_norm_gain=second_norm_gain, second_gate_weight=second_gate_weight, second_up_weight=second_up_weight, second_down_weight=second_down_weight, recurrent=recurrent, earlier_key_cache=earlier_key_cache, earlier_value_cache=earlier_value_cache, strength_logit_history=strength_logit_history, decay_input_history=decay_input_history, position_decay_extra=position_decay_extra, lengths=lengths)


def delta_rule_block(current_query, current_key, current_value, output_gate_rows, strength_logit_current, decay_input_current, recurrent, earlier_key_cache, earlier_value_cache, strength_logit_history, decay_input_history, position_decay_extra, lengths, head_decay_speed, head_decay_offset, head_norm_gain):
    batch, heads, width = current_query.shape
    depth = current_value.shape[2]
    span = earlier_key_cache.shape[1]
    position = jnp.arange(span, dtype=jnp.int32)
    current = (lengths - 1).astype(jnp.int32)[:, None, None]
    is_new = position[None, None, :] == current
    live = position[None, None, :] <= current
    keys = earlier_key_cache.astype(jnp.float32).reshape(batch, span, heads, width).transpose(0, 2, 1, 3)
    keys = jnp.where(is_new[..., None], current_key[:, :, None, :], keys)
    keys = jnp.where(live[..., None], keys, 0.0)
    keys = keys * lax.rsqrt(lax.optimization_barrier(jnp.sum(keys * keys, -1, keepdims=True)) + 1e-06)
    values = earlier_value_cache.astype(jnp.float32).reshape(batch, span, heads, depth).transpose(0, 2, 1, 3)
    values = jnp.where(is_new[..., None], current_value[:, :, None, :], values)
    values = jnp.where(live[..., None], values, 0.0)
    beta = jax.nn.sigmoid(jnp.where(is_new, strength_logit_current[:, :, None], strength_logit_history.transpose(1, 0, 2)))
    beta = jnp.where(live, beta, 0.0)
    block_record = jnp.where(is_new, decay_input_current[:, :, None], decay_input_history.transpose(1, 0, 2))
    log_decay_amount = -head_decay_speed[None, :, None] * jax.nn.softplus(block_record + head_decay_offset[None, :, None]) + position_decay_extra.transpose(1, 0, 2)
    log_decay_amount = jnp.where(live, log_decay_amount, 0.0)
    cumul = jnp.cumsum(log_decay_amount, -1)
    earlier = position[:, None] > position[None, :]
    within = position[:, None] >= position[None, :]
    gaps = jnp.exp(jnp.where(within, cumul[..., :, None] - cumul[..., None, :], -jnp.inf))
    gram = jnp.einsum('bhpk,bhsk->bhps', keys, keys, precision=lax.Precision.HIGHEST)
    coupling = jnp.where(earlier, beta[..., :, None] * gram * gaps, 0.0)
    system = coupling + jnp.eye(span, dtype=jnp.float32)
    right_side = jnp.concatenate([values * beta[..., None], keys * (beta * jnp.exp(cumul))[..., None]], -1)
    solved = jax.scipy.linalg.solve_triangular(system, right_side, lower=True, unit_diagonal=True)
    updates = solved[..., :depth] - jnp.einsum('bhpk,bhkv->bhpv', solved[..., depth:], recurrent, precision=lax.Precision.HIGHEST)
    query = current_query * lax.rsqrt(lax.optimization_barrier(jnp.sum(current_query * current_query, -1, keepdims=True)) + 1e-06) * width ** (-0.5)
    latest = lax.optimization_barrier(jnp.sum(jnp.where(is_new, cumul, 0.0), -1))
    scores = jnp.einsum('bhk,bhsk->bhs', query, keys, precision=lax.Precision.HIGHEST)
    scores = scores * jnp.exp(jnp.where(live, latest[..., None] - cumul, -jnp.inf))
    carried = jnp.exp(latest)[..., None] * jnp.einsum('bhk,bhkv->bhv', query, recurrent, precision=lax.Precision.HIGHEST)
    head_out = carried + jnp.einsum('bhs,bhsv->bhv', scores, updates, precision=lax.Precision.HIGHEST)
    normed = head_out * lax.rsqrt(lax.optimization_barrier(jnp.mean(head_out * head_out, -1, keepdims=True)) + 1e-06)
    normed = normed * head_norm_gain[None, None, :] * jax.nn.silu(output_gate_rows)
    return normed.reshape(batch, heads * depth).astype(jnp.bfloat16)

def half_branch(wide, gain, gate_w, up_w, down_w):
    factor = lax.rsqrt(lax.optimization_barrier(jnp.mean(wide * wide, -1, keepdims=True)) + 1e-06)
    scaled = (wide * gain[None, :]).astype(jnp.bfloat16)
    gate_act = factor * jnp.dot(scaled.astype(jnp.float32), gate_w.astype(jnp.float32), preferred_element_type=jnp.float32)
    up_act = factor * jnp.dot(scaled.astype(jnp.float32), up_w.astype(jnp.float32), preferred_element_type=jnp.float32)
    hidden = (jax.nn.silu(gate_act) * up_act).astype(jnp.bfloat16)
    return jnp.dot(hidden.astype(jnp.float32), down_w.astype(jnp.float32), preferred_element_type=jnp.float32)

def rounded(values):
    return lax.optimization_barrier(values.astype(jnp.bfloat16)).astype(jnp.float32)

def reference(tokens, first_norm_gain, first_gate_weight, first_up_weight, first_down_weight, mixer_norm_gain, query_weight_matrix, key_weight_matrix, value_weight_matrix, output_gate_weight, strength_weight, decay_weight, head_decay_speed, head_decay_offset, head_norm_gain, mixer_out_weight, second_norm_gain, second_gate_weight, second_up_weight, second_down_weight, recurrent, earlier_key_cache, earlier_value_cache, strength_logit_history, decay_input_history, position_decay_extra, lengths):
    first_wide = tokens.astype(jnp.float32)
    middle = rounded(first_wide + 0.5 * half_branch(first_wide, first_norm_gain, first_gate_weight, first_up_weight, first_down_weight))
    factor = lax.rsqrt(lax.optimization_barrier(jnp.mean(middle * middle, -1, keepdims=True)) + 1e-06)
    mix_input = (middle * mixer_norm_gain[None, :]).astype(jnp.bfloat16)
    batch = tokens.shape[0]

    def project(weight, size):
        return (factor * jnp.dot(mix_input.astype(jnp.float32), weight.astype(jnp.float32), preferred_element_type=jnp.float32)).reshape(batch, HEADS, size)
    current_query = project(query_weight_matrix, DK)
    current_key = project(key_weight_matrix, DK)
    current_value = project(value_weight_matrix, DV)
    output_gate_rows = project(output_gate_weight, DV)
    strength_logit_current = factor * jnp.dot(mix_input.astype(jnp.float32), strength_weight.astype(jnp.float32), preferred_element_type=jnp.float32)
    decay_input_current = factor * jnp.dot(mix_input.astype(jnp.float32), decay_weight.astype(jnp.float32), preferred_element_type=jnp.float32)
    mixer_output_rows = delta_rule_block(current_query, current_key, current_value, output_gate_rows, strength_logit_current, decay_input_current, recurrent, earlier_key_cache, earlier_value_cache, strength_logit_history, decay_input_history, position_decay_extra, lengths, head_decay_speed, head_decay_offset, head_norm_gain)
    mixer_branch = jnp.dot(mixer_output_rows.astype(jnp.float32), mixer_out_weight.astype(jnp.float32), preferred_element_type=jnp.float32)
    second = rounded(middle + mixer_branch)
    last_branch = half_branch(second, second_norm_gain, second_gate_weight, second_up_weight, second_down_weight)
    return (second + 0.5 * last_branch).astype(jnp.bfloat16)
```

```python
import jax
import jax.numpy as jnp
from jax import lax
from jax.sharding import Mesh, PartitionSpec as P

D = 4096
HIGHEST = lax.Precision.HIGHEST
f32 = jnp.float32
bf16 = jnp.bfloat16


def swap(x):
    return lax.ppermute(x, "c", [(0, 1), (1, 0)])


def to_all(x, axis):
    count = lax.axis_size(axis)
    return lax.all_to_all(jnp.broadcast_to(x[None], (count, *x.shape)), axis, 0, 0, tiled=True)


def summed(x, axis):
    count = lax.axis_size(axis)
    parts = lax.all_to_all(x.reshape(count, -1, *x.shape[1:]), axis, 0, 0, tiled=True)
    return jnp.sum(parts.astype(f32), axis=0)


def dot(x, w):
    return jnp.dot(x, w, preferred_element_type=f32)


def hi_lo(x):
    hi = x.astype(bf16)
    lo = (x - hi.astype(f32)).astype(bf16)
    return [hi, lo]


def columns(parts, width):
    used = sum(p.shape[1] for p in parts)
    fill = jnp.zeros((parts[0].shape[0], width - used), bf16)
    return jnp.concatenate([*parts, fill], axis=1)


def branch(wide, gain, gates, ups, downs):
    half = wide.shape[1] // 2
    scaled = (wide * gain).astype(bf16)
    squares = jnp.sum(wide * wide, -1, keepdims=True)
    own, other = scaled[:, :half], scaled[:, half:]
    gate = dot(own, gates[0]) + dot(other, gates[1])
    up = dot(own, ups[0]) + dot(other, ups[1])
    n = gate.shape[1]
    sent = columns([gate.astype(bf16), up.astype(bf16), *hi_lo(squares)], 2 * n + 128)
    got = summed(sent, "z")
    square = got[:, 2 * n : 2 * n + 1] + got[:, 2 * n + 1 : 2 * n + 2]
    factor = lax.rsqrt(square / D + 1e-06)
    hidden = (jax.nn.silu(got[:, :n] * factor) * (got[:, n : 2 * n] * factor)).astype(bf16)
    hidden = to_all(hidden, "z").reshape(-1, n)
    return [dot(hidden, down) for down in downs]


def earlier_state(
    recurrent, key_cache, value_cache, strength, decay, extra, lengths, speed, offset
):
    span = key_cache.shape[1]
    position = jnp.arange(span, dtype=jnp.int32)
    before = position[None, :] < (lengths - 1)[:, None]
    keys = jnp.where(before[..., None], key_cache.astype(f32), 0.0)
    keys = keys * lax.rsqrt(jnp.sum(keys * keys, -1, keepdims=True) + 1e-06)
    values = jnp.where(before[..., None], value_cache.astype(f32), 0.0)
    beta = jnp.where(before, jax.nn.sigmoid(strength), 0.0)
    amount = jnp.where(before, -speed * jax.nn.softplus(decay + offset) + extra, 0.0)
    upto = (position[:, None] <= position[None, :]).astype(f32)
    cumul = jnp.dot(amount, upto, precision=HIGHEST)
    last = cumul[:, -1:]
    earlier = position[:, None] > position[None, :]
    gaps = jnp.exp(jnp.where(earlier, cumul[:, :, None] - cumul[:, None, :], -jnp.inf))
    gram = jnp.einsum("bpk,bsk->bps", keys, keys, precision=HIGHEST)
    coupling = beta[:, :, None] * gram * gaps

    def mm(a, b):
        return jnp.einsum("bps,bsr->bpr", a, b, precision=HIGHEST)

    eye = jnp.eye(span, dtype=f32)

    def same(size):
        return (position[:, None] // size) == (position[None, :] // size)

    first = jnp.where(same(8), coupling, 0.0)
    second = mm(first, first)
    fourth = mm(second, second)
    inverse = mm(mm(eye - first, eye + second), eye + fourth)
    size = 8
    while size < span:
        below = jnp.where(same(2 * size) & ~same(size), coupling, 0.0)
        inverse = inverse - mm(mm(inverse, below), inverse)
        size *= 2
    carried = jnp.einsum("bpk,bkv->bpv", keys, recurrent, precision=HIGHEST)
    right = beta[..., None] * (values - jnp.exp(cumul)[..., None] * carried)
    updates = mm(inverse, right) * jnp.exp(last - cumul)[..., None]
    return jnp.exp(last)[..., None] * recurrent + jnp.einsum(
        "bpk,bpv->bkv", keys, updates, precision=HIGHEST
    )


def body(
    tokens,
    first_norm_gain,
    first_gate_weight,
    first_up_weight,
    first_down_weight,
    mixer_norm_gain,
    query_weight_matrix,
    key_weight_matrix,
    value_weight_matrix,
    output_gate_weight,
    strength_weight,
    decay_weight,
    head_decay_speed,
    head_decay_offset,
    head_norm_gain,
    mixer_out_weight,
    second_norm_gain,
    second_gate_weight,
    second_up_weight,
    second_down_weight,
    recurrent,
    earlier_key_cache,
    earlier_value_cache,
    strength_logit_history,
    decay_input_history,
    position_decay_extra,
    lengths,
):
    core, tp, z = lax.axis_index("c"), lax.axis_index("tp"), lax.axis_index("z")
    plane = lax.axis_size("tp")
    count, width = tokens.shape
    rows = count // 2

    def pair(x):
        return x, swap(x)

    gate1, up1, down1 = pair(first_gate_weight), pair(first_up_weight), pair(first_down_weight)
    gate2, up2, down2 = pair(second_gate_weight), pair(second_up_weight), pair(second_down_weight)
    projections = pair(
        jnp.concatenate(
            [query_weight_matrix, key_weight_matrix, value_weight_matrix, output_gate_weight], 1
        )
    )
    outs = pair(mixer_out_weight)
    gains = jnp.stack([first_norm_gain, mixer_norm_gain, second_norm_gain])
    gains = jnp.concatenate(pair(gains), axis=1)

    def small(which):
        corner = ((z * 2 + which) * width, tp)
        return jnp.concatenate(
            [lax.dynamic_slice(w, corner, (width, 1)) for w in (strength_weight, decay_weight)], 1
        )

    smalls = small(core), small(1 - core)

    state = earlier_state(
        recurrent[:, 0],
        earlier_key_cache,
        earlier_value_cache,
        strength_logit_history[0],
        decay_input_history[0],
        position_decay_extra[0],
        lengths,
        head_decay_speed[0],
        head_decay_offset[0],
    )

    blocks = jnp.broadcast_to(tokens.reshape(2, 1, rows, width), (2, plane, rows, width))
    got = lax.all_to_all(
        blocks.reshape(2 * plane, rows, width), ("c", "tp"), 0, 0, tiled=True
    ).reshape(2, plane * rows, width)
    wide = jnp.where(
        core == 0,
        jnp.concatenate([got[0], got[1]], 1),
        jnp.concatenate([got[1], got[0]], 1),
    ).astype(f32)

    part = branch(wide, gains[0], gate1, up1, down1)
    first_sum = summed(jnp.concatenate([p.astype(bf16) for p in part], 1), "tp")
    wide_own = lax.dynamic_slice_in_dim(wide, tp * rows, rows, 0)
    middle_own = (wide_own + 0.5 * first_sum).astype(bf16)
    middle = to_all(middle_own, "tp").reshape(-1, 2 * width).astype(f32)

    mix = (middle * gains[1]).astype(bf16)
    own, other = mix[:, :width], mix[:, width:]
    main = dot(own, projections[0]) + dot(other, projections[1])
    logit = dot(own, smalls[0]) + dot(other, smalls[1])
    squares = jnp.sum(middle * middle, -1, keepdims=True)
    n = main.shape[1]
    tail = hi_lo(jnp.concatenate([logit, squares], 1))
    got = summed(columns([main.astype(bf16), *tail], n + 128), "z")
    small_sums = got[:, n : n + 3] + got[:, n + 3 : n + 6]
    factor = lax.rsqrt(small_sums[:, 2:3] / D + 1e-06)
    dk = n // 4
    new_query, new_key, new_value, out_gate = [
        got[:, i * dk : (i + 1) * dk] * factor for i in range(4)
    ]
    beta = jax.nn.sigmoid(small_sums[:, 0:1] * factor)
    span = earlier_key_cache.shape[1]
    position = jnp.arange(span, dtype=jnp.int32)
    extra_new = jnp.sum(
        jnp.where(position[None, :] == (lengths - 1)[:, None], position_decay_extra[0], 0.0),
        -1,
        keepdims=True,
    )
    amount = (
        -head_decay_speed * jax.nn.softplus(small_sums[:, 1:2] * factor + head_decay_offset)
        + extra_new
    )
    query = new_query * lax.rsqrt(jnp.sum(new_query * new_query, -1, keepdims=True) + 1e-06)
    query = query * dk ** (-0.5)
    key = new_key * lax.rsqrt(jnp.sum(new_key * new_key, -1, keepdims=True) + 1e-06)
    score = jnp.sum(query * key, -1, keepdims=True)
    reduced = query - (score * beta) * key
    head_out = jnp.exp(amount) * jnp.einsum(
        "bk,bkv->bv", reduced, state, precision=HIGHEST
    ) + (score * beta) * new_value
    normed = head_out * lax.rsqrt(jnp.mean(head_out * head_out, -1, keepdims=True) + 1e-06)
    mixed = (normed * head_norm_gain[None, :] * jax.nn.silu(out_gate)).astype(bf16)

    mixed = to_all(mixed, "z").reshape(-1, dk)
    part = [dot(mixed, w) for w in outs]
    mixer_sum = summed(jnp.concatenate([p.astype(bf16) for p in part], 1), "tp")
    second_own = (middle_own.astype(f32) + mixer_sum).astype(bf16)
    got = to_all(second_own, ("c", "tp")).reshape(2, plane, rows, 2 * width)
    second = lax.dynamic_index_in_dim(got, core, 0, keepdims=False)
    second = second.reshape(-1, 2 * width).astype(f32)

    part = [p.astype(bf16) for p in branch(second, gains[2], gate2, up2, down2)]
    ordered = jnp.where(core == 0, jnp.stack(part), jnp.stack(part[::-1]))
    last = lax.all_to_all(
        ordered.reshape(2 * plane, rows, width), ("c", "tp"), 0, 0, tiled=True
    ).reshape(2, plane, rows, width)
    last = jnp.sum(last.astype(f32), axis=1).reshape(count, width)
    mine = lax.dynamic_index_in_dim(got, tp, 1, keepdims=False)
    flip = (lax.broadcasted_iota(jnp.int32, (2, 1, 1), 0) == core)
    mine = jnp.where(flip, mine[..., :width], mine[..., width:]).reshape(count, width)
    return (mine.astype(f32) + 0.5 * last).astype(bf16)


def solution(mesh):
    kv, tp = mesh.shape["kv"], mesh.shape["tp"]
    split = Mesh(mesh.devices.reshape(kv // 2, 2, tp), ("z", "c", "tp"))
    kv = ("z", "c")
    return jax.shard_map(
        body,
        mesh=split,
        in_specs=(
            P("tp", kv),
            P(kv),
            P(kv, "tp"),
            P(kv, "tp"),
            P("tp", kv),
            P(kv),
            P(kv, "tp"),
            P(kv, "tp"),
            P(kv, "tp"),
            P(kv, "tp"),
            P(),
            P(),
            P("tp"),
            P("tp"),
            P(),
            P("tp", kv),
            P(kv),
            P(kv, "tp"),
            P(kv, "tp"),
            P("tp", kv),
            P(kv, "tp", None, None),
            P(kv, None, "tp"),
            P(kv, None, "tp"),
            P("tp", kv, None),
            P("tp", kv, None),
            P("tp", kv, None),
            P(kv),
        ),
        out_specs=P("tp", kv),
        check_vma=False,
    )
```

```python
import functools

import jax
import jax.numpy as jnp
from jax import lax
from jax.experimental import pallas as pl
from jax.experimental.pallas import tpu as pltpu
from jax.sharding import Mesh, PartitionSpec as P

HIGHEST = lax.Precision.HIGHEST
f32 = jnp.float32
bf16 = jnp.bfloat16
LANES = 128
EPS = 1e-06


def kernel(fn, out, *args, scalars=0, flops=1 << 20, limit=12 << 20, **static):
    outs = out if isinstance(out, list) else [out]
    smem = pl.BlockSpec(memory_space=pltpu.SMEM)
    vmem = pl.BlockSpec(memory_space=pltpu.VMEM)
    shapes = [jax.ShapeDtypeStruct(s, d) for s, d in outs]
    size = sum(a.size * a.dtype.itemsize for a in args)
    got = pl.pallas_call(
        functools.partial(fn, **static),
        out_shape=shapes,
        in_specs=[smem] * scalars + [vmem] * (len(args) - scalars),
        out_specs=[vmem] * len(outs),
        compiler_params=pltpu.CompilerParams(vmem_limit_bytes=limit),
        cost_estimate=pl.CostEstimate(flops=flops, bytes_accessed=size, transcendentals=0),
        name=fn.__name__,
    )(*args)
    return got if isinstance(out, list) else got[0]


def dot(x, w):
    return jnp.dot(x, w, preferred_element_type=f32)


def dot_t(x, w):
    return lax.dot_general(x, w, (((1,), (1,)), ((), ())), preferred_element_type=f32)


def exact(x, y, contract=((1,), (0,))):
    return lax.dot_general(
        x, y, (contract, ((), ())), precision=HIGHEST, preferred_element_type=f32
    )


def flat(x):
    x = x.astype(f32)
    return x.reshape(-1, x.shape[-1])


def blocked(x, count):
    return x.reshape(count, -1, x.shape[-1])


def lane_tile(rows, columns):
    lane = lax.broadcasted_iota(jnp.int32, (rows, LANES), 1)
    tile = jnp.zeros((rows, LANES), f32)
    for i, column in enumerate(columns):
        high = column.astype(bf16).astype(f32)
        tile = jnp.where(lane == i, high, tile)
        tile = jnp.where(lane == i + len(columns), column - high, tile)
    return tile


def column_of(sums, start, i, count):
    at = start + i
    return sums[:, at : at + 1] + sums[:, at + count : at + count + 1]


def silu(x):
    return x * jax.nn.sigmoid(x)


def softplus(x):
    return jnp.maximum(x, 0.0) + jnp.log1p(jnp.exp(-jnp.abs(x)))


def gate_up(own, other, gain, gain_x, gates, ups, out):
    n = gates[0].shape[1]
    count = out.shape[0]
    scaled, scaled_x = (own * gain).astype(bf16), (other * gain_x).astype(bf16)
    for at, pair in ((0, gates), (n, ups)):
        part = dot(scaled, pair[0][...]) + dot(scaled_x, pair[1][...])
        out[:, :, at : at + n] = blocked(part, count).astype(bf16)
    square = jnp.sum(own * own + other * other, -1, keepdims=True)
    out[:, :, 2 * n :] = blocked(lane_tile(own.shape[0], [square]), count).astype(bf16)


def first_products(ids, got, gains, gains_x, gate, gate_x, up, up_x, out):
    core = ids[0]
    gate_up(
        flat(got[core]),
        flat(got[1 - core]),
        gains[0:1],
        gains_x[0:1],
        (gate, gate_x),
        (up, up_x),
        out,
    )


def second_products(ids, got, gains, gains_x, gate, gate_x, up, up_x, out):
    wide = flat(got[ids[0]])
    half = wide.shape[1] // 2
    gate_up(
        wide[:, :half],
        wide[:, half:],
        gains[2:3],
        gains_x[2:3],
        (gate, gate_x),
        (up, up_x),
        out,
    )


def activate(parts, out, *, features):
    sums = jnp.sum(parts[...].astype(f32), axis=0)
    n = (sums.shape[1] - LANES) // 2
    factor = lax.rsqrt(column_of(sums, 2 * n, 0, 1) / features + EPS)
    hidden = silu(sums[:, :n] * factor) * (sums[:, n : 2 * n] * factor)
    out[...] = jnp.broadcast_to(hidden[None], out.shape).astype(bf16)


def down(hidden, weight, weight_x, out):
    rows = flat(hidden[...]).astype(bf16)
    half = weight.shape[1]
    out[:, :, :half] = blocked(dot(rows, weight[...]), out.shape[0]).astype(bf16)
    out[:, :, half:] = blocked(dot(rows, weight_x[...]), out.shape[0]).astype(bf16)


def last_down(ids, hidden, weight, weight_x, out):
    rows = flat(hidden[...]).astype(bf16)
    out[ids[0]] = blocked(dot(rows, weight[...]), out.shape[1]).astype(bf16)
    out[1 - ids[0]] = blocked(dot(rows, weight_x[...]), out.shape[1]).astype(bf16)


def add_first(ids, parts, got, out):
    sums = jnp.sum(parts[...].astype(f32), axis=0)
    core, block = ids[0], ids[1]
    own, other = got[core, block].astype(f32), got[1 - core, block].astype(f32)
    rows = jnp.concatenate([own, other], 1) + 0.5 * sums
    out[...] = jnp.broadcast_to(rows[None], out.shape).astype(bf16)


def add_mixer(ids, parts, middle, out):
    sums = jnp.sum(parts[...].astype(f32), axis=0)
    rows = middle[ids[1]].astype(f32) + sums
    out[...] = jnp.broadcast_to(rows[None], out.shape).astype(bf16)


def project(ids, middle, gains, gains_x, main, main_x, ws, ws_x, wd, wd_x, out):
    wide = flat(middle[...])
    half = wide.shape[1] // 2
    own, other = wide[:, :half], wide[:, half:]
    scaled, scaled_x = (own * gains[1:2]).astype(bf16), (other * gains_x[1:2]).astype(bf16)
    n, count = main.shape[1], out.shape[0]
    part = dot(scaled, main[...]) + dot(scaled_x, main_x[...])
    out[:, :, :n] = blocked(part, count).astype(bf16)
    heads = ws.shape[0]
    mine = lax.broadcasted_iota(jnp.int32, (wide.shape[0], heads), 1) == ids[1]
    columns = []
    for w, w_x in ((ws, ws_x), (wd, wd_x)):
        logit = dot_t(scaled, w[...]) + dot_t(scaled_x, w_x[...])
        columns.append(jnp.sum(jnp.where(mine, logit, 0.0), -1, keepdims=True))
    columns.append(jnp.sum(own * own + other * other, -1, keepdims=True))
    out[:, :, n:] = blocked(lane_tile(wide.shape[0], columns), count).astype(bf16)


def earlier_state(lengths, head, recurrent, keys, values, strength, decay, extra, state, new):
    count, span = strength.shape
    sequence = lax.broadcasted_iota(jnp.int32, (count, span), 0)
    lane = lax.broadcasted_iota(jnp.int32, (count, span), 1)
    latest = jnp.zeros((count, span), jnp.int32)
    for b in range(count):
        latest = jnp.where(sequence == b, lengths[b] - 1, latest)
    before = lane < latest
    beta = jnp.where(before, jax.nn.sigmoid(strength[...]), 0.0)
    amount = extra[...] - head[0] * softplus(decay[...] + head[1])
    amount = jnp.where(before, amount, 0.0)
    new_extra = jnp.sum(jnp.where(lane == latest, extra[...], 0.0), -1, keepdims=True)
    new[...] = jnp.broadcast_to(new_extra, new.shape)
    row = lax.broadcasted_iota(jnp.int32, (span, span), 0)
    col = lax.broadcasted_iota(jnp.int32, (span, span), 1)
    cumul = exact(amount, (row <= col).astype(f32))
    last = cumul[:, span - 1 : span]
    eye = (row == col).astype(f32)
    stacked = jnp.concatenate(
        [beta, cumul, jnp.exp(cumul), jnp.exp(last - cumul), before.astype(f32)], 0
    )
    upright = exact(eye, stacked, ((1,), (1,)))

    def upright_column(which, b):
        at = which * count + b
        return upright[:, at : at + 1]

    every = range(count)
    ks, couplings = [], []
    for b in every:
        k = keys[b].astype(f32) * upright_column(4, b)
        k = k * lax.rsqrt(jnp.sum(k * k, -1, keepdims=True) + EPS)
        gap = upright_column(1, b) - cumul[b : b + 1]
        gap = jnp.exp(jnp.where(row > col, gap, -jnp.inf))
        ks.append(k)
        couplings.append(upright_column(0, b) * exact(k, k, ((1,), (1,))) * gap)

    def same(size):
        return (row // size) == (col // size)

    first = [jnp.where(same(8), c, 0.0) for c in couplings]
    second = [exact(a, a) for a in first]
    fourth = [exact(a, a) for a in second]
    inverse = [exact(eye - a, eye + b) for a, b in zip(first, second)]
    inverse = [exact(a, eye + b) for a, b in zip(inverse, fourth)]
    size = 8
    while size < span:
        inside = same(2 * size) & ~same(size)
        right = [exact(jnp.where(inside, c, 0.0), a) for c, a in zip(couplings, inverse)]
        inverse = [a - exact(a, r) for a, r in zip(inverse, right)]
        size *= 2
    for b in every:
        carried = exact(ks[b], recurrent[b])
        value = values[b].astype(f32) * upright_column(4, b)
        side = upright_column(0, b) * (value - upright_column(2, b) * carried)
        update = exact(inverse[b], side) * upright_column(3, b)
        kept = jnp.exp(last[b : b + 1]) * recurrent[b]
        state[b] = kept + exact(ks[b], update, ((0,), (0,)))


def new_token(head, parts, state, new_extra, norm_gain, out, *, features):
    sums = jnp.sum(parts[...].astype(f32), axis=0)
    dk = (sums.shape[1] - LANES) // 4
    strength, decay, square = (column_of(sums, 4 * dk, i, 3) for i in range(3))
    factor = lax.rsqrt(square / features + EPS)
    query, key, value, gate = (sums[:, i * dk : (i + 1) * dk] * factor for i in range(4))
    beta = jax.nn.sigmoid(strength * factor)
    amount = new_extra[:, 0:1] - head[0] * softplus(decay * factor + head[1])
    query = query * lax.rsqrt(jnp.sum(query * query, -1, keepdims=True) + EPS) * dk**-0.5
    key = key * lax.rsqrt(jnp.sum(key * key, -1, keepdims=True) + EPS)
    score = jnp.sum(query * key, -1, keepdims=True)
    reduced = jnp.transpose(query - (score * beta) * key)
    sequence = lax.broadcasted_iota(jnp.int32, value.shape, 0)
    read = jnp.zeros(value.shape, f32)
    for b in range(value.shape[0]):
        one = jnp.sum(reduced[:, b : b + 1] * state[b], axis=0, keepdims=True)
        read = jnp.where(sequence == b, one, read)
    rows = jnp.exp(amount) * read + (score * beta) * value
    rows = rows * lax.rsqrt(jnp.mean(rows * rows, -1, keepdims=True) + EPS)
    rows = rows * norm_gain[...] * silu(gate)
    out[...] = jnp.broadcast_to(rows[None], out.shape).astype(bf16)


def finish(ids, parts, got, out):
    core, block = ids[0], ids[1]
    sums = jnp.sum(parts[...].astype(f32), axis=1)
    half = sums.shape[-1]
    rows = []
    for c in range(2):
        wide = got[c, block].astype(f32)
        mine = jnp.where(core == c, wide[:, :half], wide[:, half:])
        rows.append(mine + 0.5 * sums[c])
    out[...] = jnp.concatenate(rows, 0).astype(bf16)


def exchange(x, axis):
    return lax.all_to_all(x, axis, 0, 0, tiled=True)


def swap(x):
    return lax.ppermute(x, "c", [(0, 1), (1, 0)])


def together(*trees):
    return lax.optimization_barrier(trees)


def body(
    tokens,
    first_norm_gain,
    first_gate_weight,
    first_up_weight,
    first_down_weight,
    mixer_norm_gain,
    query_weight_matrix,
    key_weight_matrix,
    value_weight_matrix,
    output_gate_weight,
    strength_weight,
    decay_weight,
    head_decay_speed,
    head_decay_offset,
    head_norm_gain,
    mixer_out_weight,
    second_norm_gain,
    second_gate_weight,
    second_up_weight,
    second_down_weight,
    recurrent,
    earlier_key_cache,
    earlier_value_cache,
    strength_logit_history,
    decay_input_history,
    position_decay_extra,
    lengths,
):
    core, tp, z = lax.axis_index("c"), lax.axis_index("tp"), lax.axis_index("z")
    plane, ring = lax.axis_size("tp"), lax.axis_size("z")
    count, width = tokens.shape
    rows = count // 2
    features = 2 * ring * width
    hidden_units = first_gate_weight.shape[1]
    dk = query_weight_matrix.shape[1]
    ids = jnp.stack([core, tp]).astype(jnp.int32)
    head = jnp.concatenate([head_decay_speed, head_decay_offset])

    blocks = jnp.broadcast_to(tokens.reshape(2, 1, rows, width), (2, plane, rows, width))
    with jax.named_scope("tokens"):
        got = exchange(blocks.reshape(2 * plane, rows, width), ("c", "tp"))
    got = got.reshape(2, plane, rows, width)

    gains = jnp.stack([first_norm_gain, mixer_norm_gain, second_norm_gain])
    with jax.named_scope("early"):
        gains_x, gate_x, up_x = swap(gains), swap(first_gate_weight), swap(first_up_weight)
    sent = kernel(
        first_products,
        ((ring, rows, 2 * hidden_units + LANES), bf16),
        ids,
        got,
        gains,
        gains_x,
        first_gate_weight,
        gate_x,
        first_up_weight,
        up_x,
        scalars=1,
    )

    sent, later = together(
        sent,
        (
            first_down_weight,
            query_weight_matrix,
            key_weight_matrix,
            value_weight_matrix,
            output_gate_weight,
            strength_weight,
            decay_weight,
            recurrent,
            earlier_key_cache,
            earlier_value_cache,
            strength_logit_history,
            decay_input_history,
            position_decay_extra,
            lengths,
            mixer_out_weight,
            second_gate_weight,
            second_up_weight,
            second_down_weight,
        ),
    )
    (
        first_down_weight,
        query_weight_matrix,
        key_weight_matrix,
        value_weight_matrix,
        output_gate_weight,
        strength_weight,
        decay_weight,
        recurrent,
        earlier_key_cache,
        earlier_value_cache,
        strength_logit_history,
        decay_input_history,
        position_decay_extra,
        lengths,
        mixer_out_weight,
        second_gate_weight,
        second_up_weight,
        second_down_weight,
    ) = later
    parts = exchange(sent, "z")
    down_x = swap(first_down_weight)
    main = jnp.concatenate(
        [query_weight_matrix, key_weight_matrix, value_weight_matrix, output_gate_weight], 1
    )
    main_x = swap(main)

    def small(w, which):
        return lax.dynamic_slice_in_dim(w.T, (z * 2 + which) * width, width, 1)

    ws, ws_x = small(strength_weight, core), small(strength_weight, 1 - core)
    wd, wd_x = small(decay_weight, core), small(decay_weight, 1 - core)
    local = lengths.shape[0]
    state, new_extra = kernel(
        earlier_state,
        [((local, dk, recurrent.shape[-1]), f32), ((local, LANES), f32)],
        lengths,
        head,
        recurrent[:, 0],
        earlier_key_cache,
        earlier_value_cache,
        strength_logit_history[0],
        decay_input_history[0],
        position_decay_extra[0],
        scalars=2,
        flops=1 << 28,
    )
    parts, down_x, main, main_x, ws, ws_x, wd, wd_x, state, new_extra = together(
        parts, down_x, main, main_x, ws, ws_x, wd, wd_x, state, new_extra
    )

    hidden = kernel(
        activate, ((ring, rows, hidden_units), bf16), parts, features=features
    )
    hidden, later = together(
        hidden, (mixer_out_weight, second_gate_weight, second_up_weight, second_down_weight)
    )
    mixer_out_weight, second_gate_weight, second_up_weight, second_down_weight = later
    hidden = exchange(hidden, "z")
    out_x, gate2_x = swap(mixer_out_weight), swap(second_gate_weight)
    up2_x, down2_x = swap(second_up_weight), swap(second_down_weight)
    hidden, out_x, gate2_x, up2_x, down2_x = together(hidden, out_x, gate2_x, up2_x, down2_x)

    parts = kernel(down, ((plane, rows, 2 * width), bf16), hidden, first_down_weight, down_x)
    parts = exchange(parts, "tp")
    middle = kernel(add_first, ((plane, rows, 2 * width), bf16), ids, parts, got, scalars=1)
    middle = exchange(middle, "tp")

    parts = kernel(
        project,
        ((ring, rows, 4 * dk + LANES), bf16),
        ids,
        middle,
        gains,
        gains_x,
        main,
        main_x,
        ws,
        ws_x,
        wd,
        wd_x,
        scalars=1,
    )
    parts = exchange(parts, "z")
    mixed = kernel(
        new_token,
        ((ring, rows, dk), bf16),
        head,
        parts,
        state,
        new_extra,
        head_norm_gain[None],
        scalars=1,
        features=features,
    )
    mixed = exchange(mixed, "z")
    parts = kernel(down, ((plane, rows, 2 * width), bf16), mixed, mixer_out_weight, out_x)
    parts = exchange(parts, "tp")
    second = kernel(add_mixer, ((2 * plane, rows, 2 * width), bf16), ids, parts, middle, scalars=1)
    second = exchange(second, ("c", "tp")).reshape(2, plane, rows, 2 * width)

    sent = kernel(
        second_products,
        ((ring, rows, 2 * hidden_units + LANES), bf16),
        ids,
        second,
        gains,
        gains_x,
        second_gate_weight,
        gate2_x,
        second_up_weight,
        up2_x,
        scalars=1,
    )
    parts = exchange(sent, "z")
    hidden = kernel(
        activate, ((ring, rows, hidden_units), bf16), parts, features=features
    )
    hidden = exchange(hidden, "z")
    parts = kernel(
        last_down,
        ((2, plane, rows, width), bf16),
        ids,
        hidden,
        second_down_weight,
        down2_x,
        scalars=1,
    )
    parts = exchange(parts.reshape(2 * plane, rows, width), ("c", "tp"))
    parts = parts.reshape(2, plane, rows, width)
    return kernel(finish, ((count, width), bf16), ids, parts, second, scalars=1)


def solution(mesh):
    kv, tp = mesh.shape["kv"], mesh.shape["tp"]
    split = Mesh(mesh.devices.reshape(kv // 2, 2, tp), ("z", "c", "tp"))
    kv = ("z", "c")
    return jax.shard_map(
        body,
        mesh=split,
        in_specs=(
            P("tp", kv),
            P(kv),
            P(kv, "tp"),
            P(kv, "tp"),
            P("tp", kv),
            P(kv),
            P(kv, "tp"),
            P(kv, "tp"),
            P(kv, "tp"),
            P(kv, "tp"),
            P(),
            P(),
            P("tp"),
            P("tp"),
            P(),
            P("tp", kv),
            P(kv),
            P(kv, "tp"),
            P(kv, "tp"),
            P("tp", kv),
            P(kv, "tp", None, None),
            P(kv, None, "tp"),
            P(kv, None, "tp"),
            P("tp", kv, None),
            P("tp", kv, None),
            P("tp", kv, None),
            P(kv),
        ),
        out_specs=P("tp", kv),
        check_vma=False,
    )
```

```python
import functools

import jax
import jax.numpy as jnp
from jax import lax
from jax.experimental import pallas as pl
from jax.experimental.pallas import tpu as pltpu
from jax.sharding import Mesh, PartitionSpec as P

HIGHEST = lax.Precision.HIGHEST
f32 = jnp.float32
bf16 = jnp.bfloat16
LANES = 128
EPS = 1e-06


def kernel(fn, out, *args, scalars=0, flops=1 << 20, limit=12 << 20, **static):
    outs = out if isinstance(out, list) else [out]
    smem = pl.BlockSpec(memory_space=pltpu.SMEM)
    vmem = pl.BlockSpec(memory_space=pltpu.VMEM)
    shapes = [jax.ShapeDtypeStruct(s, d) for s, d in outs]
    size = sum(a.size * a.dtype.itemsize for a in args)
    got = pl.pallas_call(
        functools.partial(fn, **static),
        out_shape=shapes,
        in_specs=[smem] * scalars + [vmem] * (len(args) - scalars),
        out_specs=[vmem] * len(outs),
        compiler_params=pltpu.CompilerParams(vmem_limit_bytes=limit),
        cost_estimate=pl.CostEstimate(flops=flops, bytes_accessed=size, transcendentals=0),
    )(*args)
    return got if isinstance(out, list) else got[0]


def dot(x, w):
    return jnp.dot(x, w, preferred_element_type=f32)


def dot_t(x, w):
    return lax.dot_general(x, w, (((1,), (1,)), ((), ())), preferred_element_type=f32)


def exact(x, y, contract=((1,), (0,))):
    return lax.dot_general(
        x, y, (contract, ((), ())), precision=HIGHEST, preferred_element_type=f32
    )


def flat(x):
    x = x.astype(f32)
    return x.reshape(-1, x.shape[-1])


def blocked(x, count):
    return x.reshape(count, -1, x.shape[-1])


def lane_tile(rows, columns):
    lane = lax.broadcasted_iota(jnp.int32, (rows, LANES), 1)
    tile = jnp.zeros((rows, LANES), f32)
    for i, column in enumerate(columns):
        high = column.astype(bf16).astype(f32)
        tile = jnp.where(lane == i, high, tile)
        tile = jnp.where(lane == i + len(columns), column - high, tile)
    return tile


def column_of(sums, start, i, count):
    at = start + i
    return sums[:, at : at + 1] + sums[:, at + count : at + count + 1]


def silu(x):
    return x * jax.nn.sigmoid(x)


def softplus(x):
    return jnp.maximum(x, 0.0) + jnp.log1p(jnp.exp(-jnp.abs(x)))


def gate_up(own, other, gain, gain_x, gates, ups, out):
    n = gates[0].shape[1]
    count = out.shape[0]
    scaled, scaled_x = (own * gain).astype(bf16), (other * gain_x).astype(bf16)
    for at, pair in ((0, gates), (n, ups)):
        part = dot(scaled, pair[0][...]) + dot(scaled_x, pair[1][...])
        out[:, :, at : at + n] = blocked(part, count).astype(bf16)
    square = jnp.sum(own * own + other * other, -1, keepdims=True)
    out[:, :, 2 * n :] = blocked(lane_tile(own.shape[0], [square]), count).astype(bf16)


def first_products(ids, got, gains, gains_x, gate, gate_x, up, up_x, out):
    core = ids[0]
    gate_up(
        flat(got[core]),
        flat(got[1 - core]),
        gains[0:1],
        gains_x[0:1],
        (gate, gate_x),
        (up, up_x),
        out,
    )


def second_products(ids, got, gains, gains_x, gate, gate_x, up, up_x, out):
    wide = flat(got[ids[0]])
    half = wide.shape[1] // 2
    gate_up(
        wide[:, :half],
        wide[:, half:],
        gains[2:3],
        gains_x[2:3],
        (gate, gate_x),
        (up, up_x),
        out,
    )


def activate(parts, out, *, features):
    sums = jnp.sum(parts[...].astype(f32), axis=0)
    n = (sums.shape[1] - LANES) // 2
    factor = lax.rsqrt(column_of(sums, 2 * n, 0, 1) / features + EPS)
    hidden = silu(sums[:, :n] * factor) * (sums[:, n : 2 * n] * factor)
    out[...] = jnp.broadcast_to(hidden[None], out.shape).astype(bf16)


def down(hidden, weight, weight_x, out):
    rows = flat(hidden[...]).astype(bf16)
    half = weight.shape[1]
    out[:, :, :half] = blocked(dot(rows, weight[...]), out.shape[0]).astype(bf16)
    out[:, :, half:] = blocked(dot(rows, weight_x[...]), out.shape[0]).astype(bf16)


def last_down(ids, hidden, weight, weight_x, out):
    rows = flat(hidden[...]).astype(bf16)
    out[ids[0]] = blocked(dot(rows, weight[...]), out.shape[1]).astype(bf16)
    out[1 - ids[0]] = blocked(dot(rows, weight_x[...]), out.shape[1]).astype(bf16)


def add_first(ids, parts, got, out):
    sums = jnp.sum(parts[...].astype(f32), axis=0)
    core, block = ids[0], ids[1]
    own, other = got[core, block].astype(f32), got[1 - core, block].astype(f32)
    rows = jnp.concatenate([own, other], 1) + 0.5 * sums
    out[...] = jnp.broadcast_to(rows[None], out.shape).astype(bf16)


def add_mixer(ids, parts, middle, out):
    sums = jnp.sum(parts[...].astype(f32), axis=0)
    rows = middle[ids[1]].astype(f32) + sums
    out[...] = jnp.broadcast_to(rows[None], out.shape).astype(bf16)


def project(ids, middle, gains, gains_x, main, main_x, ws, ws_x, wd, wd_x, out):
    wide = flat(middle[...])
    half = wide.shape[1] // 2
    own, other = wide[:, :half], wide[:, half:]
    scaled, scaled_x = (own * gains[1:2]).astype(bf16), (other * gains_x[1:2]).astype(bf16)
    n, count = main.shape[1], out.shape[0]
    part = dot(scaled, main[...]) + dot(scaled_x, main_x[...])
    out[:, :, :n] = blocked(part, count).astype(bf16)
    heads = ws.shape[0]
    mine = lax.broadcasted_iota(jnp.int32, (wide.shape[0], heads), 1) == ids[1]
    columns = []
    for w, w_x in ((ws, ws_x), (wd, wd_x)):
        logit = dot_t(scaled, w[...]) + dot_t(scaled_x, w_x[...])
        columns.append(jnp.sum(jnp.where(mine, logit, 0.0), -1, keepdims=True))
    columns.append(jnp.sum(own * own + other * other, -1, keepdims=True))
    out[:, :, n:] = blocked(lane_tile(wide.shape[0], columns), count).astype(bf16)


def earlier_state(
    lengths, head, recurrent, keys, values, strength, decay, extra, gain, state, new, gains
):
    count, span = strength.shape
    sequence = lax.broadcasted_iota(jnp.int32, (count, span), 0)
    lane = lax.broadcasted_iota(jnp.int32, (count, span), 1)
    latest = jnp.zeros((count, span), jnp.int32)
    for b in range(count):
        latest = jnp.where(sequence == b, lengths[b] - 1, latest)
    before = lane < latest
    beta = jnp.where(before, jax.nn.sigmoid(strength[...]), 0.0)
    amount = extra[...] - head[0] * softplus(decay[...] + head[1])
    amount = jnp.where(before, amount, 0.0)
    new_extra = jnp.sum(jnp.where(lane == latest, extra[...], 0.0), -1, keepdims=True)
    new[...] = jnp.broadcast_to(new_extra, new.shape)
    gains[...] = jnp.broadcast_to(gain[...], gains.shape)
    row = lax.broadcasted_iota(jnp.int32, (span, span), 0)
    col = lax.broadcasted_iota(jnp.int32, (span, span), 1)
    cumul = exact(amount, (row <= col).astype(f32))
    last = cumul[:, span - 1 : span]
    eye = (row == col).astype(f32)
    stacked = jnp.concatenate(
        [beta, cumul, jnp.exp(cumul), jnp.exp(last - cumul), before.astype(f32)], 0
    )
    upright = exact(eye, stacked, ((1,), (1,)))

    def upright_column(which, b):
        at = which * count + b
        return upright[:, at : at + 1]

    every = range(count)
    ks, couplings = [], []
    for b in every:
        k = keys[b].astype(f32) * upright_column(4, b)
        k = k * lax.rsqrt(jnp.sum(k * k, -1, keepdims=True) + EPS)
        gap = upright_column(1, b) - cumul[b : b + 1]
        gap = jnp.exp(jnp.where(row > col, gap, -jnp.inf))
        ks.append(k)
        couplings.append(upright_column(0, b) * exact(k, k, ((1,), (1,))) * gap)

    def same(size):
        return (row // size) == (col // size)

    first = [jnp.where(same(8), c, 0.0) for c in couplings]
    second = [exact(a, a) for a in first]
    fourth = [exact(a, a) for a in second]
    inverse = [exact(eye - a, eye + b) for a, b in zip(first, second)]
    inverse = [exact(a, eye + b) for a, b in zip(inverse, fourth)]
    size = 8
    while size < span:
        inside = same(2 * size) & ~same(size)
        right = [exact(jnp.where(inside, c, 0.0), a) for c, a in zip(couplings, inverse)]
        inverse = [a - exact(a, r) for a, r in zip(inverse, right)]
        size *= 2
    for b in every:
        carried = exact(ks[b], recurrent[b])
        value = values[b].astype(f32) * upright_column(4, b)
        side = upright_column(0, b) * (value - upright_column(2, b) * carried)
        update = exact(inverse[b], side) * upright_column(3, b)
        kept = jnp.exp(last[b : b + 1]) * recurrent[b]
        state[b] = kept + exact(ks[b], update, ((0,), (0,)))


def new_token(head, parts, state, new_extra, norm_gain, out, *, features):
    sums = jnp.sum(parts[...].astype(f32), axis=0)
    dk = (sums.shape[1] - LANES) // 4
    strength, decay, square = (column_of(sums, 4 * dk, i, 3) for i in range(3))
    factor = lax.rsqrt(square / features + EPS)
    query, key, value, gate = (sums[:, i * dk : (i + 1) * dk] * factor for i in range(4))
    beta = jax.nn.sigmoid(strength * factor)
    amount = new_extra[:, 0:1] - head[0] * softplus(decay * factor + head[1])
    query = query * lax.rsqrt(jnp.sum(query * query, -1, keepdims=True) + EPS) * dk**-0.5
    key = key * lax.rsqrt(jnp.sum(key * key, -1, keepdims=True) + EPS)
    score = jnp.sum(query * key, -1, keepdims=True)
    reduced = jnp.transpose(query - (score * beta) * key)
    sequence = lax.broadcasted_iota(jnp.int32, value.shape, 0)
    read = jnp.zeros(value.shape, f32)
    for b in range(value.shape[0]):
        one = jnp.sum(reduced[:, b : b + 1] * state[b], axis=0, keepdims=True)
        read = jnp.where(sequence == b, one, read)
    rows = jnp.exp(amount) * read + (score * beta) * value
    rows = rows * lax.rsqrt(jnp.mean(rows * rows, -1, keepdims=True) + EPS)
    rows = rows * norm_gain[...] * silu(gate)
    out[...] = jnp.broadcast_to(rows[None], out.shape).astype(bf16)


def finish(ids, parts, got, out):
    core, block = ids[0], ids[1]
    sums = jnp.sum(parts[...].astype(f32), axis=1)
    half = sums.shape[-1]
    rows = []
    for c in range(2):
        wide = got[c, block].astype(f32)
        mine = jnp.where(core == c, wide[:, :half], wide[:, half:])
        rows.append(mine + 0.5 * sums[c])
    out[...] = jnp.concatenate(rows, 0).astype(bf16)


def exchange(x, axis):
    return lax.all_to_all(x, axis, 0, 0, tiled=True)


def swap(x):
    return lax.ppermute(x, "c", [(0, 1), (1, 0)])


def together(*trees):
    return lax.optimization_barrier(trees)


def layer(
    tokens,
    first_norm_gain,
    first_gate_weight,
    first_up_weight,
    first_down_weight,
    mixer_norm_gain,
    query_weight_matrix,
    key_weight_matrix,
    value_weight_matrix,
    output_gate_weight,
    strength_weight,
    decay_weight,
    head_decay_speed,
    head_decay_offset,
    head_norm_gain,
    mixer_out_weight,
    second_norm_gain,
    second_gate_weight,
    second_up_weight,
    second_down_weight,
    recurrent,
    earlier_key_cache,
    earlier_value_cache,
    strength_logit_history,
    decay_input_history,
    position_decay_extra,
    lengths,
):
    core, tp, z = lax.axis_index("c"), lax.axis_index("tp"), lax.axis_index("z")
    plane, ring = lax.axis_size("tp"), lax.axis_size("z")
    count, width = tokens.shape
    rows = count // 2
    features = 2 * ring * width
    hidden_units = first_gate_weight.shape[1]
    dk = query_weight_matrix.shape[1]
    ids = jnp.stack([core, tp]).astype(jnp.int32)
    head = jnp.concatenate([head_decay_speed, head_decay_offset])

    blocks = jnp.broadcast_to(tokens.reshape(2, 1, rows, width), (2, plane, rows, width))
    got = exchange(blocks.reshape(2 * plane, rows, width), ("c", "tp"))
    got = got.reshape(2, plane, rows, width)

    gains = jnp.stack([first_norm_gain, mixer_norm_gain, second_norm_gain])
    gate_x = swap(first_gate_weight)
    up_x = swap(first_up_weight)
    gains_x = swap(gains)
    sent = kernel(
        first_products,
        ((ring, rows, 2 * hidden_units + LANES), bf16),
        ids,
        got,
        gains,
        gains_x,
        first_gate_weight,
        gate_x,
        first_up_weight,
        up_x,
        scalars=1,
    )

    sent, later = together(
        sent,
        (
            first_down_weight,
            query_weight_matrix,
            key_weight_matrix,
            value_weight_matrix,
            output_gate_weight,
            strength_weight,
            decay_weight,
            recurrent,
            earlier_key_cache,
            earlier_value_cache,
            strength_logit_history,
            decay_input_history,
            position_decay_extra,
            lengths,
            head_norm_gain,
            mixer_out_weight,
            second_gate_weight,
            second_up_weight,
            second_down_weight,
        ),
    )
    (
        first_down_weight,
        query_weight_matrix,
        key_weight_matrix,
        value_weight_matrix,
        output_gate_weight,
        strength_weight,
        decay_weight,
        recurrent,
        earlier_key_cache,
        earlier_value_cache,
        strength_logit_history,
        decay_input_history,
        position_decay_extra,
        lengths,
        head_norm_gain,
        mixer_out_weight,
        second_gate_weight,
        second_up_weight,
        second_down_weight,
    ) = later
    parts = exchange(sent, "z")
    down_x = swap(first_down_weight)
    main = jnp.concatenate(
        [query_weight_matrix, key_weight_matrix, value_weight_matrix, output_gate_weight], 1
    )
    main_x = swap(main)

    def small(w, which):
        return lax.dynamic_slice_in_dim(w.T, (z * 2 + which) * width, width, 1)

    ws, ws_x = small(strength_weight, core), small(strength_weight, 1 - core)
    wd, wd_x = small(decay_weight, core), small(decay_weight, 1 - core)
    local = lengths.shape[0]
    state, new_extra, norm_gain = kernel(
        earlier_state,
        [
            ((local, dk, recurrent.shape[-1]), f32),
            ((local, LANES), f32),
            ((local, recurrent.shape[-1]), f32),
        ],
        lengths,
        head,
        recurrent[:, 0],
        earlier_key_cache,
        earlier_value_cache,
        strength_logit_history[0],
        decay_input_history[0],
        position_decay_extra[0],
        head_norm_gain[None],
        scalars=2,
        flops=1 << 28,
    )
    parts, down_x, main, main_x, ws, ws_x, wd, wd_x, state, new_extra, norm_gain = together(
        parts, down_x, main, main_x, ws, ws_x, wd, wd_x, state, new_extra, norm_gain
    )

    hidden = kernel(
        activate, ((ring, rows, hidden_units), bf16), parts, features=features
    )
    hidden, later = together(
        hidden, (mixer_out_weight, second_gate_weight, second_up_weight, second_down_weight)
    )
    mixer_out_weight, second_gate_weight, second_up_weight, second_down_weight = later
    hidden = exchange(hidden, "z")
    out_x, gate2_x = swap(mixer_out_weight), swap(second_gate_weight)
    up2_x, down2_x = swap(second_up_weight), swap(second_down_weight)
    hidden, out_x, gate2_x, up2_x, down2_x = together(hidden, out_x, gate2_x, up2_x, down2_x)

    parts = kernel(down, ((plane, rows, 2 * width), bf16), hidden, first_down_weight, down_x)
    parts = exchange(parts, "tp")
    middle = kernel(add_first, ((plane, rows, 2 * width), bf16), ids, parts, got, scalars=1)
    middle = exchange(middle, "tp")

    parts = kernel(
        project,
        ((ring, rows, 4 * dk + LANES), bf16),
        ids,
        middle,
        gains,
        gains_x,
        main,
        main_x,
        ws,
        ws_x,
        wd,
        wd_x,
        scalars=1,
    )
    parts = exchange(parts, "z")
    mixed = kernel(
        new_token,
        ((ring, rows, dk), bf16),
        head,
        parts,
        state,
        new_extra,
        norm_gain,
        scalars=1,
        features=features,
    )
    mixed = exchange(mixed, "z")
    parts = kernel(down, ((plane, rows, 2 * width), bf16), mixed, mixer_out_weight, out_x)
    parts = exchange(parts, "tp")
    second = kernel(add_mixer, ((2 * plane, rows, 2 * width), bf16), ids, parts, middle, scalars=1)
    second = exchange(second, ("c", "tp")).reshape(2, plane, rows, 2 * width)

    sent = kernel(
        second_products,
        ((ring, rows, 2 * hidden_units + LANES), bf16),
        ids,
        second,
        gains,
        gains_x,
        second_gate_weight,
        gate2_x,
        second_up_weight,
        up2_x,
        scalars=1,
    )
    parts = exchange(sent, "z")
    hidden = kernel(
        activate, ((ring, rows, hidden_units), bf16), parts, features=features
    )
    hidden = exchange(hidden, "z")
    parts = kernel(
        last_down,
        ((2, plane, rows, width), bf16),
        ids,
        hidden,
        second_down_weight,
        down2_x,
        scalars=1,
    )
    parts = exchange(parts.reshape(2 * plane, rows, width), ("c", "tp"))
    parts = parts.reshape(2, plane, rows, width)
    return kernel(finish, ((count, width), bf16), ids, parts, second, scalars=1)


def solution(mesh):
    kv, tp = mesh.shape["kv"], mesh.shape["tp"]
    split = Mesh(mesh.devices.reshape(kv // 2, 2, tp), ("z", "c", "tp"))
    kv = ("z", "c")
    return jax.shard_map(
        layer,
        mesh=split,
        in_specs=(
            P("tp", kv),
            P(kv),
            P(kv, "tp"),
            P(kv, "tp"),
            P("tp", kv),
            P(kv),
            P(kv, "tp"),
            P(kv, "tp"),
            P(kv, "tp"),
            P(kv, "tp"),
            P(),
            P(),
            P("tp"),
            P("tp"),
            P(),
            P("tp", kv),
            P(kv),
            P(kv, "tp"),
            P(kv, "tp"),
            P("tp", kv),
            P(kv, "tp", None, None),
            P(kv, None, "tp"),
            P(kv, None, "tp"),
            P("tp", kv, None),
            P("tp", kv, None),
            P("tp", kv, None),
            P(kv),
        ),
        out_specs=P("tp", kv),
        check_vma=False,
    )
```

```python
import functools

import jax
import jax.numpy as jnp
from jax import lax
from jax.experimental import pallas as pl
from jax.experimental.pallas import tpu as pltpu
from jax.sharding import Mesh, PartitionSpec as P

HIGHEST = lax.Precision.HIGHEST
f32 = jnp.float32
bf16 = jnp.bfloat16
LANES = 128
Z = ("zh", "za")
EPS = 1e-06


def kernel(fn, out, *args, scalars=0, flops=1 << 20, limit=12 << 20, **static):
    outs = out if isinstance(out, list) else [out]
    smem = pl.BlockSpec(memory_space=pltpu.SMEM)
    vmem = pl.BlockSpec(memory_space=pltpu.VMEM)
    shapes = [jax.ShapeDtypeStruct(s, d) for s, d in outs]
    size = sum(a.size * a.dtype.itemsize for a in args)
    got = pl.pallas_call(
        functools.partial(fn, **static),
        out_shape=shapes,
        in_specs=[smem] * scalars + [vmem] * (len(args) - scalars),
        out_specs=[vmem] * len(outs),
        compiler_params=pltpu.CompilerParams(vmem_limit_bytes=limit),
        cost_estimate=pl.CostEstimate(flops=flops, bytes_accessed=size, transcendentals=0),
    )(*args)
    return got if isinstance(out, list) else got[0]


def dot(x, w):
    return jnp.dot(x, w, preferred_element_type=f32)


def dot_t(x, w):
    return lax.dot_general(x, w, (((1,), (1,)), ((), ())), preferred_element_type=f32)


def exact(x, y, contract=((1,), (0,))):
    return lax.dot_general(
        x, y, (contract, ((), ())), precision=HIGHEST, preferred_element_type=f32
    )


def flat(x):
    x = x.astype(f32)
    return x.reshape(-1, x.shape[-1])


def blocked(x, count):
    return x.reshape(count, -1, x.shape[-1])


def lane_tile(rows, columns):
    lane = lax.broadcasted_iota(jnp.int32, (rows, LANES), 1)
    tile = jnp.zeros((rows, LANES), f32)
    for i, column in enumerate(columns):
        high = column.astype(bf16).astype(f32)
        tile = jnp.where(lane == i, high, tile)
        tile = jnp.where(lane == i + len(columns), column - high, tile)
    return tile


def column_of(sums, start, i, count):
    at = start + i
    return sums[:, at : at + 1] + sums[:, at + count : at + count + 1]


def silu(x):
    return x * jax.nn.sigmoid(x)


def softplus(x):
    return jnp.maximum(x, 0.0) + jnp.log1p(jnp.exp(-jnp.abs(x)))


def gate_up(slots, gates, ups, out):
    n = gates[0].shape[1]
    count = out.shape[0]
    scaled = [(x * gain).astype(bf16) for x, gain in slots]
    for at, weights in ((0, gates), (n, ups)):
        part = sum(dot(x, w[...]) for x, w in zip(scaled, weights))
        out[:, :, at : at + n] = blocked(part, count).astype(bf16)
    square = jnp.sum(sum(x * x for x, _ in slots), -1, keepdims=True)
    out[:, :, 2 * n :] = blocked(lane_tile(square.shape[0], [square]), count).astype(bf16)


def first_products(ids, got, gains, gains_x, gate, gate_x, up, up_x, out):
    core = ids[0]
    slots = [(flat(got[core]), gains[0:1]), (flat(got[1 - core]), gains_x[0:1])]
    gate_up(slots, (gate, gate_x), (up, up_x), out)


def second_products(ids, got, gains, gains_x, gains_z, *refs):
    out = refs[-1]
    side = ids[2]
    slots = []
    for chip, pair in ((side, (gains, gains_x)), (1 - side, (gains_z.at[0], gains_z.at[1]))):
        wide = flat(got[chip, :, side])
        half = wide.shape[1] // 2
        slots += [(wide[:, :half], pair[0][2:3]), (wide[:, half:], pair[1][2:3])]
    gate_up(slots, refs[0:4], refs[4:8], out)


def activate(parts, out, *, features):
    sums = jnp.sum(parts[...].astype(f32), axis=0)
    n = (sums.shape[1] - LANES) // 2
    factor = lax.rsqrt(column_of(sums, 2 * n, 0, 1) / features + EPS)
    hidden = silu(sums[:, :n] * factor) * (sums[:, n : 2 * n] * factor)
    out[...] = jnp.broadcast_to(hidden[None], out.shape).astype(bf16)


def down(hidden, weight, weight_x, out):
    rows = flat(hidden[...]).astype(bf16)
    half = weight.shape[1]
    out[:, :, :half] = blocked(dot(rows, weight[...]), out.shape[0]).astype(bf16)
    out[:, :, half:] = blocked(dot(rows, weight_x[...]), out.shape[0]).astype(bf16)


def last_down(ids, hidden, *refs):
    out = refs[-1]
    core, side = ids[0], ids[2]
    rows = flat(hidden[...]).astype(bf16)
    out[...] = jnp.zeros(out.shape, bf16)
    for i, weight in enumerate(refs[:-1]):
        chip, half = (side, 1 - side)[i // 2], (core, 1 - core)[i % 2]
        out[chip, half, :, side] = blocked(dot(rows, weight[...]), out.shape[2]).astype(bf16)


def add_first(ids, parts, got, out):
    sums = jnp.sum(parts[...].astype(f32), axis=0)
    core, block = ids[0], ids[1]
    own, other = got[core, block].astype(f32), got[1 - core, block].astype(f32)
    rows = jnp.concatenate([own, other], 1) + 0.5 * sums
    out[...] = jnp.broadcast_to(rows[None], out.shape).astype(bf16)


def add_mixer(ids, parts, middle, out, other):
    sums = jnp.sum(parts[...].astype(f32), axis=0)
    rows = (middle[ids[1]].astype(f32) + sums).astype(bf16)
    out[...] = jnp.broadcast_to(rows.astype(f32)[None], out.shape).astype(bf16)
    other[...] = rows[:, rows.shape[1] // 2 :]


def project(ids, middle, gains, gains_x, main, main_x, ws, ws_x, wd, wd_x, out):
    wide = flat(middle[...])
    half = wide.shape[1] // 2
    own, other = wide[:, :half], wide[:, half:]
    scaled, scaled_x = (own * gains[1:2]).astype(bf16), (other * gains_x[1:2]).astype(bf16)
    n, count = main.shape[1], out.shape[0]
    part = dot(scaled, main[...]) + dot(scaled_x, main_x[...])
    out[:, :, :n] = blocked(part, count).astype(bf16)
    heads = ws.shape[0]
    mine = lax.broadcasted_iota(jnp.int32, (wide.shape[0], heads), 1) == ids[1]
    columns = []
    for w, w_x in ((ws, ws_x), (wd, wd_x)):
        logit = dot_t(scaled, w[...]) + dot_t(scaled_x, w_x[...])
        columns.append(jnp.sum(jnp.where(mine, logit, 0.0), -1, keepdims=True))
    columns.append(jnp.sum(own * own + other * other, -1, keepdims=True))
    out[:, :, n:] = blocked(lane_tile(wide.shape[0], columns), count).astype(bf16)


def earlier_state(
    lengths, head, recurrent, keys, values, strength, decay, extra, gain, state, new, gains
):
    count, span = strength.shape
    sequence = lax.broadcasted_iota(jnp.int32, (count, span), 0)
    lane = lax.broadcasted_iota(jnp.int32, (count, span), 1)
    latest = jnp.zeros((count, span), jnp.int32)
    for b in range(count):
        latest = jnp.where(sequence == b, lengths[b] - 1, latest)
    before = lane < latest
    beta = jnp.where(before, jax.nn.sigmoid(strength[...]), 0.0)
    amount = extra[...] - head[0] * softplus(decay[...] + head[1])
    amount = jnp.where(before, amount, 0.0)
    new_extra = jnp.sum(jnp.where(lane == latest, extra[...], 0.0), -1, keepdims=True)
    new[...] = jnp.broadcast_to(new_extra, new.shape)
    gains[...] = jnp.broadcast_to(gain[...], gains.shape)
    row = lax.broadcasted_iota(jnp.int32, (span, span), 0)
    col = lax.broadcasted_iota(jnp.int32, (span, span), 1)
    cumul = exact(amount, (row <= col).astype(f32))
    last = cumul[:, span - 1 : span]
    eye = (row == col).astype(f32)
    stacked = jnp.concatenate(
        [beta, cumul, jnp.exp(cumul), jnp.exp(last - cumul), before.astype(f32)], 0
    )
    upright = exact(eye, stacked, ((1,), (1,)))

    def upright_column(which, b):
        at = which * count + b
        return upright[:, at : at + 1]

    every = range(count)
    ks, couplings = [], []
    for b in every:
        k = keys[b].astype(f32) * upright_column(4, b)
        k = k * lax.rsqrt(jnp.sum(k * k, -1, keepdims=True) + EPS)
        gap = upright_column(1, b) - cumul[b : b + 1]
        gap = jnp.exp(jnp.where(row > col, gap, -jnp.inf))
        ks.append(k)
        couplings.append(upright_column(0, b) * exact(k, k, ((1,), (1,))) * gap)

    def same(size):
        return (row // size) == (col // size)

    first = [jnp.where(same(8), c, 0.0) for c in couplings]
    second = [exact(a, a) for a in first]
    fourth = [exact(a, a) for a in second]
    inverse = [exact(eye - a, eye + b) for a, b in zip(first, second)]
    inverse = [exact(a, eye + b) for a, b in zip(inverse, fourth)]
    size = 8
    while size < span:
        inside = same(2 * size) & ~same(size)
        right = [exact(jnp.where(inside, c, 0.0), a) for c, a in zip(couplings, inverse)]
        inverse = [a - exact(a, r) for a, r in zip(inverse, right)]
        size *= 2
    for b in every:
        carried = exact(ks[b], recurrent[b])
        value = values[b].astype(f32) * upright_column(4, b)
        side = upright_column(0, b) * (value - upright_column(2, b) * carried)
        update = exact(inverse[b], side) * upright_column(3, b)
        kept = jnp.exp(last[b : b + 1]) * recurrent[b]
        state[b] = kept + exact(ks[b], update, ((0,), (0,)))


def new_token(head, parts, state, new_extra, norm_gain, out, *, features):
    sums = jnp.sum(parts[...].astype(f32), axis=0)
    dk = (sums.shape[1] - LANES) // 4
    strength, decay, square = (column_of(sums, 4 * dk, i, 3) for i in range(3))
    factor = lax.rsqrt(square / features + EPS)
    query, key, value, gate = (sums[:, i * dk : (i + 1) * dk] * factor for i in range(4))
    beta = jax.nn.sigmoid(strength * factor)
    amount = new_extra[:, 0:1] - head[0] * softplus(decay * factor + head[1])
    query = query * lax.rsqrt(jnp.sum(query * query, -1, keepdims=True) + EPS) * dk**-0.5
    key = key * lax.rsqrt(jnp.sum(key * key, -1, keepdims=True) + EPS)
    score = jnp.sum(query * key, -1, keepdims=True)
    reduced = jnp.transpose(query - (score * beta) * key)
    sequence = lax.broadcasted_iota(jnp.int32, value.shape, 0)
    read = jnp.zeros(value.shape, f32)
    for b in range(value.shape[0]):
        one = jnp.sum(reduced[:, b : b + 1] * state[b], axis=0, keepdims=True)
        read = jnp.where(sequence == b, one, read)
    rows = jnp.exp(amount) * read + (score * beta) * value
    rows = rows * lax.rsqrt(jnp.mean(rows * rows, -1, keepdims=True) + EPS)
    rows = rows * norm_gain[...] * silu(gate)
    out[...] = jnp.broadcast_to(rows[None], out.shape).astype(bf16)


def finish(ids, parts, got, other, out):
    core, block, side = ids[0], ids[1], ids[2]
    sums = jnp.sum(parts[ids[3]].astype(f32), axis=1)
    mine = got[side, block][:, : sums.shape[-1]].astype(f32)
    theirs = other[...].astype(f32)
    low = jnp.where(core == 0, mine, theirs) + 0.5 * sums[0]
    high = jnp.where(core == 0, theirs, mine) + 0.5 * sums[1]
    out[...] = jnp.concatenate([low, high], 0).astype(bf16)


def exchange(x, axis):
    return lax.all_to_all(x, axis, 0, 0, tiled=True)


def swap(x):
    return lax.ppermute(x, "c", [(0, 1), (1, 0)])


def swap_chips(x):
    return lax.ppermute(x, "za", [(0, 1), (1, 0)])


def together(*trees):
    return lax.optimization_barrier(trees)


def layer(
    tokens,
    first_norm_gain,
    first_gate_weight,
    first_up_weight,
    first_down_weight,
    mixer_norm_gain,
    query_weight_matrix,
    key_weight_matrix,
    value_weight_matrix,
    output_gate_weight,
    strength_weight,
    decay_weight,
    head_decay_speed,
    head_decay_offset,
    head_norm_gain,
    mixer_out_weight,
    second_norm_gain,
    second_gate_weight,
    second_up_weight,
    second_down_weight,
    recurrent,
    earlier_key_cache,
    earlier_value_cache,
    strength_logit_history,
    decay_input_history,
    position_decay_extra,
    lengths,
):
    core, tp, z = lax.axis_index("c"), lax.axis_index("tp"), lax.axis_index(Z)
    side = lax.axis_index("za")
    plane, ring = lax.axis_size("tp"), lax.axis_size(Z)
    count, width = tokens.shape
    rows = count // 2
    features = 2 * ring * width
    hidden_units = first_gate_weight.shape[1]
    dk = query_weight_matrix.shape[1]
    ids = jnp.stack([core, tp, side, tp % 2]).astype(jnp.int32)
    head = jnp.concatenate([head_decay_speed, head_decay_offset])

    blocks = jnp.broadcast_to(tokens.reshape(2, 1, rows, width), (2, plane, rows, width))
    got = exchange(blocks.reshape(2 * plane, rows, width), ("c", "tp"))
    got = got.reshape(2, plane, rows, width)

    gains = jnp.stack([first_norm_gain, mixer_norm_gain, second_norm_gain])
    gate_x = swap(first_gate_weight)
    up_x = swap(first_up_weight)
    gains_x = swap(gains)
    sent = kernel(
        first_products,
        ((ring, rows, 2 * hidden_units + LANES), bf16),
        ids,
        got,
        gains,
        gains_x,
        first_gate_weight,
        gate_x,
        first_up_weight,
        up_x,
        scalars=1,
    )

    sent, later = together(
        sent,
        (
            first_down_weight,
            query_weight_matrix,
            key_weight_matrix,
            value_weight_matrix,
            output_gate_weight,
            strength_weight,
            decay_weight,
            recurrent,
            earlier_key_cache,
            earlier_value_cache,
            strength_logit_history,
            decay_input_history,
            position_decay_extra,
            lengths,
            head_norm_gain,
            mixer_out_weight,
            second_gate_weight,
            second_up_weight,
            second_down_weight,
        ),
    )
    (
        first_down_weight,
        query_weight_matrix,
        key_weight_matrix,
        value_weight_matrix,
        output_gate_weight,
        strength_weight,
        decay_weight,
        recurrent,
        earlier_key_cache,
        earlier_value_cache,
        strength_logit_history,
        decay_input_history,
        position_decay_extra,
        lengths,
        head_norm_gain,
        mixer_out_weight,
        second_gate_weight,
        second_up_weight,
        second_down_weight,
    ) = later
    parts = exchange(sent, Z)
    down_x = swap(first_down_weight)
    main = jnp.concatenate(
        [query_weight_matrix, key_weight_matrix, value_weight_matrix, output_gate_weight], 1
    )
    main_x = swap(main)

    def small(w, which):
        return lax.dynamic_slice_in_dim(w.T, (z * 2 + which) * width, width, 1)

    ws, ws_x = small(strength_weight, core), small(strength_weight, 1 - core)
    wd, wd_x = small(decay_weight, core), small(decay_weight, 1 - core)
    local = lengths.shape[0]
    state, new_extra, norm_gain = kernel(
        earlier_state,
        [
            ((local, dk, recurrent.shape[-1]), f32),
            ((local, LANES), f32),
            ((local, recurrent.shape[-1]), f32),
        ],
        lengths,
        head,
        recurrent[:, 0],
        earlier_key_cache,
        earlier_value_cache,
        strength_logit_history[0],
        decay_input_history[0],
        position_decay_extra[0],
        head_norm_gain[None],
        scalars=2,
        flops=1 << 28,
    )
    parts, down_x, main, main_x, ws, ws_x, wd, wd_x, state, new_extra, norm_gain = together(
        parts, down_x, main, main_x, ws, ws_x, wd, wd_x, state, new_extra, norm_gain
    )

    hidden = kernel(
        activate, ((ring, rows, hidden_units), bf16), parts, features=features
    )
    hidden, later = together(
        hidden, (mixer_out_weight, second_gate_weight, second_up_weight, second_down_weight)
    )
    mixer_out_weight, second_gate_weight, second_up_weight, second_down_weight = later
    hidden = exchange(hidden, Z)
    out_x, gate2_x = swap(mixer_out_weight), swap(second_gate_weight)
    up2_x, down2_x = swap(second_up_weight), swap(second_down_weight)
    hidden, out_x, gate2_x, up2_x, down2_x = together(hidden, out_x, gate2_x, up2_x, down2_x)

    parts = kernel(down, ((plane, rows, 2 * width), bf16), hidden, first_down_weight, down_x)
    parts, gate2, up2, down2 = together(
        parts, second_gate_weight, second_up_weight, second_down_weight
    )
    parts = exchange(parts, "tp")
    gate2_z = swap_chips(gate2)
    up2_z = swap_chips(up2)
    parts, gate2_z, up2_z = together(parts, gate2_z, up2_z)
    middle = kernel(add_first, ((plane, rows, 2 * width), bf16), ids, parts, got, scalars=1)
    middle, down2, both_gains = together(middle, down2, jnp.stack([gains, gains_x]))
    middle = exchange(middle, "tp")
    down2_z = swap_chips(down2)
    gains_z = swap_chips(both_gains)
    middle, down2_z, gains_z = together(middle, down2_z, gains_z)

    parts = kernel(
        project,
        ((ring, rows, 4 * dk + LANES), bf16),
        ids,
        middle,
        gains,
        gains_x,
        main,
        main_x,
        ws,
        ws_x,
        wd,
        wd_x,
        scalars=1,
    )
    parts, gate2_z, up2_z, down2_z = together(parts, gate2_z, up2_z, down2_z)
    parts = exchange(parts, Z)
    gate2_zx, up2_zx, down2_zx = swap(gate2_z), swap(up2_z), swap(down2_z)
    parts, gate2_zx, up2_zx, down2_zx = together(parts, gate2_zx, up2_zx, down2_zx)
    mixed = kernel(
        new_token,
        ((ring, rows, dk), bf16),
        head,
        parts,
        state,
        new_extra,
        norm_gain,
        scalars=1,
        features=features,
    )
    mixed = exchange(mixed, Z)
    parts = kernel(down, ((plane, rows, 2 * width), bf16), mixed, mixer_out_weight, out_x)
    parts = exchange(parts, "tp")
    second, other = kernel(
        add_mixer,
        [((2 * plane, rows, 2 * width), bf16), ((rows, width), bf16)],
        ids,
        parts,
        middle,
        scalars=1,
    )
    second = exchange(second, ("za", "tp"))
    other = swap(other)
    second, other = together(second, other)
    half = ring // 2
    sent = kernel(
        second_products,
        ((half, rows, 2 * hidden_units + LANES), bf16),
        ids,
        second.reshape(2, plane // 2, 2, rows, 2 * width),
        gains,
        gains_x,
        gains_z,
        *(second_gate_weight, gate2_x, gate2_z, gate2_zx),
        *(second_up_weight, up2_x, up2_z, up2_zx),
        scalars=1,
    )
    parts = exchange(sent, "zh")
    hidden = kernel(
        activate, ((half, rows, hidden_units), bf16), parts, features=features
    )
    hidden = exchange(hidden, "zh")
    parts = kernel(
        last_down,
        ((2, 2, plane // 2, 2, rows, width), bf16),
        ids,
        hidden,
        *(second_down_weight, down2_x, down2_z, down2_zx),
        scalars=1,
    )
    parts = exchange(parts.reshape(4 * plane, rows, width), ("za", "c", "tp"))
    return kernel(
        finish,
        ((count, width), bf16),
        ids,
        parts.reshape(2, 2, plane, rows, width),
        second.reshape(2, plane, rows, 2 * width),
        other,
        scalars=1,
    )


def solution(mesh):
    kv, tp = mesh.shape["kv"], mesh.shape["tp"]
    split = Mesh(mesh.devices.reshape(kv // 4, 2, 2, tp), (*Z, "c", "tp"))
    kv = (*Z, "c")
    return jax.shard_map(
        layer,
        mesh=split,
        in_specs=(
            P("tp", kv),
            P(kv),
            P(kv, "tp"),
            P(kv, "tp"),
            P("tp", kv),
            P(kv),
            P(kv, "tp"),
            P(kv, "tp"),
            P(kv, "tp"),
            P(kv, "tp"),
            P(),
            P(),
            P("tp"),
            P("tp"),
            P(),
            P("tp", kv),
            P(kv),
            P(kv, "tp"),
            P(kv, "tp"),
            P("tp", kv),
            P(kv, "tp", None, None),
            P(kv, None, "tp"),
            P(kv, None, "tp"),
            P("tp", kv, None),
            P("tp", kv, None),
            P("tp", kv, None),
            P(kv),
        ),
        out_specs=P("tp", kv),
        check_vma=False,
    )
```

```python
import functools

import jax
import jax.numpy as jnp
from jax import lax
from jax.experimental import pallas as pl
from jax.experimental.pallas import tpu as pltpu
from jax.sharding import Mesh, PartitionSpec as P

HIGHEST = lax.Precision.HIGHEST
f32 = jnp.float32
bf16 = jnp.bfloat16
LANES = 128
Z = ("zh", "za")
EPS = 1e-06


def kernel(fn, out, *args, scalars=0, flops=1 << 20, limit=12 << 20, **static):
    outs = out if isinstance(out, list) else [out]
    smem = pl.BlockSpec(memory_space=pltpu.SMEM)
    vmem = pl.BlockSpec(memory_space=pltpu.VMEM)
    shapes = [jax.ShapeDtypeStruct(s, d) for s, d in outs]
    size = sum(a.size * a.dtype.itemsize for a in args)
    got = pl.pallas_call(
        functools.partial(fn, **static),
        out_shape=shapes,
        in_specs=[smem] * scalars + [vmem] * (len(args) - scalars),
        out_specs=[vmem] * len(outs),
        compiler_params=pltpu.CompilerParams(vmem_limit_bytes=limit),
        cost_estimate=pl.CostEstimate(flops=flops, bytes_accessed=size, transcendentals=0),
    )(*args)
    return got if isinstance(out, list) else got[0]


def dot(x, w):
    return jnp.dot(x, w, preferred_element_type=f32)


def dot_t(x, w):
    return lax.dot_general(x, w, (((1,), (1,)), ((), ())), preferred_element_type=f32)


def exact(x, y, contract=((1,), (0,))):
    return lax.dot_general(
        x, y, (contract, ((), ())), precision=HIGHEST, preferred_element_type=f32
    )


def flat(x):
    x = x.astype(f32)
    return x.reshape(-1, x.shape[-1])


def blocked(x, count):
    return x.reshape(count, -1, x.shape[-1])


def lane_tile(rows, columns):
    lane = lax.broadcasted_iota(jnp.int32, (rows, LANES), 1)
    tile = jnp.zeros((rows, LANES), f32)
    for i, column in enumerate(columns):
        high = column.astype(bf16).astype(f32)
        tile = jnp.where(lane == i, high, tile)
        tile = jnp.where(lane == i + len(columns), column - high, tile)
    return tile


def column_of(sums, start, i, count):
    at = start + i
    return sums[:, at : at + 1] + sums[:, at + count : at + count + 1]


def silu(x):
    return x * jax.nn.sigmoid(x)


def softplus(x):
    return jnp.maximum(x, 0.0) + jnp.log1p(jnp.exp(-jnp.abs(x)))


def gate_up(slots, gates, ups, out):
    n = gates[0].shape[1]
    count = out.shape[0]
    scaled = [(x * gain).astype(bf16) for x, gain in slots]
    for at, weights in ((0, gates), (n, ups)):
        part = sum(dot(x, w[...]) for x, w in zip(scaled, weights))
        out[:, :, at : at + n] = blocked(part, count).astype(bf16)
    square = jnp.sum(sum(x * x for x, _ in slots), -1, keepdims=True)
    out[:, :, 2 * n :] = blocked(lane_tile(square.shape[0], [square]), count).astype(bf16)


def first_products(ids, got, gains, gains_x, gate, gate_x, up, up_x, out):
    core = ids[0]
    slots = [(flat(got[core]), gains[0:1]), (flat(got[1 - core]), gains_x[0:1])]
    gate_up(slots, (gate, gate_x), (up, up_x), out)


def second_products(ids, got, gains, gains_x, gains_z, *refs):
    out = refs[-1]
    side = ids[2]
    slots = []
    for chip, pair in ((side, (gains, gains_x)), (1 - side, (gains_z.at[0], gains_z.at[1]))):
        wide = flat(got[chip, :, side])
        half = wide.shape[1] // 2
        slots += [(wide[:, :half], pair[0][2:3]), (wide[:, half:], pair[1][2:3])]
    gate_up(slots, refs[0:4], refs[4:8], out)


def activate(parts, out, *, features):
    sums = jnp.sum(parts[...].astype(f32), axis=0)
    n = (sums.shape[1] - LANES) // 2
    factor = lax.rsqrt(column_of(sums, 2 * n, 0, 1) / features + EPS)
    hidden = silu(sums[:, :n] * factor) * (sums[:, n : 2 * n] * factor)
    out[...] = jnp.broadcast_to(hidden[None], out.shape).astype(bf16)


def down(hidden, weight, weight_x, out):
    rows = flat(hidden[...]).astype(bf16)
    half = weight.shape[1]
    out[:, :, :half] = blocked(dot(rows, weight[...]), out.shape[0]).astype(bf16)
    out[:, :, half:] = blocked(dot(rows, weight_x[...]), out.shape[0]).astype(bf16)


def last_down(ids, hidden, *refs):
    out = refs[-1]
    core, side = ids[0], ids[2]
    rows = flat(hidden[...]).astype(bf16)
    out[...] = jnp.zeros(out.shape, bf16)
    for i, weight in enumerate(refs[:-1]):
        chip, half = (side, 1 - side)[i // 2], (core, 1 - core)[i % 2]
        out[chip, half, :, side] = blocked(dot(rows, weight[...]), out.shape[2]).astype(bf16)


def add_first(ids, parts, got, out):
    sums = jnp.sum(parts[...].astype(f32), axis=0)
    core, block = ids[0], ids[1]
    own, other = got[core, block].astype(f32), got[1 - core, block].astype(f32)
    rows = jnp.concatenate([own, other], 1) + 0.5 * sums
    out[...] = jnp.broadcast_to(rows[None], out.shape).astype(bf16)


def add_mixer(ids, parts, middle, out, other):
    sums = jnp.sum(parts[...].astype(f32), axis=0)
    rows = (middle[ids[1]].astype(f32) + sums).astype(bf16)
    out[...] = jnp.broadcast_to(rows.astype(f32)[None], out.shape).astype(bf16)
    other[...] = rows[:, rows.shape[1] // 2 :]


def project(ids, middle, gains, gains_x, main, main_x, ws, ws_x, wd, wd_x, out):
    wide = flat(middle[...])
    half = wide.shape[1] // 2
    own, other = wide[:, :half], wide[:, half:]
    scaled, scaled_x = (own * gains[1:2]).astype(bf16), (other * gains_x[1:2]).astype(bf16)
    n, count = main.shape[1], out.shape[0]
    part = dot(scaled, main[...]) + dot(scaled_x, main_x[...])
    out[:, :, :n] = blocked(part, count).astype(bf16)
    heads = ws.shape[0]
    mine = lax.broadcasted_iota(jnp.int32, (wide.shape[0], heads), 1) == ids[1]
    columns = []
    for w, w_x in ((ws, ws_x), (wd, wd_x)):
        logit = dot_t(scaled, w[...]) + dot_t(scaled_x, w_x[...])
        columns.append(jnp.sum(jnp.where(mine, logit, 0.0), -1, keepdims=True))
    columns.append(jnp.sum(own * own + other * other, -1, keepdims=True))
    out[:, :, n:] = blocked(lane_tile(wide.shape[0], columns), count).astype(bf16)


def earlier_state(
    lengths, head, recurrent, keys, values, strength, decay, extra, gain, state, new, gains
):
    count, span = strength.shape
    sequence = lax.broadcasted_iota(jnp.int32, (count, span), 0)
    lane = lax.broadcasted_iota(jnp.int32, (count, span), 1)
    latest = jnp.zeros((count, span), jnp.int32)
    for b in range(count):
        latest = jnp.where(sequence == b, lengths[b] - 1, latest)
    before = lane < latest
    beta = jnp.where(before, jax.nn.sigmoid(strength[...]), 0.0)
    amount = extra[...] - head[0] * softplus(decay[...] + head[1])
    amount = jnp.where(before, amount, 0.0)
    new_extra = jnp.sum(jnp.where(lane == latest, extra[...], 0.0), -1, keepdims=True)
    new[...] = jnp.broadcast_to(new_extra, new.shape)
    gains[...] = jnp.broadcast_to(gain[...], gains.shape)
    row = lax.broadcasted_iota(jnp.int32, (span, span), 0)
    col = lax.broadcasted_iota(jnp.int32, (span, span), 1)
    cumul = exact(amount, (row <= col).astype(f32))
    last = cumul[:, span - 1 : span]
    eye = (row == col).astype(f32)
    stacked = jnp.concatenate(
        [beta, cumul, jnp.exp(cumul), jnp.exp(last - cumul), before.astype(f32)], 0
    )
    upright = exact(eye, stacked, ((1,), (1,)))

    def upright_column(which, b):
        at = which * count + b
        return upright[:, at : at + 1]

    every = range(count)
    ks, couplings = [], []
    for b in every:
        k = keys[b].astype(f32) * upright_column(4, b)
        k = k * lax.rsqrt(jnp.sum(k * k, -1, keepdims=True) + EPS)
        gap = upright_column(1, b) - cumul[b : b + 1]
        gap = jnp.exp(jnp.where(row > col, gap, -jnp.inf))
        ks.append(k)
        couplings.append(upright_column(0, b) * exact(k, k, ((1,), (1,))) * gap)

    def same(size):
        return (row // size) == (col // size)

    first = [jnp.where(same(8), c, 0.0) for c in couplings]
    second = [exact(a, a) for a in first]
    fourth = [exact(a, a) for a in second]
    inverse = [exact(eye - a, eye + b) for a, b in zip(first, second)]
    inverse = [exact(a, eye + b) for a, b in zip(inverse, fourth)]
    size = 8
    while size < span:
        inside = same(2 * size) & ~same(size)
        right = [exact(jnp.where(inside, c, 0.0), a) for c, a in zip(couplings, inverse)]
        inverse = [a - exact(a, r) for a, r in zip(inverse, right)]
        size *= 2
    for b in every:
        carried = exact(ks[b], recurrent[b])
        value = values[b].astype(f32) * upright_column(4, b)
        side = upright_column(0, b) * (value - upright_column(2, b) * carried)
        update = exact(inverse[b], side) * upright_column(3, b)
        kept = jnp.exp(last[b : b + 1]) * recurrent[b]
        state[b] = kept + exact(ks[b], update, ((0,), (0,)))


def new_token(head, parts, state, new_extra, norm_gain, out, *, features):
    sums = jnp.sum(parts[...].astype(f32), axis=0)
    dk = (sums.shape[1] - LANES) // 4
    strength, decay, square = (column_of(sums, 4 * dk, i, 3) for i in range(3))
    factor = lax.rsqrt(square / features + EPS)
    query, key, value, gate = (sums[:, i * dk : (i + 1) * dk] * factor for i in range(4))
    beta = jax.nn.sigmoid(strength * factor)
    amount = new_extra[:, 0:1] - head[0] * softplus(decay * factor + head[1])
    query = query * lax.rsqrt(jnp.sum(query * query, -1, keepdims=True) + EPS) * dk**-0.5
    key = key * lax.rsqrt(jnp.sum(key * key, -1, keepdims=True) + EPS)
    score = jnp.sum(query * key, -1, keepdims=True)
    reduced = jnp.transpose(query - (score * beta) * key)
    sequence = lax.broadcasted_iota(jnp.int32, value.shape, 0)
    read = jnp.zeros(value.shape, f32)
    for b in range(value.shape[0]):
        one = jnp.sum(reduced[:, b : b + 1] * state[b], axis=0, keepdims=True)
        read = jnp.where(sequence == b, one, read)
    rows = jnp.exp(amount) * read + (score * beta) * value
    rows = rows * lax.rsqrt(jnp.mean(rows * rows, -1, keepdims=True) + EPS)
    rows = rows * norm_gain[...] * silu(gate)
    out[...] = jnp.broadcast_to(rows[None], out.shape).astype(bf16)


def finish(ids, parts, got, other, out):
    core, block, side = ids[0], ids[1], ids[2]
    sums = jnp.sum(parts[ids[3]].astype(f32), axis=1)
    mine = got[side, block][:, : sums.shape[-1]].astype(f32)
    theirs = other[...].astype(f32)
    low = jnp.where(core == 0, mine, theirs) + 0.5 * sums[0]
    high = jnp.where(core == 0, theirs, mine) + 0.5 * sums[1]
    out[...] = jnp.concatenate([low, high], 0).astype(bf16)


def exchange(x, axis):
    return lax.all_to_all(x, axis, 0, 0, tiled=True)


def swap(x):
    return lax.ppermute(x, "c", [(0, 1), (1, 0)])


def swap_chips(x):
    return lax.ppermute(x, "za", [(0, 1), (1, 0)])


def together(*trees):
    return lax.optimization_barrier(trees)


def layer(
    tokens,
    first_norm_gain,
    first_gate_weight,
    first_up_weight,
    first_down_weight,
    mixer_norm_gain,
    query_weight_matrix,
    key_weight_matrix,
    value_weight_matrix,
    output_gate_weight,
    strength_weight,
    decay_weight,
    head_decay_speed,
    head_decay_offset,
    head_norm_gain,
    mixer_out_weight,
    second_norm_gain,
    second_gate_weight,
    second_up_weight,
    second_down_weight,
    recurrent,
    earlier_key_cache,
    earlier_value_cache,
    strength_logit_history,
    decay_input_history,
    position_decay_extra,
    lengths,
):
    core, tp, z = lax.axis_index("c"), lax.axis_index("tp"), lax.axis_index(Z)
    side = lax.axis_index("za")
    plane, ring = lax.axis_size("tp"), lax.axis_size(Z)
    count, width = tokens.shape
    rows = count // 2
    features = 2 * ring * width
    hidden_units = first_gate_weight.shape[1]
    dk = query_weight_matrix.shape[1]
    ids = jnp.stack([core, tp, side, tp % 2]).astype(jnp.int32)
    head = jnp.concatenate([head_decay_speed, head_decay_offset])

    blocks = jnp.broadcast_to(tokens.reshape(2, 1, rows, width), (2, plane, rows, width))
    got = exchange(blocks.reshape(2 * plane, rows, width), ("c", "tp"))
    got = got.reshape(2, plane, rows, width)

    gains = jnp.stack([first_norm_gain, mixer_norm_gain, second_norm_gain])
    gate_x = swap(first_gate_weight)
    up_x = swap(first_up_weight)
    gains_x = swap(gains)
    sent = kernel(
        first_products,
        ((ring, rows, 2 * hidden_units + LANES), bf16),
        ids,
        got,
        gains,
        gains_x,
        first_gate_weight,
        gate_x,
        first_up_weight,
        up_x,
        scalars=1,
    )

    both_gains = jnp.stack([gains, gains_x])
    sent, later = together(
        sent,
        (
            first_down_weight,
            query_weight_matrix,
            key_weight_matrix,
            value_weight_matrix,
            output_gate_weight,
            strength_weight,
            decay_weight,
            recurrent,
            earlier_key_cache,
            earlier_value_cache,
            strength_logit_history,
            decay_input_history,
            position_decay_extra,
            lengths,
            head_norm_gain,
            mixer_out_weight,
            second_gate_weight,
            second_up_weight,
            second_down_weight,
        ),
    )
    (
        first_down_weight,
        query_weight_matrix,
        key_weight_matrix,
        value_weight_matrix,
        output_gate_weight,
        strength_weight,
        decay_weight,
        recurrent,
        earlier_key_cache,
        earlier_value_cache,
        strength_logit_history,
        decay_input_history,
        position_decay_extra,
        lengths,
        head_norm_gain,
        mixer_out_weight,
        second_gate_weight,
        second_up_weight,
        second_down_weight,
    ) = later
    parts = exchange(sent, Z)
    down_x = swap(first_down_weight)
    main = jnp.concatenate(
        [query_weight_matrix, key_weight_matrix, value_weight_matrix, output_gate_weight], 1
    )
    main_x = swap(main)

    def small(w, which):
        return lax.dynamic_slice_in_dim(w.T, (z * 2 + which) * width, width, 1)

    ws, ws_x = small(strength_weight, core), small(strength_weight, 1 - core)
    wd, wd_x = small(decay_weight, core), small(decay_weight, 1 - core)
    local = lengths.shape[0]
    state, new_extra, norm_gain = kernel(
        earlier_state,
        [
            ((local, dk, recurrent.shape[-1]), f32),
            ((local, LANES), f32),
            ((local, recurrent.shape[-1]), f32),
        ],
        lengths,
        head,
        recurrent[:, 0],
        earlier_key_cache,
        earlier_value_cache,
        strength_logit_history[0],
        decay_input_history[0],
        position_decay_extra[0],
        head_norm_gain[None],
        scalars=2,
        flops=1 << 28,
    )
    state, gate2, up2, down2 = together(
        state, second_gate_weight, second_up_weight, second_down_weight
    )
    gate2_z = swap_chips(gate2)
    up2_z = swap_chips(up2)
    down2_z = swap_chips(down2)
    parts, down_x, main, main_x, ws, ws_x, wd, wd_x, state, new_extra, norm_gain, both_gains = (
        together(
            parts,
            down_x,
            main,
            main_x,
            ws,
            ws_x,
            wd,
            wd_x,
            state,
            new_extra,
            norm_gain,
            both_gains,
        )
    )

    hidden = kernel(
        activate, ((ring, rows, hidden_units), bf16), parts, features=features
    )
    hidden, later = together(
        hidden, (mixer_out_weight, second_gate_weight, second_up_weight, second_down_weight)
    )
    mixer_out_weight, second_gate_weight, second_up_weight, second_down_weight = later
    hidden = exchange(hidden, Z)
    out_x, gate2_x = swap(mixer_out_weight), swap(second_gate_weight)
    up2_x, down2_x = swap(second_up_weight), swap(second_down_weight)
    hidden, out_x, gate2_x, up2_x, down2_x, gate2_z, up2_z, down2_z = together(
        hidden, out_x, gate2_x, up2_x, down2_x, gate2_z, up2_z, down2_z
    )

    parts = kernel(down, ((plane, rows, 2 * width), bf16), hidden, first_down_weight, down_x)
    parts = exchange(parts, "tp")
    middle = kernel(add_first, ((plane, rows, 2 * width), bf16), ids, parts, got, scalars=1)
    middle = exchange(middle, "tp")

    parts = kernel(
        project,
        ((ring, rows, 4 * dk + LANES), bf16),
        ids,
        middle,
        gains,
        gains_x,
        main,
        main_x,
        ws,
        ws_x,
        wd,
        wd_x,
        scalars=1,
    )
    parts, gate2_z, up2_z, down2_z, both_gains = together(
        parts, gate2_z, up2_z, down2_z, both_gains
    )
    parts = exchange(parts, Z)
    gate2_zx, up2_zx, down2_zx = swap(gate2_z), swap(up2_z), swap(down2_z)
    gains_z = swap_chips(both_gains)
    parts, gate2_zx, up2_zx, down2_zx, gains_z = together(
        parts, gate2_zx, up2_zx, down2_zx, gains_z
    )
    mixed = kernel(
        new_token,
        ((ring, rows, dk), bf16),
        head,
        parts,
        state,
        new_extra,
        norm_gain,
        scalars=1,
        features=features,
    )
    mixed = exchange(mixed, Z)
    parts = kernel(down, ((plane, rows, 2 * width), bf16), mixed, mixer_out_weight, out_x)
    parts = exchange(parts, "tp")
    second, other = kernel(
        add_mixer,
        [((2 * plane, rows, 2 * width), bf16), ((rows, width), bf16)],
        ids,
        parts,
        middle,
        scalars=1,
    )
    second = exchange(second, ("za", "tp"))
    other = swap(other)
    second, other = together(second, other)
    half = ring // 2
    sent = kernel(
        second_products,
        ((half, rows, 2 * hidden_units + LANES), bf16),
        ids,
        second.reshape(2, plane // 2, 2, rows, 2 * width),
        gains,
        gains_x,
        gains_z,
        *(second_gate_weight, gate2_x, gate2_z, gate2_zx),
        *(second_up_weight, up2_x, up2_z, up2_zx),
        scalars=1,
    )
    parts = exchange(sent, "zh")
    hidden = kernel(
        activate, ((half, rows, hidden_units), bf16), parts, features=features
    )
    hidden = exchange(hidden, "zh")
    parts = kernel(
        last_down,
        ((2, 2, plane // 2, 2, rows, width), bf16),
        ids,
        hidden,
        *(second_down_weight, down2_x, down2_z, down2_zx),
        scalars=1,
    )
    parts = exchange(parts.reshape(4 * plane, rows, width), ("za", "c", "tp"))
    return kernel(
        finish,
        ((count, width), bf16),
        ids,
        parts.reshape(2, 2, plane, rows, width),
        second.reshape(2, plane, rows, 2 * width),
        other,
        scalars=1,
    )


def solution(mesh):
    kv, tp = mesh.shape["kv"], mesh.shape["tp"]
    split = Mesh(mesh.devices.reshape(kv // 4, 2, 2, tp), (*Z, "c", "tp"))
    kv = (*Z, "c")
    return jax.shard_map(
        layer,
        mesh=split,
        in_specs=(
            P("tp", kv),
            P(kv),
            P(kv, "tp"),
            P(kv, "tp"),
            P("tp", kv),
            P(kv),
            P(kv, "tp"),
            P(kv, "tp"),
            P(kv, "tp"),
            P(kv, "tp"),
            P(),
            P(),
            P("tp"),
            P("tp"),
            P(),
            P("tp", kv),
            P(kv),
            P(kv, "tp"),
            P(kv, "tp"),
            P("tp", kv),
            P(kv, "tp", None, None),
            P(kv, None, "tp"),
            P(kv, None, "tp"),
            P("tp", kv, None),
            P("tp", kv, None),
            P("tp", kv, None),
            P(kv),
        ),
        out_specs=P("tp", kv),
        check_vma=False,
    )
```

```python
import functools

import jax
import jax.numpy as jnp
from jax import lax
from jax.experimental import pallas as pl
from jax.experimental.pallas import tpu as pltpu
from jax.sharding import Mesh, PartitionSpec as P

HIGHEST = lax.Precision.HIGHEST
f32 = jnp.float32
bf16 = jnp.bfloat16
LANES = 128
Z = ("zh", "za")
EPS = 1e-06


def kernel(fn, out, *args, scalars=0, flops=1 << 20, limit=12 << 20, **static):
    outs = out if isinstance(out, list) else [out]
    smem = pl.BlockSpec(memory_space=pltpu.SMEM)
    vmem = pl.BlockSpec(memory_space=pltpu.VMEM)
    shapes = [jax.ShapeDtypeStruct(s, d) for s, d in outs]
    size = sum(a.size * a.dtype.itemsize for a in args)
    got = pl.pallas_call(
        functools.partial(fn, **static),
        out_shape=shapes,
        in_specs=[smem] * scalars + [vmem] * (len(args) - scalars),
        out_specs=[vmem] * len(outs),
        compiler_params=pltpu.CompilerParams(vmem_limit_bytes=limit),
        cost_estimate=pl.CostEstimate(flops=flops, bytes_accessed=size, transcendentals=0),
    )(*args)
    return got if isinstance(out, list) else got[0]


def dot(x, w):
    return jnp.dot(x, w, preferred_element_type=f32)


def dot_t(x, w):
    return lax.dot_general(x, w, (((1,), (1,)), ((), ())), preferred_element_type=f32)


def exact(x, y, contract=((1,), (0,))):
    return lax.dot_general(
        x, y, (contract, ((), ())), precision=HIGHEST, preferred_element_type=f32
    )


def flat(x):
    x = x.astype(f32)
    return x.reshape(-1, x.shape[-1])


def blocked(x, count):
    return x.reshape(count, -1, x.shape[-1])


def lane_tile(rows, columns):
    lane = lax.broadcasted_iota(jnp.int32, (rows, LANES), 1)
    tile = jnp.zeros((rows, LANES), f32)
    for i, column in enumerate(columns):
        high = column.astype(bf16).astype(f32)
        tile = jnp.where(lane == i, high, tile)
        tile = jnp.where(lane == i + len(columns), column - high, tile)
    return tile


def column_of(sums, start, i, count):
    at = start + i
    return sums[:, at : at + 1] + sums[:, at + count : at + count + 1]


def silu(x):
    return x * jax.nn.sigmoid(x)


def softplus(x):
    return jnp.maximum(x, 0.0) + jnp.log1p(jnp.exp(-jnp.abs(x)))


def pack(gate, up, down, gains, out):
    n = gate.shape[1]
    out[:, :n] = gate[...]
    out[:, n : 2 * n] = up[...]
    for i in range(n // LANES):
        at = 2 * n + i * LANES
        out[:, at : at + LANES] = down[i * LANES : (i + 1) * LANES]
    rest = gains[2:3]
    row = lax.broadcasted_iota(jnp.int32, (out.shape[0], LANES), 0)
    tile = jnp.zeros(row.shape, f32)
    for i in range(3):
        part = rest.astype(bf16).astype(f32)
        tile = jnp.where(row == i, part, tile)
        rest = rest - part
    out[:, 3 * n :] = tile.astype(bf16)


def gate_up(slots, weights, out):
    n = (out.shape[2] - LANES) // 2
    count = out.shape[0]
    scaled = [(x * gain).astype(bf16) for x, gain in slots]
    for i in range(2):
        part = sum(dot(x, w[i]) for x, w in zip(scaled, weights))
        out[:, :, i * n : (i + 1) * n] = blocked(part, count).astype(bf16)
    square = jnp.sum(sum(x * x for x, _ in slots), -1, keepdims=True)
    out[:, :, 2 * n :] = blocked(lane_tile(square.shape[0], [square]), count).astype(bf16)


def first_products(ids, got, gains, gains_x, gate, gate_x, up, up_x, out):
    core = ids[0]
    slots = [(flat(got[core]), gains[0:1]), (flat(got[1 - core]), gains_x[0:1])]
    gate_up(slots, ((gate[...], up[...]), (gate_x[...], up_x[...])), out)


def second_products(ids, got, *refs):
    out = refs[-1]
    side = ids[2]
    n = (out.shape[2] - LANES) // 2
    slots, weights = [], []
    for i, packed in enumerate(refs[:-1]):
        if i % 2 == 0:
            wide = flat(got[(side, 1 - side)[i // 2], :, side])
        half = wide.shape[1] // 2
        gain = packed[0:16, 3 * n :].astype(f32)
        gain = gain[0:1] + gain[1:2] + gain[2:3]
        slots.append((wide[:, i % 2 * half : (i % 2 + 1) * half], gain))
        weights.append((packed[:, :n], packed[:, n : 2 * n]))
    gate_up(slots, weights, out)


def activate(parts, out, *, features):
    sums = jnp.sum(parts[...].astype(f32), axis=0)
    n = (sums.shape[1] - LANES) // 2
    factor = lax.rsqrt(column_of(sums, 2 * n, 0, 1) / features + EPS)
    hidden = silu(sums[:, :n] * factor) * (sums[:, n : 2 * n] * factor)
    out[...] = jnp.broadcast_to(hidden[None], out.shape).astype(bf16)


def down(hidden, weight, weight_x, out):
    rows = flat(hidden[...]).astype(bf16)
    half = weight.shape[1]
    out[:, :, :half] = blocked(dot(rows, weight[...]), out.shape[0]).astype(bf16)
    out[:, :, half:] = blocked(dot(rows, weight_x[...]), out.shape[0]).astype(bf16)


def last_down(ids, hidden, second, *refs):
    out = refs[-1]
    core, side = ids[0], ids[2]
    rows = flat(hidden[...]).astype(bf16)
    n = rows.shape[1]
    for i, packed in enumerate(refs[:-1]):
        chip, half = (side, 1 - side)[i // 2], (core, 1 - core)[i % 2]
        part = sum(
            dot(rows[:, j : j + LANES], packed[:, 2 * n + j : 2 * n + j + LANES])
            for j in range(0, n, LANES)
        )
        out[chip, half, :, side] = blocked(part, out.shape[2]).astype(bf16)
        at = i % 2 * LANES
        out[chip, half, :, 1 - side] = second[chip, :, 1 - side, :, at : at + LANES]


def add_first(ids, parts, got, out):
    sums = jnp.sum(parts[...].astype(f32), axis=0)
    core, block = ids[0], ids[1]
    own, other = got[core, block].astype(f32), got[1 - core, block].astype(f32)
    rows = jnp.concatenate([own, other], 1) + 0.5 * sums
    out[...] = jnp.broadcast_to(rows[None], out.shape).astype(bf16)


def add_mixer(ids, parts, middle, out):
    sums = jnp.sum(parts[...].astype(f32), axis=0)
    rows = middle[ids[1]].astype(f32) + sums
    out[...] = jnp.broadcast_to(rows[None], out.shape).astype(bf16)


def project(ids, middle, gains, gains_x, main, main_x, ws, ws_x, wd, wd_x, out):
    wide = flat(middle[...])
    half = wide.shape[1] // 2
    own, other = wide[:, :half], wide[:, half:]
    scaled, scaled_x = (own * gains[1:2]).astype(bf16), (other * gains_x[1:2]).astype(bf16)
    n, count = main.shape[1], out.shape[0]
    part = dot(scaled, main[...]) + dot(scaled_x, main_x[...])
    out[:, :, :n] = blocked(part, count).astype(bf16)
    heads = ws.shape[0]
    mine = lax.broadcasted_iota(jnp.int32, (wide.shape[0], heads), 1) == ids[1]
    columns = []
    for w, w_x in ((ws, ws_x), (wd, wd_x)):
        logit = dot_t(scaled, w[...]) + dot_t(scaled_x, w_x[...])
        columns.append(jnp.sum(jnp.where(mine, logit, 0.0), -1, keepdims=True))
    columns.append(jnp.sum(own * own + other * other, -1, keepdims=True))
    out[:, :, n:] = blocked(lane_tile(wide.shape[0], columns), count).astype(bf16)


def earlier_state(
    lengths, head, recurrent, keys, values, strength, decay, extra, gain, state, new, gains
):
    count, span = strength.shape
    sequence = lax.broadcasted_iota(jnp.int32, (count, span), 0)
    lane = lax.broadcasted_iota(jnp.int32, (count, span), 1)
    latest = jnp.zeros((count, span), jnp.int32)
    for b in range(count):
        latest = jnp.where(sequence == b, lengths[b] - 1, latest)
    before = lane < latest
    beta = jnp.where(before, jax.nn.sigmoid(strength[...]), 0.0)
    amount = extra[...] - head[0] * softplus(decay[...] + head[1])
    amount = jnp.where(before, amount, 0.0)
    new_extra = jnp.sum(jnp.where(lane == latest, extra[...], 0.0), -1, keepdims=True)
    new[...] = jnp.broadcast_to(new_extra, new.shape)
    gains[...] = jnp.broadcast_to(gain[...], gains.shape)
    row = lax.broadcasted_iota(jnp.int32, (span, span), 0)
    col = lax.broadcasted_iota(jnp.int32, (span, span), 1)
    cumul = exact(amount, (row <= col).astype(f32))
    last = cumul[:, span - 1 : span]
    eye = (row == col).astype(f32)
    stacked = jnp.concatenate(
        [beta, cumul, jnp.exp(cumul), jnp.exp(last - cumul), before.astype(f32)], 0
    )
    upright = exact(eye, stacked, ((1,), (1,)))

    def upright_column(which, b):
        at = which * count + b
        return upright[:, at : at + 1]

    every = range(count)
    ks, couplings = [], []
    for b in every:
        k = keys[b].astype(f32) * upright_column(4, b)
        k = k * lax.rsqrt(jnp.sum(k * k, -1, keepdims=True) + EPS)
        gap = upright_column(1, b) - cumul[b : b + 1]
        gap = jnp.exp(jnp.where(row > col, gap, -jnp.inf))
        ks.append(k)
        couplings.append(upright_column(0, b) * exact(k, k, ((1,), (1,))) * gap)

    def same(size):
        return (row // size) == (col // size)

    first = [jnp.where(same(8), c, 0.0) for c in couplings]
    second = [exact(a, a) for a in first]
    fourth = [exact(a, a) for a in second]
    inverse = [exact(eye - a, eye + b) for a, b in zip(first, second)]
    inverse = [exact(a, eye + b) for a, b in zip(inverse, fourth)]
    size = 8
    while size < span:
        inside = same(2 * size) & ~same(size)
        right = [exact(jnp.where(inside, c, 0.0), a) for c, a in zip(couplings, inverse)]
        inverse = [a - exact(a, r) for a, r in zip(inverse, right)]
        size *= 2
    for b in every:
        carried = exact(ks[b], recurrent[b])
        value = values[b].astype(f32) * upright_column(4, b)
        side = upright_column(0, b) * (value - upright_column(2, b) * carried)
        update = exact(inverse[b], side) * upright_column(3, b)
        kept = jnp.exp(last[b : b + 1]) * recurrent[b]
        state[b] = kept + exact(ks[b], update, ((0,), (0,)))


def new_token(head, parts, state, new_extra, norm_gain, out, *, features):
    sums = jnp.sum(parts[...].astype(f32), axis=0)
    dk = (sums.shape[1] - LANES) // 4
    strength, decay, square = (column_of(sums, 4 * dk, i, 3) for i in range(3))
    factor = lax.rsqrt(square / features + EPS)
    query, key, value, gate = (sums[:, i * dk : (i + 1) * dk] * factor for i in range(4))
    beta = jax.nn.sigmoid(strength * factor)
    amount = new_extra[:, 0:1] - head[0] * softplus(decay * factor + head[1])
    query = query * lax.rsqrt(jnp.sum(query * query, -1, keepdims=True) + EPS) * dk**-0.5
    key = key * lax.rsqrt(jnp.sum(key * key, -1, keepdims=True) + EPS)
    score = jnp.sum(query * key, -1, keepdims=True)
    reduced = jnp.transpose(query - (score * beta) * key)
    sequence = lax.broadcasted_iota(jnp.int32, value.shape, 0)
    read = jnp.zeros(value.shape, f32)
    for b in range(value.shape[0]):
        one = jnp.sum(reduced[:, b : b + 1] * state[b], axis=0, keepdims=True)
        read = jnp.where(sequence == b, one, read)
    rows = jnp.exp(amount) * read + (score * beta) * value
    rows = rows * lax.rsqrt(jnp.mean(rows * rows, -1, keepdims=True) + EPS)
    rows = rows * norm_gain[...] * silu(gate)
    out[...] = jnp.broadcast_to(rows[None], out.shape).astype(bf16)


def finish(ids, parts, out):
    sums = jnp.sum(parts[ids[3]].astype(f32), axis=1)
    rows = [parts[1 - ids[3], c, 0].astype(f32) + 0.5 * sums[c] for c in range(2)]
    out[...] = jnp.concatenate(rows, 0).astype(bf16)


def exchange(x, axis):
    return lax.all_to_all(x, axis, 0, 0, tiled=True)


def swap(x):
    return lax.ppermute(x, "c", [(0, 1), (1, 0)])


def swap_chips(x):
    return lax.ppermute(x, "za", [(0, 1), (1, 0)])


def together(*trees):
    return lax.optimization_barrier(trees)


def layer(
    tokens,
    first_norm_gain,
    first_gate_weight,
    first_up_weight,
    first_down_weight,
    mixer_norm_gain,
    query_weight_matrix,
    key_weight_matrix,
    value_weight_matrix,
    output_gate_weight,
    strength_weight,
    decay_weight,
    head_decay_speed,
    head_decay_offset,
    head_norm_gain,
    mixer_out_weight,
    second_norm_gain,
    second_gate_weight,
    second_up_weight,
    second_down_weight,
    recurrent,
    earlier_key_cache,
    earlier_value_cache,
    strength_logit_history,
    decay_input_history,
    position_decay_extra,
    lengths,
):
    core, tp, z = lax.axis_index("c"), lax.axis_index("tp"), lax.axis_index(Z)
    side = lax.axis_index("za")
    plane, ring = lax.axis_size("tp"), lax.axis_size(Z)
    count, width = tokens.shape
    rows = count // 2
    features = 2 * ring * width
    hidden_units = first_gate_weight.shape[1]
    dk = query_weight_matrix.shape[1]
    ids = jnp.stack([core, tp, side, tp % 2]).astype(jnp.int32)
    head = jnp.concatenate([head_decay_speed, head_decay_offset])

    blocks = jnp.broadcast_to(tokens.reshape(2, 1, rows, width), (2, plane, rows, width))
    got = exchange(blocks.reshape(2 * plane, rows, width), ("c", "tp"))
    got = got.reshape(2, plane, rows, width)

    gains = jnp.stack([first_norm_gain, mixer_norm_gain, second_norm_gain])
    gate_x = swap(first_gate_weight)
    up_x = swap(first_up_weight)
    gains_x = swap(gains)
    sent = kernel(
        first_products,
        ((ring, rows, 2 * hidden_units + LANES), bf16),
        ids,
        got,
        gains,
        gains_x,
        first_gate_weight,
        gate_x,
        first_up_weight,
        up_x,
        scalars=1,
    )

    sent, later = together(
        sent,
        (
            first_down_weight,
            query_weight_matrix,
            key_weight_matrix,
            value_weight_matrix,
            output_gate_weight,
            strength_weight,
            decay_weight,
            recurrent,
            earlier_key_cache,
            earlier_value_cache,
            strength_logit_history,
            decay_input_history,
            position_decay_extra,
            lengths,
            head_norm_gain,
            mixer_out_weight,
            second_gate_weight,
            second_up_weight,
            second_down_weight,
        ),
    )
    (
        first_down_weight,
        query_weight_matrix,
        key_weight_matrix,
        value_weight_matrix,
        output_gate_weight,
        strength_weight,
        decay_weight,
        recurrent,
        earlier_key_cache,
        earlier_value_cache,
        strength_logit_history,
        decay_input_history,
        position_decay_extra,
        lengths,
        head_norm_gain,
        mixer_out_weight,
        second_gate_weight,
        second_up_weight,
        second_down_weight,
    ) = later
    parts = exchange(sent, Z)
    down_x = swap(first_down_weight)
    main = jnp.concatenate(
        [query_weight_matrix, key_weight_matrix, value_weight_matrix, output_gate_weight], 1
    )
    main_x = swap(main)

    def small(w, which):
        return lax.dynamic_slice_in_dim(w.T, (z * 2 + which) * width, width, 1)

    ws, ws_x = small(strength_weight, core), small(strength_weight, 1 - core)
    wd, wd_x = small(decay_weight, core), small(decay_weight, 1 - core)
    local = lengths.shape[0]
    state, new_extra, norm_gain = kernel(
        earlier_state,
        [
            ((local, dk, recurrent.shape[-1]), f32),
            ((local, LANES), f32),
            ((local, recurrent.shape[-1]), f32),
        ],
        lengths,
        head,
        recurrent[:, 0],
        earlier_key_cache,
        earlier_value_cache,
        strength_logit_history[0],
        decay_input_history[0],
        position_decay_extra[0],
        head_norm_gain[None],
        scalars=2,
        flops=1 << 28,
    )
    packed = kernel(
        pack,
        ((width, 3 * hidden_units + LANES), bf16),
        second_gate_weight,
        second_up_weight,
        second_down_weight,
        gains,
    )
    state, packed = together(state, packed)
    packed_z = swap_chips(packed)
    parts, down_x, main, main_x, ws, ws_x, wd, wd_x, state, new_extra, norm_gain, packed = (
        together(
            parts,
            down_x,
            main,
            main_x,
            ws,
            ws_x,
            wd,
            wd_x,
            state,
            new_extra,
            norm_gain,
            packed,
        )
    )

    hidden = kernel(
        activate, ((ring, rows, hidden_units), bf16), parts, features=features
    )
    hidden, mixer_out_weight, packed = together(hidden, mixer_out_weight, packed)
    hidden = exchange(hidden, Z)
    out_x, packed_x = swap(mixer_out_weight), swap(packed)
    packed_zx = swap(packed_z)
    hidden, out_x, packed_x, packed_z, packed_zx = together(
        hidden, out_x, packed_x, packed_z, packed_zx
    )

    parts = kernel(down, ((plane, rows, 2 * width), bf16), hidden, first_down_weight, down_x)
    parts = exchange(parts, "tp")
    middle = kernel(add_first, ((plane, rows, 2 * width), bf16), ids, parts, got, scalars=1)
    middle = exchange(middle, "tp")

    parts = kernel(
        project,
        ((ring, rows, 4 * dk + LANES), bf16),
        ids,
        middle,
        gains,
        gains_x,
        main,
        main_x,
        ws,
        ws_x,
        wd,
        wd_x,
        scalars=1,
    )
    parts = exchange(parts, Z)
    mixed = kernel(
        new_token,
        ((ring, rows, dk), bf16),
        head,
        parts,
        state,
        new_extra,
        norm_gain,
        scalars=1,
        features=features,
    )
    mixed = exchange(mixed, Z)
    parts = kernel(down, ((plane, rows, 2 * width), bf16), mixed, mixer_out_weight, out_x)
    parts = exchange(parts, "tp")
    second = kernel(add_mixer, ((2 * plane, rows, 2 * width), bf16), ids, parts, middle, scalars=1)
    second = exchange(second, ("za", "tp")).reshape(2, plane // 2, 2, rows, 2 * width)
    half = ring // 2
    slots = (packed, packed_x, packed_z, packed_zx)
    sent = kernel(
        second_products,
        ((half, rows, 2 * hidden_units + LANES), bf16),
        ids,
        second,
        *slots,
        scalars=1,
    )
    parts = exchange(sent, "zh")
    hidden = kernel(
        activate, ((half, rows, hidden_units), bf16), parts, features=features
    )
    hidden = exchange(hidden, "zh")
    parts = kernel(
        last_down,
        ((2, 2, plane // 2, 2, rows, width), bf16),
        ids,
        hidden,
        second,
        *slots,
        scalars=1,
    )
    parts = exchange(parts.reshape(4 * plane, rows, width), ("za", "c", "tp"))
    parts = parts.reshape(2, 2, plane, rows, width)
    return kernel(finish, ((count, width), bf16), ids, parts, scalars=1)


def solution(mesh):
    kv, tp = mesh.shape["kv"], mesh.shape["tp"]
    split = Mesh(mesh.devices.reshape(kv // 4, 2, 2, tp), (*Z, "c", "tp"))
    kv = (*Z, "c")
    return jax.shard_map(
        layer,
        mesh=split,
        in_specs=(
            P("tp", kv),
            P(kv),
            P(kv, "tp"),
            P(kv, "tp"),
            P("tp", kv),
            P(kv),
            P(kv, "tp"),
            P(kv, "tp"),
            P(kv, "tp"),
            P(kv, "tp"),
            P(),
            P(),
            P("tp"),
            P("tp"),
            P(),
            P("tp", kv),
            P(kv),
            P(kv, "tp"),
            P(kv, "tp"),
            P("tp", kv),
            P(kv, "tp", None, None),
            P(kv, None, "tp"),
            P(kv, None, "tp"),
            P("tp", kv, None),
            P("tp", kv, None),
            P("tp", kv, None),
            P(kv),
        ),
        out_specs=P("tp", kv),
        check_vma=False,
    )
```

```python
import functools

import jax
import jax.numpy as jnp
from jax import lax
from jax.experimental import pallas as pl
from jax.experimental.pallas import tpu as pltpu
from jax.sharding import Mesh, PartitionSpec as P

HIGHEST = lax.Precision.HIGHEST
f32 = jnp.float32
bf16 = jnp.bfloat16
LANES = 128
Z = ("zh", "za")
EPS = 1e-06


def kernel(fn, out, *args, scalars=0, flops=1 << 20, limit=12 << 20, **static):
    outs = out if isinstance(out, list) else [out]
    smem = pl.BlockSpec(memory_space=pltpu.SMEM)
    vmem = pl.BlockSpec(memory_space=pltpu.VMEM)
    shapes = [jax.ShapeDtypeStruct(s, d) for s, d in outs]
    size = sum(a.size * a.dtype.itemsize for a in args)
    got = pl.pallas_call(
        functools.partial(fn, **static),
        out_shape=shapes,
        in_specs=[smem] * scalars + [vmem] * (len(args) - scalars),
        out_specs=[vmem] * len(outs),
        compiler_params=pltpu.CompilerParams(vmem_limit_bytes=limit),
        cost_estimate=pl.CostEstimate(flops=flops, bytes_accessed=size, transcendentals=0),
    )(*args)
    return got if isinstance(out, list) else got[0]


def dot(x, w):
    return jnp.dot(x, w, preferred_element_type=f32)


def dot_t(x, w):
    return lax.dot_general(x, w, (((1,), (1,)), ((), ())), preferred_element_type=f32)


def exact(x, y, contract=((1,), (0,))):
    return lax.dot_general(
        x, y, (contract, ((), ())), precision=HIGHEST, preferred_element_type=f32
    )


def flat(x):
    x = x.astype(f32)
    return x.reshape(-1, x.shape[-1])


def blocked(x, count):
    return x.reshape(count, -1, x.shape[-1])


def lane_tile(rows, columns):
    lane = lax.broadcasted_iota(jnp.int32, (rows, LANES), 1)
    tile = jnp.zeros((rows, LANES), f32)
    for i, column in enumerate(columns):
        high = column.astype(bf16).astype(f32)
        tile = jnp.where(lane == i, high, tile)
        tile = jnp.where(lane == i + len(columns), column - high, tile)
    return tile


def column_of(sums, start, i, count):
    at = start + i
    return sums[:, at : at + 1] + sums[:, at + count : at + count + 1]


def silu(x):
    return x * jax.nn.sigmoid(x)


def softplus(x):
    return jnp.maximum(x, 0.0) + jnp.log1p(jnp.exp(-jnp.abs(x)))


def spread(tokens, gain, out):
    raw = tokens[...].astype(f32)
    both = jnp.concatenate([raw, raw * gain[...]], 1)
    both = both.reshape(out.shape[0], 1, out.shape[2], out.shape[3])
    out[...] = jnp.broadcast_to(both, out.shape).astype(bf16)


def pack_first(gate, up, out):
    n = gate.shape[1]
    out[:, :n] = gate[...]
    out[:, n:] = up[...]


def pack(gate, up, down, query, key, value, outer, mixer_out, gains, out):
    n = gate.shape[1]
    down = [down[i : i + LANES] for i in range(0, n, LANES)]
    at = 0
    for part in (gate, up, *down, query, key, value, outer, mixer_out):
        out[:, at : at + part.shape[1]] = part[...]
        at += part.shape[1]
    row = lax.broadcasted_iota(jnp.int32, (out.shape[0], LANES), 0)
    tile = jnp.zeros(row.shape, f32)
    for which in range(2):
        rest = gains[which : which + 1]
        for i in range(3):
            part = rest.astype(bf16).astype(f32)
            tile = jnp.where(row == 3 * which + i, part, tile)
            rest = rest - part
    out[:, at:] = tile.astype(bf16)


def packed_gain(packed, which):
    tile = packed[0:16, packed.shape[1] - LANES :].astype(f32)
    at = 3 * which
    return tile[at : at + 1] + tile[at + 1 : at + 2] + tile[at + 2 : at + 3]


def order(ids):
    core, side = ids[0], ids[2]
    return [(chip, half) for chip in (side, 1 - side) for half in (core, 1 - core)]


def gate_up(scaled, weights, square, out):
    n = (out.shape[2] - LANES) // 2
    count = out.shape[0]
    for i in range(2):
        part = sum(dot(x, w[:, i * n : (i + 1) * n]) for x, w in zip(scaled, weights))
        out[:, :, i * n : (i + 1) * n] = blocked(part, count).astype(bf16)
    out[:, :, 2 * n :] = blocked(lane_tile(square.shape[0], [square]), count).astype(bf16)


def row_sum(xs):
    return jnp.sum(sum(x * x for x in xs), -1, keepdims=True)


def first_products(ids, got, weights, weights_x, out):
    core = ids[0]
    wide = [flat(got[core]), flat(got[1 - core])]
    raw = [x[:, :LANES] for x in wide]
    scaled = [x[:, LANES:].astype(bf16) for x in wide]
    gate_up(scaled, (weights, weights_x), row_sum(raw), out)


def slices(ids, wide):
    out = []
    for chip in (ids[2], 1 - ids[2]):
        rows = flat(wide(chip))
        half = rows.shape[1] // 2
        out += [rows[:, :half], rows[:, half:]]
    return out


def second_products(ids, second, *refs):
    out, packs = refs[-1], refs[:-1]
    raw = slices(ids, lambda chip: second[:, chip])
    scaled = [(x * packed_gain(p, 1)).astype(bf16) for x, p in zip(raw, packs)]
    gate_up(scaled, packs, row_sum(raw), out)


def activate(parts, out, *, features):
    sums = jnp.sum(parts[...].astype(f32), axis=0)
    n = (sums.shape[1] - LANES) // 2
    factor = lax.rsqrt(column_of(sums, 2 * n, 0, 1) / features + EPS)
    hidden = silu(sums[:, :n] * factor) * (sums[:, n : 2 * n] * factor)
    out[...] = jnp.broadcast_to(hidden[None], out.shape).astype(bf16)


def first_down(hidden, weight, weight_x, out):
    rows = flat(hidden[...]).astype(bf16)
    half = weight.shape[1]
    out[:, :, :half] = blocked(dot(rows, weight[...]), out.shape[0]).astype(bf16)
    out[:, :, half:] = blocked(dot(rows, weight_x[...]), out.shape[0]).astype(bf16)


def last_down(ids, hidden, second, *refs):
    out = refs[-1]
    side = ids[2]
    rows = flat(hidden[...]).astype(bf16)
    n = rows.shape[1]
    for i, ((chip, half), packed) in enumerate(zip(order(ids), refs[:-1])):
        part = sum(
            dot(rows[:, j : j + LANES], packed[:, 2 * n + j : 2 * n + j + LANES])
            for j in range(0, n, LANES)
        )
        out[chip, half, :, side, :, :LANES] = blocked(part, out.shape[2]).astype(bf16)
        at = i % 2 * LANES
        out[chip, half, :, side, :, LANES:] = second[:, chip, :, at : at + LANES]
        out[chip, half, :, 1 - side] = jnp.zeros((out.shape[2], *out.shape[4:]), bf16)


def mixer_down(ids, mixed, *refs):
    out = refs[-1]
    rows = flat(mixed[...]).astype(bf16)
    for i, ((chip, _), packed) in enumerate(zip(order(ids), refs[:-1])):
        weight = packed[:, packed.shape[1] - 2 * LANES : packed.shape[1] - LANES]
        at = i % 2 * LANES
        out[:, chip, :, at : at + LANES] = blocked(dot(rows, weight), out.shape[0]).astype(bf16)


def add_first(ids, parts, got, out):
    sums = jnp.sum(parts[...].astype(f32), axis=0)
    core, block = ids[0], ids[1]
    own, other = got[core, block].astype(f32), got[1 - core, block].astype(f32)
    rows = jnp.concatenate([own[:, :LANES], other[:, :LANES]], 1) + 0.5 * sums
    out[...] = jnp.broadcast_to(rows[None], out.shape).astype(bf16)


def add_mixer(ids, parts, middle, out):
    sums = jnp.sum(parts[...].astype(f32), axis=0)
    rows = middle[ids[3], ids[4], ids[2]].astype(f32) + sums
    out[...] = jnp.broadcast_to(rows[None], out.shape).astype(bf16)


def project(ids, middle, logits, *refs):
    out, packs = refs[-1], refs[:-1]
    side = ids[2]
    n, count = out.shape[2] - LANES, out.shape[0]
    raw = slices(ids, lambda chip: middle[chip, :, side])
    scaled = [(x * packed_gain(p, 0)).astype(bf16) for x, p in zip(raw, packs)]
    at = packs[0].shape[1] - 2 * LANES - n
    part = sum(dot(x, p[:, at : at + n]) for x, p in zip(scaled, packs))
    out[:, :, :n] = blocked(part, count).astype(bf16)
    heads = logits.shape[2]
    mine = lax.broadcasted_iota(jnp.int32, (part.shape[0], heads), 1) == ids[1]
    columns = []
    for i in range(2):
        logit = sum(
            dot_t(x, logits[i, chip * 2 + half]) for x, (chip, half) in zip(scaled, order(ids))
        )
        columns.append(jnp.sum(jnp.where(mine, logit, 0.0), -1, keepdims=True))
    columns.append(row_sum(raw))
    out[:, :, n:] = blocked(lane_tile(part.shape[0], columns), count).astype(bf16)


def earlier_state(
    lengths, head, recurrent, keys, values, strength, decay, extra, gain, state, new, gains
):
    count, span = strength.shape
    sequence = lax.broadcasted_iota(jnp.int32, (count, span), 0)
    lane = lax.broadcasted_iota(jnp.int32, (count, span), 1)
    latest = jnp.zeros((count, span), jnp.int32)
    for b in range(count):
        latest = jnp.where(sequence == b, lengths[b] - 1, latest)
    before = lane < latest
    beta = jnp.where(before, jax.nn.sigmoid(strength[...]), 0.0)
    amount = extra[...] - head[0] * softplus(decay[...] + head[1])
    amount = jnp.where(before, amount, 0.0)
    new_extra = jnp.sum(jnp.where(lane == latest, extra[...], 0.0), -1, keepdims=True)
    new[...] = jnp.broadcast_to(new_extra, new.shape)
    gains[...] = jnp.broadcast_to(gain[...], gains.shape)
    row = lax.broadcasted_iota(jnp.int32, (span, span), 0)
    col = lax.broadcasted_iota(jnp.int32, (span, span), 1)
    cumul = exact(amount, (row <= col).astype(f32))
    last = cumul[:, span - 1 : span]
    eye = (row == col).astype(f32)
    stacked = jnp.concatenate(
        [beta, cumul, jnp.exp(cumul), jnp.exp(last - cumul), before.astype(f32)], 0
    )
    upright = exact(eye, stacked, ((1,), (1,)))

    def upright_column(which, b):
        at = which * count + b
        return upright[:, at : at + 1]

    every = range(count)
    ks, couplings = [], []
    for b in every:
        k = keys[b].astype(f32) * upright_column(4, b)
        k = k * lax.rsqrt(jnp.sum(k * k, -1, keepdims=True) + EPS)
        gap = upright_column(1, b) - cumul[b : b + 1]
        gap = jnp.exp(jnp.where(row > col, gap, -jnp.inf))
        ks.append(k)
        couplings.append(upright_column(0, b) * exact(k, k, ((1,), (1,))) * gap)

    def same(size):
        return (row // size) == (col // size)

    first = [jnp.where(same(8), c, 0.0) for c in couplings]
    second = [exact(a, a) for a in first]
    fourth = [exact(a, a) for a in second]
    inverse = [exact(eye - a, eye + b) for a, b in zip(first, second)]
    inverse = [exact(a, eye + b) for a, b in zip(inverse, fourth)]
    size = 8
    while size < span:
        inside = same(2 * size) & ~same(size)
        right = [exact(jnp.where(inside, c, 0.0), a) for c, a in zip(couplings, inverse)]
        inverse = [a - exact(a, r) for a, r in zip(inverse, right)]
        size *= 2
    for b in every:
        carried = exact(ks[b], recurrent[b])
        value = values[b].astype(f32) * upright_column(4, b)
        side = upright_column(0, b) * (value - upright_column(2, b) * carried)
        update = exact(inverse[b], side) * upright_column(3, b)
        kept = jnp.exp(last[b : b + 1]) * recurrent[b]
        state[b] = kept + exact(ks[b], update, ((0,), (0,)))


def new_token(head, parts, state, new_extra, norm_gain, out, *, features):
    sums = jnp.sum(parts[...].astype(f32), axis=0)
    dk = (sums.shape[1] - LANES) // 4
    strength, decay, square = (column_of(sums, 4 * dk, i, 3) for i in range(3))
    factor = lax.rsqrt(square / features + EPS)
    query, key, value, gate = (sums[:, i * dk : (i + 1) * dk] * factor for i in range(4))
    beta = jax.nn.sigmoid(strength * factor)
    amount = new_extra[:, 0:1] - head[0] * softplus(decay * factor + head[1])
    query = query * lax.rsqrt(jnp.sum(query * query, -1, keepdims=True) + EPS) * dk**-0.5
    key = key * lax.rsqrt(jnp.sum(key * key, -1, keepdims=True) + EPS)
    score = jnp.sum(query * key, -1, keepdims=True)
    reduced = jnp.transpose(query - (score * beta) * key)
    sequence = lax.broadcasted_iota(jnp.int32, value.shape, 0)
    read = jnp.zeros(value.shape, f32)
    for b in range(value.shape[0]):
        one = jnp.sum(reduced[:, b : b + 1] * state[b], axis=0, keepdims=True)
        read = jnp.where(sequence == b, one, read)
    rows = jnp.exp(amount) * read + (score * beta) * value
    rows = rows * lax.rsqrt(jnp.mean(rows * rows, -1, keepdims=True) + EPS)
    rows = rows * norm_gain[...] * silu(gate)
    out[...] = jnp.broadcast_to(rows[None], out.shape).astype(bf16)


def finish(ids, parts, out):
    side = ids[3]
    sums = jnp.sum(parts[side].astype(f32), axis=1)
    half = out.shape[1]
    rows = []
    for c in range(2):
        rows.append(parts[side, c, 0].astype(f32)[:, half:] + 0.5 * sums[c][:, :half])
    out[...] = jnp.concatenate(rows, 0).astype(bf16)


def exchange(x, axis):
    return lax.all_to_all(x, axis, 0, 0, tiled=True)


def swap(x):
    return lax.ppermute(x, "c", [(0, 1), (1, 0)])


def swap_chips(x):
    return lax.ppermute(x, "za", [(0, 1), (1, 0)])


def together(*trees):
    return lax.optimization_barrier(trees)


def layer(
    tokens,
    first_norm_gain,
    first_gate_weight,
    first_up_weight,
    first_down_weight,
    mixer_norm_gain,
    query_weight_matrix,
    key_weight_matrix,
    value_weight_matrix,
    output_gate_weight,
    strength_weight,
    decay_weight,
    head_decay_speed,
    head_decay_offset,
    head_norm_gain,
    mixer_out_weight,
    second_norm_gain,
    second_gate_weight,
    second_up_weight,
    second_down_weight,
    recurrent,
    earlier_key_cache,
    earlier_value_cache,
    strength_logit_history,
    decay_input_history,
    position_decay_extra,
    lengths,
):
    core, tp, side = lax.axis_index("c"), lax.axis_index("tp"), lax.axis_index("za")
    plane, ring = lax.axis_size("tp"), lax.axis_size(Z)
    count, width = tokens.shape
    rows, half = count // 2, ring // 2
    features = 2 * ring * width
    hidden_units = first_gate_weight.shape[1]
    dk = query_weight_matrix.shape[1]
    ids = jnp.stack([core, tp, side, tp & 1, tp >> 1]).astype(jnp.int32)

    sent = kernel(
        spread, ((2, plane, rows, 2 * width), bf16), tokens, first_norm_gain[None]
    )
    got = exchange(sent.reshape(2 * plane, rows, 2 * width), ("c", "tp"))
    got = got.reshape(2, plane, rows, 2 * width)
    first = kernel(
        pack_first, ((width, 2 * hidden_units), bf16), first_gate_weight, first_up_weight
    )
    first_x = swap(first)
    sent = kernel(
        first_products,
        ((ring, rows, 2 * hidden_units + LANES), bf16),
        ids,
        got,
        first,
        first_x,
        scalars=1,
    )

    sent, later = together(
        sent,
        (
            first_down_weight,
            (second_gate_weight, second_up_weight, second_down_weight),
            (query_weight_matrix, key_weight_matrix, value_weight_matrix, output_gate_weight),
            (mixer_out_weight, mixer_norm_gain, second_norm_gain),
            (strength_weight, decay_weight),
            (head_decay_speed, head_decay_offset),
            (recurrent, earlier_key_cache, earlier_value_cache),
            (strength_logit_history, decay_input_history, position_decay_extra),
            (lengths, head_norm_gain),
        ),
    )
    down, branch, heads, outer, logits, decays, caches, histories, others = later
    parts = exchange(sent, Z)
    down_x = swap(down)
    gains = jnp.stack(outer[1:])
    head = jnp.concatenate(decays)
    lengths, head_norm_gain = others
    local = lengths.shape[0]
    state, new_extra, norm_gain = kernel(
        earlier_state,
        [
            ((local, dk, recurrent.shape[-1]), f32),
            ((local, LANES), f32),
            ((local, recurrent.shape[-1]), f32),
        ],
        lengths,
        head,
        caches[0][:, 0],
        *caches[1:],
        *(h[0] for h in histories),
        head_norm_gain[None],
        scalars=2,
        flops=1 << 28,
    )
    packed = kernel(
        pack,
        ((width, 3 * hidden_units + 4 * dk + width + LANES), bf16),
        *branch,
        *heads,
        outer[0],
        gains,
    )
    state, packed = together(state, packed)
    packed_z = swap_chips(packed)
    start = lax.axis_index("zh") * 4 * width
    logits = [lax.dynamic_slice_in_dim(w.T, start, 4 * width, 1) for w in logits]
    logits = jnp.stack(logits).reshape(2, -1, 4, width).transpose(0, 2, 1, 3)
    parts, down_x, logits, state, new_extra, norm_gain, packed = together(
        parts, down_x, logits, state, new_extra, norm_gain, packed
    )

    hidden = kernel(activate, ((ring, rows, hidden_units), bf16), parts, features=features)
    hidden, packed = together(hidden, packed)
    hidden = exchange(hidden, Z)
    packed_x = swap(packed)
    packed_zx = swap(packed_z)
    hidden, packed_x, packed_z, packed_zx = together(hidden, packed_x, packed_z, packed_zx)
    packs = (packed, packed_x, packed_z, packed_zx)

    parts = kernel(first_down, ((plane, rows, 2 * width), bf16), hidden, down, down_x)
    parts = exchange(parts, "tp")
    middle = kernel(add_first, ((2 * plane, rows, 2 * width), bf16), ids, parts, got, scalars=1)
    middle = exchange(middle, ("za", "tp")).reshape(2, plane // 2, 2, rows, 2 * width)

    parts = kernel(
        project,
        ((half, rows, 4 * dk + LANES), bf16),
        ids,
        middle,
        logits,
        *packs,
        scalars=1,
    )
    parts = exchange(parts, "zh")
    mixed = kernel(
        new_token,
        ((half, rows, dk), bf16),
        head,
        parts,
        state,
        new_extra,
        norm_gain,
        scalars=1,
        features=features,
    )
    mixed = exchange(mixed, "zh")
    parts = kernel(
        mixer_down, ((plane // 2, 2, rows, 2 * width), bf16), ids, mixed, *packs, scalars=1
    )
    parts = exchange(parts.reshape(plane, rows, 2 * width), "tp")
    second = kernel(add_mixer, ((plane, rows, 2 * width), bf16), ids, parts, middle, scalars=1)
    second = exchange(second, "tp").reshape(plane // 2, 2, rows, 2 * width)

    sent = kernel(
        second_products,
        ((half, rows, 2 * hidden_units + LANES), bf16),
        ids,
        second,
        *packs,
        scalars=1,
    )
    parts = exchange(sent, "zh")
    hidden = kernel(activate, ((half, rows, hidden_units), bf16), parts, features=features)
    hidden = exchange(hidden, "zh")
    parts = kernel(
        last_down,
        ((2, 2, plane // 2, 2, rows, 2 * width), bf16),
        ids,
        hidden,
        second,
        *packs,
        scalars=1,
    )
    parts = exchange(parts.reshape(4 * plane, rows, 2 * width), ("za", "c", "tp"))
    parts = parts.reshape(2, 2, plane, rows, 2 * width)
    return kernel(finish, ((count, width), bf16), ids, parts, scalars=1)


def solution(mesh):
    kv, tp = mesh.shape["kv"], mesh.shape["tp"]
    split = Mesh(mesh.devices.reshape(kv // 4, 2, 2, tp), (*Z, "c", "tp"))
    kv = (*Z, "c")
    return jax.shard_map(
        layer,
        mesh=split,
        in_specs=(
            P("tp", kv),
            P(kv),
            P(kv, "tp"),
            P(kv, "tp"),
            P("tp", kv),
            P(kv),
            P(kv, "tp"),
            P(kv, "tp"),
            P(kv, "tp"),
            P(kv, "tp"),
            P(),
            P(),
            P("tp"),
            P("tp"),
            P(),
            P("tp", kv),
            P(kv),
            P(kv, "tp"),
            P(kv, "tp"),
            P("tp", kv),
            P(kv, "tp", None, None),
            P(kv, None, "tp"),
            P(kv, None, "tp"),
            P("tp", kv, None),
            P("tp", kv, None),
            P("tp", kv, None),
            P(kv),
        ),
        out_specs=P("tp", kv),
        check_vma=False,
    )
```

```python
import functools

import jax
import jax.numpy as jnp
from jax import lax
from jax.experimental import pallas as pl
from jax.experimental.pallas import tpu as pltpu
from jax.sharding import Mesh, PartitionSpec as P

HIGHEST = lax.Precision.HIGHEST
f32 = jnp.float32
bf16 = jnp.bfloat16
LANES = 128
Z = ("zh", "za")
EPS = 1e-06


def kernel(fn, out, *args, scalars=0, flops=1 << 20, limit=12 << 20, **static):
    outs = out if isinstance(out, list) else [out]
    smem = pl.BlockSpec(memory_space=pltpu.SMEM)
    vmem = pl.BlockSpec(memory_space=pltpu.VMEM)
    shapes = [jax.ShapeDtypeStruct(s, d) for s, d in outs]
    size = sum(a.size * a.dtype.itemsize for a in args)
    got = pl.pallas_call(
        functools.partial(fn, **static),
        out_shape=shapes,
        in_specs=[smem] * scalars + [vmem] * (len(args) - scalars),
        out_specs=[vmem] * len(outs),
        compiler_params=pltpu.CompilerParams(vmem_limit_bytes=limit),
        cost_estimate=pl.CostEstimate(flops=flops, bytes_accessed=size, transcendentals=0),
    )(*args)
    return got if isinstance(out, list) else got[0]


def dot(x, w):
    return jnp.dot(x, w, preferred_element_type=f32)


def dot_t(x, w):
    return lax.dot_general(x, w, (((1,), (1,)), ((), ())), preferred_element_type=f32)


def exact(x, y, contract=((1,), (0,))):
    return lax.dot_general(
        x, y, (contract, ((), ())), precision=HIGHEST, preferred_element_type=f32
    )


def flat(x):
    x = x.astype(f32)
    return x.reshape(-1, x.shape[-1])


def blocked(x, count):
    return x.reshape(count, -1, x.shape[-1])


def lane_tile(rows, columns):
    lane = lax.broadcasted_iota(jnp.int32, (rows, LANES), 1)
    tile = jnp.zeros((rows, LANES), f32)
    for i, column in enumerate(columns):
        high = column.astype(bf16).astype(f32)
        tile = jnp.where(lane == i, high, tile)
        tile = jnp.where(lane == i + len(columns), column - high, tile)
    return tile


def column_of(sums, start, i, count):
    at = start + i
    return sums[:, at : at + 1] + sums[:, at + count : at + count + 1]


def silu(x):
    return x * jax.nn.sigmoid(x)


def softplus(x):
    return jnp.maximum(x, 0.0) + jnp.log1p(jnp.exp(-jnp.abs(x)))


def spread(tokens, gain, out):
    raw = tokens[...].astype(f32)
    both = jnp.concatenate([raw, raw * gain[...]], 1)
    both = both.reshape(out.shape[0], 1, out.shape[2], out.shape[3])
    out[...] = jnp.broadcast_to(both, out.shape).astype(bf16)


def pack_first(gate, up, out):
    n = gate.shape[1]
    out[:, :n] = gate[...]
    out[:, n:] = up[...]


def pack(gate, up, down, first, query, key, value, outer, mixer_out, gains, out):
    n = gate.shape[1]
    down = [w[i : i + LANES] for w in (down, first) for i in range(0, n, LANES)]
    at = 0
    for part in (gate, up, *down, query, key, value, outer, mixer_out):
        out[:, at : at + part.shape[1]] = part[...]
        at += part.shape[1]
    row = lax.broadcasted_iota(jnp.int32, (out.shape[0], LANES), 0)
    tile = jnp.zeros(row.shape, f32)
    for which in range(2):
        rest = gains[which : which + 1]
        for i in range(3):
            part = rest.astype(bf16).astype(f32)
            tile = jnp.where(row == 3 * which + i, part, tile)
            rest = rest - part
    out[:, at:] = tile.astype(bf16)


def packed_gain(packed, which):
    tile = packed[0:16, packed.shape[1] - LANES :].astype(f32)
    at = 3 * which
    return tile[at : at + 1] + tile[at + 1 : at + 2] + tile[at + 2 : at + 3]


def order(ids):
    core, side = ids[0], ids[2]
    return [(chip, half) for chip in (side, 1 - side) for half in (core, 1 - core)]


def gate_up(scaled, weights, square, out):
    n = (out.shape[2] - LANES) // 2
    count = out.shape[0]
    for i in range(2):
        part = sum(dot(x, w[:, i * n : (i + 1) * n]) for x, w in zip(scaled, weights))
        out[:, :, i * n : (i + 1) * n] = blocked(part, count).astype(bf16)
    out[:, :, 2 * n :] = blocked(lane_tile(square.shape[0], [square]), count).astype(bf16)


def row_sum(xs):
    return jnp.sum(sum(x * x for x in xs), -1, keepdims=True)


def first_products(ids, got, weights, weights_x, out):
    core = ids[0]
    wide = [flat(got[core]), flat(got[1 - core])]
    raw = [x[:, :LANES] for x in wide]
    scaled = [x[:, LANES:].astype(bf16) for x in wide]
    gate_up(scaled, (weights, weights_x), row_sum(raw), out)


def slices(ids, wide):
    out = []
    for chip in (ids[2], 1 - ids[2]):
        rows = flat(wide(chip))
        half = rows.shape[1] // 2
        out += [rows[:, :half], rows[:, half:]]
    return out


def second_products(ids, second, *refs):
    out, packs = refs[-1], refs[:-1]
    raw = slices(ids, lambda chip: second[:, chip])
    scaled = [(x * packed_gain(p, 1)).astype(bf16) for x, p in zip(raw, packs)]
    gate_up(scaled, packs, row_sum(raw), out)


def activate(parts, out, *, features):
    sums = jnp.sum(parts[...].astype(f32), axis=0)
    n = (sums.shape[1] - LANES) // 2
    factor = lax.rsqrt(column_of(sums, 2 * n, 0, 1) / features + EPS)
    hidden = silu(sums[:, :n] * factor) * (sums[:, n : 2 * n] * factor)
    out[...] = jnp.broadcast_to(hidden[None], out.shape).astype(bf16)


def down_product(rows, packed, at):
    n = rows.shape[1]
    return sum(
        dot(rows[:, j : j + LANES], packed[:, at + j : at + j + LANES])
        for j in range(0, n, LANES)
    )


def first_down(ids, hidden, *refs):
    out = refs[-1]
    rows = flat(hidden[...]).astype(bf16)
    for i, ((chip, _), packed) in enumerate(zip(order(ids), refs[:-1])):
        at = i % 2 * LANES
        part = down_product(rows, packed, 3 * rows.shape[1])
        out[:, chip, :, at : at + LANES] = blocked(part, out.shape[0]).astype(bf16)


def last_down(ids, hidden, second, *refs):
    out = refs[-1]
    side = ids[2]
    rows = flat(hidden[...]).astype(bf16)
    n = rows.shape[1]
    for i, ((chip, half), packed) in enumerate(zip(order(ids), refs[:-1])):
        part = down_product(rows, packed, 2 * n)
        out[chip, half, :, side, :, :LANES] = blocked(part, out.shape[2]).astype(bf16)
        at = i % 2 * LANES
        out[chip, half, :, side, :, LANES:] = second[:, chip, :, at : at + LANES]
        out[chip, half, :, 1 - side] = jnp.zeros((out.shape[2], *out.shape[4:]), bf16)


def mixer_down(ids, mixed, *refs):
    out = refs[-1]
    rows = flat(mixed[...]).astype(bf16)
    for i, ((chip, _), packed) in enumerate(zip(order(ids), refs[:-1])):
        weight = packed[:, packed.shape[1] - 2 * LANES : packed.shape[1] - LANES]
        at = i % 2 * LANES
        out[:, chip, :, at : at + LANES] = blocked(dot(rows, weight), out.shape[0]).astype(bf16)


def add_first(ids, parts, got, got_z, out):
    sums = jnp.sum(parts[...].astype(f32), axis=0)
    core, side, chip = ids[0], ids[2], ids[3]
    block = 2 * ids[4] + side
    halves = []
    for c in (core, 1 - core):
        mine, theirs = got[c, block].astype(f32), got_z[c, block].astype(f32)
        halves.append(jnp.where(chip == side, mine, theirs)[:, :LANES])
    rows = jnp.concatenate(halves, 1) + 0.5 * sums
    out[...] = jnp.broadcast_to(rows[None], out.shape).astype(bf16)


def add_mixer(ids, parts, middle, out):
    sums = jnp.sum(parts[...].astype(f32), axis=0)
    rows = middle[ids[4], ids[3]].astype(f32) + sums
    out[...] = jnp.broadcast_to(rows[None], out.shape).astype(bf16)


def project(ids, middle, logits, *refs):
    out, packs = refs[-1], refs[:-1]
    n, count = out.shape[2] - LANES, out.shape[0]
    raw = slices(ids, lambda chip: middle[:, chip])
    scaled = [(x * packed_gain(p, 0)).astype(bf16) for x, p in zip(raw, packs)]
    at = packs[0].shape[1] - 2 * LANES - n
    part = sum(dot(x, p[:, at : at + n]) for x, p in zip(scaled, packs))
    out[:, :, :n] = blocked(part, count).astype(bf16)
    heads = logits.shape[2]
    mine = lax.broadcasted_iota(jnp.int32, (part.shape[0], heads), 1) == ids[1]
    columns = []
    for i in range(2):
        logit = sum(
            dot_t(x, logits[i, chip * 2 + half]) for x, (chip, half) in zip(scaled, order(ids))
        )
        columns.append(jnp.sum(jnp.where(mine, logit, 0.0), -1, keepdims=True))
    columns.append(row_sum(raw))
    out[:, :, n:] = blocked(lane_tile(part.shape[0], columns), count).astype(bf16)


def earlier_state(
    lengths, head, recurrent, keys, values, strength, decay, extra, gain, state, new, gains
):
    count, span = strength.shape
    sequence = lax.broadcasted_iota(jnp.int32, (count, span), 0)
    lane = lax.broadcasted_iota(jnp.int32, (count, span), 1)
    latest = jnp.zeros((count, span), jnp.int32)
    for b in range(count):
        latest = jnp.where(sequence == b, lengths[b] - 1, latest)
    before = lane < latest
    beta = jnp.where(before, jax.nn.sigmoid(strength[...]), 0.0)
    amount = extra[...] - head[0] * softplus(decay[...] + head[1])
    amount = jnp.where(before, amount, 0.0)
    new_extra = jnp.sum(jnp.where(lane == latest, extra[...], 0.0), -1, keepdims=True)
    new[...] = jnp.broadcast_to(new_extra, new.shape)
    gains[...] = jnp.broadcast_to(gain[...], gains.shape)
    row = lax.broadcasted_iota(jnp.int32, (span, span), 0)
    col = lax.broadcasted_iota(jnp.int32, (span, span), 1)
    cumul = exact(amount, (row <= col).astype(f32))
    last = cumul[:, span - 1 : span]
    eye = (row == col).astype(f32)
    stacked = jnp.concatenate(
        [beta, cumul, jnp.exp(cumul), jnp.exp(last - cumul), before.astype(f32)], 0
    )
    upright = exact(eye, stacked, ((1,), (1,)))

    def upright_column(which, b):
        at = which * count + b
        return upright[:, at : at + 1]

    every = range(count)
    ks, couplings = [], []
    for b in every:
        k = keys[b].astype(f32) * upright_column(4, b)
        k = k * lax.rsqrt(jnp.sum(k * k, -1, keepdims=True) + EPS)
        gap = upright_column(1, b) - cumul[b : b + 1]
        gap = jnp.exp(jnp.where(row > col, gap, -jnp.inf))
        ks.append(k)
        couplings.append(upright_column(0, b) * exact(k, k, ((1,), (1,))) * gap)

    def same(size):
        return (row // size) == (col // size)

    first = [jnp.where(same(8), c, 0.0) for c in couplings]
    second = [exact(a, a) for a in first]
    fourth = [exact(a, a) for a in second]
    inverse = [exact(eye - a, eye + b) for a, b in zip(first, second)]
    inverse = [exact(a, eye + b) for a, b in zip(inverse, fourth)]
    size = 8
    while size < span:
        inside = same(2 * size) & ~same(size)
        right = [exact(jnp.where(inside, c, 0.0), a) for c, a in zip(couplings, inverse)]
        inverse = [a - exact(a, r) for a, r in zip(inverse, right)]
        size *= 2
    for b in every:
        carried = exact(ks[b], recurrent[b])
        value = values[b].astype(f32) * upright_column(4, b)
        side = upright_column(0, b) * (value - upright_column(2, b) * carried)
        update = exact(inverse[b], side) * upright_column(3, b)
        kept = jnp.exp(last[b : b + 1]) * recurrent[b]
        state[b] = kept + exact(ks[b], update, ((0,), (0,)))


def new_token(head, parts, state, new_extra, norm_gain, out, *, features):
    sums = jnp.sum(parts[...].astype(f32), axis=0)
    dk = (sums.shape[1] - LANES) // 4
    strength, decay, square = (column_of(sums, 4 * dk, i, 3) for i in range(3))
    factor = lax.rsqrt(square / features + EPS)
    query, key, value, gate = (sums[:, i * dk : (i + 1) * dk] * factor for i in range(4))
    beta = jax.nn.sigmoid(strength * factor)
    amount = new_extra[:, 0:1] - head[0] * softplus(decay * factor + head[1])
    query = query * lax.rsqrt(jnp.sum(query * query, -1, keepdims=True) + EPS) * dk**-0.5
    key = key * lax.rsqrt(jnp.sum(key * key, -1, keepdims=True) + EPS)
    score = jnp.sum(query * key, -1, keepdims=True)
    reduced = jnp.transpose(query - (score * beta) * key)
    sequence = lax.broadcasted_iota(jnp.int32, value.shape, 0)
    read = jnp.zeros(value.shape, f32)
    for b in range(value.shape[0]):
        one = jnp.sum(reduced[:, b : b + 1] * state[b], axis=0, keepdims=True)
        read = jnp.where(sequence == b, one, read)
    rows = jnp.exp(amount) * read + (score * beta) * value
    rows = rows * lax.rsqrt(jnp.mean(rows * rows, -1, keepdims=True) + EPS)
    rows = rows * norm_gain[...] * silu(gate)
    out[...] = jnp.broadcast_to(rows[None], out.shape).astype(bf16)


def finish(ids, parts, out):
    side = ids[3]
    sums = jnp.sum(parts[side].astype(f32), axis=1)
    half = out.shape[1]
    rows = []
    for c in range(2):
        rows.append(parts[side, c, 0].astype(f32)[:, half:] + 0.5 * sums[c][:, :half])
    out[...] = jnp.concatenate(rows, 0).astype(bf16)


def exchange(x, axis):
    return lax.all_to_all(x, axis, 0, 0, tiled=True)


def swap(x):
    return lax.ppermute(x, "c", [(0, 1), (1, 0)])


def swap_chips(x):
    return lax.ppermute(x, "za", [(0, 1), (1, 0)])


def together(*trees):
    return lax.optimization_barrier(trees)


def layer(
    tokens,
    first_norm_gain,
    first_gate_weight,
    first_up_weight,
    first_down_weight,
    mixer_norm_gain,
    query_weight_matrix,
    key_weight_matrix,
    value_weight_matrix,
    output_gate_weight,
    strength_weight,
    decay_weight,
    head_decay_speed,
    head_decay_offset,
    head_norm_gain,
    mixer_out_weight,
    second_norm_gain,
    second_gate_weight,
    second_up_weight,
    second_down_weight,
    recurrent,
    earlier_key_cache,
    earlier_value_cache,
    strength_logit_history,
    decay_input_history,
    position_decay_extra,
    lengths,
):
    core, tp, side = lax.axis_index("c"), lax.axis_index("tp"), lax.axis_index("za")
    plane, ring = lax.axis_size("tp"), lax.axis_size(Z)
    count, width = tokens.shape
    rows, half = count // 2, ring // 2
    features = 2 * ring * width
    hidden_units = first_gate_weight.shape[1]
    dk = query_weight_matrix.shape[1]
    ids = jnp.stack([core, tp, side, tp & 1, tp >> 1]).astype(jnp.int32)

    sent = kernel(
        spread, ((2, plane, rows, 2 * width), bf16), tokens, first_norm_gain[None]
    )
    got = exchange(sent.reshape(2 * plane, rows, 2 * width), ("c", "tp"))
    got = got.reshape(2, plane, rows, 2 * width)
    first = kernel(
        pack_first, ((width, 2 * hidden_units), bf16), first_gate_weight, first_up_weight
    )
    first_x = swap(first)
    sent = kernel(
        first_products,
        ((ring, rows, 2 * hidden_units + LANES), bf16),
        ids,
        got,
        first,
        first_x,
        scalars=1,
    )

    sent, later = together(
        sent,
        (
            first_down_weight,
            (second_gate_weight, second_up_weight, second_down_weight),
            (query_weight_matrix, key_weight_matrix, value_weight_matrix, output_gate_weight),
            (mixer_out_weight, mixer_norm_gain, second_norm_gain),
            (strength_weight, decay_weight),
            (head_decay_speed, head_decay_offset),
            (recurrent, earlier_key_cache, earlier_value_cache),
            (strength_logit_history, decay_input_history, position_decay_extra),
            (lengths, head_norm_gain),
        ),
    )
    down, branch, heads, outer, logits, decays, caches, histories, others = later
    parts = exchange(sent, Z)
    gains = jnp.stack(outer[1:])
    head = jnp.concatenate(decays)
    lengths, head_norm_gain = others
    local = lengths.shape[0]
    state, new_extra, norm_gain = kernel(
        earlier_state,
        [
            ((local, dk, recurrent.shape[-1]), f32),
            ((local, LANES), f32),
            ((local, recurrent.shape[-1]), f32),
        ],
        lengths,
        head,
        caches[0][:, 0],
        *caches[1:],
        *(h[0] for h in histories),
        head_norm_gain[None],
        scalars=2,
        flops=1 << 28,
    )
    packed = kernel(
        pack,
        ((width, 4 * hidden_units + 4 * dk + width + LANES), bf16),
        *branch,
        down,
        *heads,
        outer[0],
        gains,
    )
    state, packed = together(state, packed)
    packed_z = swap_chips(packed)
    got_z = swap_chips(got)
    start = lax.axis_index("zh") * 4 * width
    logits = [lax.dynamic_slice_in_dim(w.T, start, 4 * width, 1) for w in logits]
    logits = jnp.stack(logits).reshape(2, -1, 4, width).transpose(0, 2, 1, 3)
    parts, logits, state, new_extra, norm_gain, packed = together(
        parts, logits, state, new_extra, norm_gain, packed
    )

    hidden = kernel(activate, ((half, rows, hidden_units), bf16), parts, features=features)
    hidden, packed = together(hidden, packed)
    hidden = exchange(hidden, "zh")
    packed_x = swap(packed)
    packed_zx = swap(packed_z)
    hidden, packed_x, packed_z, packed_zx, got_z = together(
        hidden, packed_x, packed_z, packed_zx, got_z
    )
    packs = (packed, packed_x, packed_z, packed_zx)

    parts = kernel(
        first_down, ((plane // 2, 2, rows, 2 * width), bf16), ids, hidden, *packs, scalars=1
    )
    parts = exchange(parts.reshape(plane, rows, 2 * width), "tp")
    middle = kernel(
        add_first, ((plane, rows, 2 * width), bf16), ids, parts, got, got_z, scalars=1
    )
    middle = exchange(middle, "tp").reshape(plane // 2, 2, rows, 2 * width)

    parts = kernel(
        project,
        ((half, rows, 4 * dk + LANES), bf16),
        ids,
        middle,
        logits,
        *packs,
        scalars=1,
    )
    parts = exchange(parts, "zh")
    mixed = kernel(
        new_token,
        ((half, rows, dk), bf16),
        head,
        parts,
        state,
        new_extra,
        norm_gain,
        scalars=1,
        features=features,
    )
    mixed = exchange(mixed, "zh")
    parts = kernel(
        mixer_down, ((plane // 2, 2, rows, 2 * width), bf16), ids, mixed, *packs, scalars=1
    )
    parts = exchange(parts.reshape(plane, rows, 2 * width), "tp")
    second = kernel(add_mixer, ((plane, rows, 2 * width), bf16), ids, parts, middle, scalars=1)
    second = exchange(second, "tp").reshape(plane // 2, 2, rows, 2 * width)

    sent = kernel(
        second_products,
        ((half, rows, 2 * hidden_units + LANES), bf16),
        ids,
        second,
        *packs,
        scalars=1,
    )
    parts = exchange(sent, "zh")
    hidden = kernel(activate, ((half, rows, hidden_units), bf16), parts, features=features)
    hidden = exchange(hidden, "zh")
    parts = kernel(
        last_down,
        ((2, 2, plane // 2, 2, rows, 2 * width), bf16),
        ids,
        hidden,
        second,
        *packs,
        scalars=1,
    )
    parts = exchange(parts.reshape(4 * plane, rows, 2 * width), ("za", "c", "tp"))
    parts = parts.reshape(2, 2, plane, rows, 2 * width)
    return kernel(finish, ((count, width), bf16), ids, parts, scalars=1)


def solution(mesh):
    kv, tp = mesh.shape["kv"], mesh.shape["tp"]
    split = Mesh(mesh.devices.reshape(kv // 4, 2, 2, tp), (*Z, "c", "tp"))
    kv = (*Z, "c")
    return jax.shard_map(
        layer,
        mesh=split,
        in_specs=(
            P("tp", kv),
            P(kv),
            P(kv, "tp"),
            P(kv, "tp"),
            P("tp", kv),
            P(kv),
            P(kv, "tp"),
            P(kv, "tp"),
            P(kv, "tp"),
            P(kv, "tp"),
            P(),
            P(),
            P("tp"),
            P("tp"),
            P(),
            P("tp", kv),
            P(kv),
            P(kv, "tp"),
            P(kv, "tp"),
            P("tp", kv),
            P(kv, "tp", None, None),
            P(kv, None, "tp"),
            P(kv, None, "tp"),
            P("tp", kv, None),
            P("tp", kv, None),
            P("tp", kv, None),
            P(kv),
        ),
        out_specs=P("tp", kv),
        check_vma=False,
    )
```

```python
import functools

import jax
import jax.numpy as jnp
from jax import lax
from jax.experimental import pallas as pl
from jax.experimental.pallas import tpu as pltpu
from jax.sharding import Mesh, PartitionSpec as P

HIGHEST = lax.Precision.HIGHEST
f32 = jnp.float32
bf16 = jnp.bfloat16
LANES = 128
Z = ("zh", "za")
EPS = 1e-06


def kernel(fn, out, *args, scalars=0, flops=1 << 20, limit=12 << 20, **static):
    outs = out if isinstance(out, list) else [out]
    smem = pl.BlockSpec(memory_space=pltpu.SMEM)
    vmem = pl.BlockSpec(memory_space=pltpu.VMEM)
    shapes = [jax.ShapeDtypeStruct(s, d) for s, d in outs]
    size = sum(a.size * a.dtype.itemsize for a in args)
    got = pl.pallas_call(
        functools.partial(fn, **static),
        out_shape=shapes,
        in_specs=[smem] * scalars + [vmem] * (len(args) - scalars),
        out_specs=[vmem] * len(outs),
        compiler_params=pltpu.CompilerParams(vmem_limit_bytes=limit),
        cost_estimate=pl.CostEstimate(flops=flops, bytes_accessed=size, transcendentals=0),
    )(*args)
    return got if isinstance(out, list) else got[0]


def dot(x, w):
    return jnp.dot(x, w, preferred_element_type=f32)


def dot_t(x, w):
    return lax.dot_general(x, w, (((1,), (1,)), ((), ())), preferred_element_type=f32)


def exact(x, y, contract=((1,), (0,))):
    return lax.dot_general(
        x, y, (contract, ((), ())), precision=HIGHEST, preferred_element_type=f32
    )


def flat(x):
    x = x.astype(f32)
    return x.reshape(-1, x.shape[-1])


def blocked(x, count):
    return x.reshape(count, -1, x.shape[-1])


def lane_tile(rows, columns):
    lane = lax.broadcasted_iota(jnp.int32, (rows, LANES), 1)
    tile = jnp.zeros((rows, LANES), f32)
    for i, column in enumerate(columns):
        high = column.astype(bf16).astype(f32)
        tile = jnp.where(lane == i, high, tile)
        tile = jnp.where(lane == i + len(columns), column - high, tile)
    return tile


def column_of(sums, start, i, count):
    at = start + i
    return sums[:, at : at + 1] + sums[:, at + count : at + count + 1]


def silu(x):
    return x * jax.nn.sigmoid(x)


def softplus(x):
    return jnp.maximum(x, 0.0) + jnp.log1p(jnp.exp(-jnp.abs(x)))


def spread(tokens, gain, out):
    raw = tokens[...].astype(f32)
    both = jnp.concatenate([raw, raw * gain[...]], 1)
    both = both.reshape(out.shape[0], 1, out.shape[2], out.shape[3])
    out[...] = jnp.broadcast_to(both, out.shape).astype(bf16)


def pack_first(gate, up, out):
    n = gate.shape[1]
    out[:, :n] = gate[...]
    out[:, n:] = up[...]


def lay(parts, out):
    rows, at = out.shape[0], 0
    for part in parts:
        for i in range(0, part.shape[0], rows):
            out[:, at : at + part.shape[1]] = part[i : i + rows]
            at += part.shape[1]
    return at


def pack(down, query, key, value, outer, mixer_out, gains, out):
    at = lay((down, query, key, value, outer, mixer_out), out)
    row = lax.broadcasted_iota(jnp.int32, (out.shape[0], LANES), 0)
    tile = jnp.zeros(row.shape, f32)
    for which in range(2):
        rest = gains[which : which + 1]
        for i in range(3):
            part = rest.astype(bf16).astype(f32)
            tile = jnp.where(row == 3 * which + i, part, tile)
            rest = rest - part
    out[:, at:] = tile.astype(bf16)


def pack_second(gate, up, down, out):
    lay((gate, up, down), out)


def packed_gain(packed, which):
    tile = packed[0:16, packed.shape[1] - LANES :].astype(f32)
    at = 3 * which
    return tile[at : at + 1] + tile[at + 1 : at + 2] + tile[at + 2 : at + 3]


def order(ids):
    core, side = ids[0], ids[2]
    return [(chip, half) for chip in (side, 1 - side) for half in (core, 1 - core)]


def gate_up(scaled, weights, square, out):
    n = (out.shape[2] - LANES) // 2
    count = out.shape[0]
    for i in range(2):
        part = sum(dot(x, w[:, i * n : (i + 1) * n]) for x, w in zip(scaled, weights))
        out[:, :, i * n : (i + 1) * n] = blocked(part, count).astype(bf16)
    out[:, :, 2 * n :] = blocked(lane_tile(square.shape[0], [square]), count).astype(bf16)


def row_sum(xs):
    return jnp.sum(sum(x * x for x in xs), -1, keepdims=True)


def first_products(ids, got, weights, weights_x, out):
    core = ids[0]
    wide = [flat(got[core]), flat(got[1 - core])]
    raw = [x[:, :LANES] for x in wide]
    scaled = [x[:, LANES:].astype(bf16) for x in wide]
    gate_up(scaled, (weights, weights_x), row_sum(raw), out)


def slices(ids, wide):
    out = []
    for chip in (ids[2], 1 - ids[2]):
        rows = flat(wide(chip))
        half = rows.shape[1] // 2
        out += [rows[:, :half], rows[:, half:]]
    return out


def second_products(ids, second, *refs):
    out, packs, weights = refs[-1], refs[:4], refs[4:8]
    raw = slices(ids, lambda chip: second[:, chip])
    scaled = [(x * packed_gain(p, 1)).astype(bf16) for x, p in zip(raw, packs)]
    gate_up(scaled, weights, row_sum(raw), out)


def activate(parts, out, *, features):
    sums = jnp.sum(parts[...].astype(f32), axis=0)
    n = (sums.shape[1] - LANES) // 2
    factor = lax.rsqrt(column_of(sums, 2 * n, 0, 1) / features + EPS)
    hidden = silu(sums[:, :n] * factor) * (sums[:, n : 2 * n] * factor)
    out[...] = jnp.broadcast_to(hidden[None], out.shape).astype(bf16)


def down_product(rows, packed, at):
    n = rows.shape[1]
    return sum(
        dot(rows[:, j : j + LANES], packed[:, at + j : at + j + LANES])
        for j in range(0, n, LANES)
    )


def first_down(ids, hidden, *refs):
    out = refs[-1]
    rows = flat(hidden[...]).astype(bf16)
    for i, ((chip, _), packed) in enumerate(zip(order(ids), refs[:-1])):
        at = i % 2 * LANES
        part = down_product(rows, packed, 0)
        out[:, chip, :, at : at + LANES] = blocked(part, out.shape[0]).astype(bf16)


def last_down(ids, hidden, second, *refs):
    out = refs[-1]
    side = ids[2]
    rows = flat(hidden[...]).astype(bf16)
    n = rows.shape[1]
    for i, ((chip, half), packed) in enumerate(zip(order(ids), refs[:-1])):
        part = down_product(rows, packed, 2 * n)
        out[chip, half, :, side, :, :LANES] = blocked(part, out.shape[2]).astype(bf16)
        at = i % 2 * LANES
        out[chip, half, :, side, :, LANES:] = second[:, chip, :, at : at + LANES]
        out[chip, half, :, 1 - side] = jnp.zeros((out.shape[2], *out.shape[4:]), bf16)


def mixer_down(ids, mixed, *refs):
    out = refs[-1]
    rows = flat(mixed[...]).astype(bf16)
    for i, ((chip, _), packed) in enumerate(zip(order(ids), refs[:-1])):
        weight = packed[:, packed.shape[1] - 2 * LANES : packed.shape[1] - LANES]
        at = i % 2 * LANES
        out[:, chip, :, at : at + LANES] = blocked(dot(rows, weight), out.shape[0]).astype(bf16)


def add_first(ids, parts, got, got_z, out):
    sums = jnp.sum(parts[...].astype(f32), axis=0)
    core, side, chip = ids[0], ids[2], ids[3]
    block = 2 * ids[4] + side
    halves = []
    for c in (core, 1 - core):
        mine, theirs = got[c, block].astype(f32), got_z[c, block].astype(f32)
        halves.append(jnp.where(chip == side, mine, theirs)[:, :LANES])
    rows = jnp.concatenate(halves, 1) + 0.5 * sums
    out[...] = jnp.broadcast_to(rows[None], out.shape).astype(bf16)


def add_mixer(ids, parts, middle, out):
    sums = jnp.sum(parts[...].astype(f32), axis=0)
    rows = middle[ids[4], ids[3]].astype(f32) + sums
    out[...] = jnp.broadcast_to(rows[None], out.shape).astype(bf16)


def project(ids, middle, logits, *refs):
    out, packs = refs[-1], refs[:-1]
    n, count = out.shape[2] - LANES, out.shape[0]
    raw = slices(ids, lambda chip: middle[:, chip])
    scaled = [(x * packed_gain(p, 0)).astype(bf16) for x, p in zip(raw, packs)]
    at = packs[0].shape[1] - 2 * LANES - n
    part = sum(dot(x, p[:, at : at + n]) for x, p in zip(scaled, packs))
    out[:, :, :n] = blocked(part, count).astype(bf16)
    heads = logits.shape[2]
    mine = lax.broadcasted_iota(jnp.int32, (part.shape[0], heads), 1) == ids[1]
    columns = []
    for i in range(2):
        logit = sum(
            dot_t(x, logits[i, chip * 2 + half]) for x, (chip, half) in zip(scaled, order(ids))
        )
        columns.append(jnp.sum(jnp.where(mine, logit, 0.0), -1, keepdims=True))
    columns.append(row_sum(raw))
    out[:, :, n:] = blocked(lane_tile(part.shape[0], columns), count).astype(bf16)


def earlier_state(
    lengths, head, recurrent, keys, values, strength, decay, extra, gain, state, new, gains
):
    count, span = strength.shape
    sequence = lax.broadcasted_iota(jnp.int32, (count, span), 0)
    lane = lax.broadcasted_iota(jnp.int32, (count, span), 1)
    latest = jnp.zeros((count, span), jnp.int32)
    for b in range(count):
        latest = jnp.where(sequence == b, lengths[b] - 1, latest)
    before = lane < latest
    beta = jnp.where(before, jax.nn.sigmoid(strength[...]), 0.0)
    amount = extra[...] - head[0] * softplus(decay[...] + head[1])
    amount = jnp.where(before, amount, 0.0)
    new_extra = jnp.sum(jnp.where(lane == latest, extra[...], 0.0), -1, keepdims=True)
    new[...] = jnp.broadcast_to(new_extra, new.shape)
    gains[...] = jnp.broadcast_to(gain[...], gains.shape)
    row = lax.broadcasted_iota(jnp.int32, (span, span), 0)
    col = lax.broadcasted_iota(jnp.int32, (span, span), 1)
    cumul = exact(amount, (row <= col).astype(f32))
    last = cumul[:, span - 1 : span]
    eye = (row == col).astype(f32)
    stacked = jnp.concatenate(
        [beta, cumul, jnp.exp(cumul), jnp.exp(last - cumul), before.astype(f32)], 0
    )
    upright = exact(eye, stacked, ((1,), (1,)))

    def upright_column(which, b):
        at = which * count + b
        return upright[:, at : at + 1]

    every = range(count)
    ks, couplings = [], []
    for b in every:
        k = keys[b].astype(f32) * upright_column(4, b)
        k = k * lax.rsqrt(jnp.sum(k * k, -1, keepdims=True) + EPS)
        gap = upright_column(1, b) - cumul[b : b + 1]
        gap = jnp.exp(jnp.where(row > col, gap, -jnp.inf))
        ks.append(k)
        couplings.append(upright_column(0, b) * exact(k, k, ((1,), (1,))) * gap)

    def same(size):
        return (row // size) == (col // size)

    first = [jnp.where(same(8), c, 0.0) for c in couplings]
    second = [exact(a, a) for a in first]
    fourth = [exact(a, a) for a in second]
    inverse = [exact(eye - a, eye + b) for a, b in zip(first, second)]
    inverse = [exact(a, eye + b) for a, b in zip(inverse, fourth)]
    size = 8
    while size < span:
        inside = same(2 * size) & ~same(size)
        right = [exact(jnp.where(inside, c, 0.0), a) for c, a in zip(couplings, inverse)]
        inverse = [a - exact(a, r) for a, r in zip(inverse, right)]
        size *= 2
    for b in every:
        carried = exact(ks[b], recurrent[b])
        value = values[b].astype(f32) * upright_column(4, b)
        side = upright_column(0, b) * (value - upright_column(2, b) * carried)
        update = exact(inverse[b], side) * upright_column(3, b)
        kept = jnp.exp(last[b : b + 1]) * recurrent[b]
        state[b] = kept + exact(ks[b], update, ((0,), (0,)))


def new_token(head, parts, state, new_extra, norm_gain, out, *, features):
    sums = jnp.sum(parts[...].astype(f32), axis=0)
    dk = (sums.shape[1] - LANES) // 4
    strength, decay, square = (column_of(sums, 4 * dk, i, 3) for i in range(3))
    factor = lax.rsqrt(square / features + EPS)
    query, key, value, gate = (sums[:, i * dk : (i + 1) * dk] * factor for i in range(4))
    beta = jax.nn.sigmoid(strength * factor)
    amount = new_extra[:, 0:1] - head[0] * softplus(decay * factor + head[1])
    query = query * lax.rsqrt(jnp.sum(query * query, -1, keepdims=True) + EPS) * dk**-0.5
    key = key * lax.rsqrt(jnp.sum(key * key, -1, keepdims=True) + EPS)
    score = jnp.sum(query * key, -1, keepdims=True)
    reduced = jnp.transpose(query - (score * beta) * key)
    sequence = lax.broadcasted_iota(jnp.int32, value.shape, 0)
    read = jnp.zeros(value.shape, f32)
    for b in range(value.shape[0]):
        one = jnp.sum(reduced[:, b : b + 1] * state[b], axis=0, keepdims=True)
        read = jnp.where(sequence == b, one, read)
    rows = jnp.exp(amount) * read + (score * beta) * value
    rows = rows * lax.rsqrt(jnp.mean(rows * rows, -1, keepdims=True) + EPS)
    rows = rows * norm_gain[...] * silu(gate)
    out[...] = jnp.broadcast_to(rows[None], out.shape).astype(bf16)


def finish(ids, parts, out):
    side = ids[3]
    sums = jnp.sum(parts[side].astype(f32), axis=1)
    half = out.shape[1]
    rows = []
    for c in range(2):
        rows.append(parts[side, c, 0].astype(f32)[:, half:] + 0.5 * sums[c][:, :half])
    out[...] = jnp.concatenate(rows, 0).astype(bf16)


def exchange(x, axis):
    return lax.all_to_all(x, axis, 0, 0, tiled=True)


def swap(x):
    return lax.ppermute(x, "c", [(0, 1), (1, 0)])


def swap_chips(x):
    return lax.ppermute(x, "za", [(0, 1), (1, 0)])


def together(*trees):
    return lax.optimization_barrier(trees)


def layer(
    tokens,
    first_norm_gain,
    first_gate_weight,
    first_up_weight,
    first_down_weight,
    mixer_norm_gain,
    query_weight_matrix,
    key_weight_matrix,
    value_weight_matrix,
    output_gate_weight,
    strength_weight,
    decay_weight,
    head_decay_speed,
    head_decay_offset,
    head_norm_gain,
    mixer_out_weight,
    second_norm_gain,
    second_gate_weight,
    second_up_weight,
    second_down_weight,
    recurrent,
    earlier_key_cache,
    earlier_value_cache,
    strength_logit_history,
    decay_input_history,
    position_decay_extra,
    lengths,
):
    core, tp, side = lax.axis_index("c"), lax.axis_index("tp"), lax.axis_index("za")
    plane, ring = lax.axis_size("tp"), lax.axis_size(Z)
    count, width = tokens.shape
    rows, half = count // 2, ring // 2
    features = 2 * ring * width
    hidden_units = first_gate_weight.shape[1]
    dk = query_weight_matrix.shape[1]
    ids = jnp.stack([core, tp, side, tp & 1, tp >> 1]).astype(jnp.int32)

    sent = kernel(
        spread, ((2, plane, rows, 2 * width), bf16), tokens, first_norm_gain[None]
    )
    got = exchange(sent.reshape(2 * plane, rows, 2 * width), ("c", "tp"))
    got = got.reshape(2, plane, rows, 2 * width)
    first = kernel(
        pack_first, ((width, 2 * hidden_units), bf16), first_gate_weight, first_up_weight
    )
    first_x = swap(first)
    sent = kernel(
        first_products,
        ((ring, rows, 2 * hidden_units + LANES), bf16),
        ids,
        got,
        first,
        first_x,
        scalars=1,
    )

    sent, later = together(
        sent,
        (
            first_down_weight,
            (second_gate_weight, second_up_weight, second_down_weight),
            (query_weight_matrix, key_weight_matrix, value_weight_matrix, output_gate_weight),
            (mixer_out_weight, mixer_norm_gain, second_norm_gain),
            (strength_weight, decay_weight),
            (head_decay_speed, head_decay_offset),
            (recurrent, earlier_key_cache, earlier_value_cache),
            (strength_logit_history, decay_input_history, position_decay_extra),
            (lengths, head_norm_gain),
        ),
    )
    down, branch, heads, outer, logits, decays, caches, histories, others = later
    parts = exchange(sent, Z)
    gains = jnp.stack(outer[1:])
    head = jnp.concatenate(decays)
    lengths, head_norm_gain = others
    local = lengths.shape[0]
    state, new_extra, norm_gain = kernel(
        earlier_state,
        [
            ((local, dk, recurrent.shape[-1]), f32),
            ((local, LANES), f32),
            ((local, recurrent.shape[-1]), f32),
        ],
        lengths,
        head,
        caches[0][:, 0],
        *caches[1:],
        *(h[0] for h in histories),
        head_norm_gain[None],
        scalars=2,
        flops=1 << 28,
    )
    packed = kernel(
        pack,
        ((width, hidden_units + 4 * dk + width + LANES), bf16),
        down,
        *heads,
        outer[0],
        gains,
    )
    state, packed = together(state, packed)
    packed_z = swap_chips(packed)
    got_z = swap_chips(got)
    start = lax.axis_index("zh") * 4 * width
    logits = [lax.dynamic_slice_in_dim(w.T, start, 4 * width, 1) for w in logits]
    logits = jnp.stack(logits).reshape(2, -1, 4, width).transpose(0, 2, 1, 3)
    parts, logits, state, new_extra, norm_gain, packed, branch = together(
        parts, logits, state, new_extra, norm_gain, packed, branch
    )

    hidden = kernel(activate, ((half, rows, hidden_units), bf16), parts, features=features)
    hidden, packed, branch = together(hidden, packed, branch)
    hidden = exchange(hidden, "zh")
    later = kernel(pack_second, ((width, 3 * hidden_units), bf16), *branch)
    packed_x = swap(packed)
    packed_zx = swap(packed_z)
    later_x = swap(later)
    hidden, packed_x, packed_z, packed_zx, got_z, later, later_x = together(
        hidden, packed_x, packed_z, packed_zx, got_z, later, later_x
    )
    packs = (packed, packed_x, packed_z, packed_zx)

    parts = kernel(
        first_down, ((plane // 2, 2, rows, 2 * width), bf16), ids, hidden, *packs, scalars=1
    )
    parts, later = together(parts, later)
    parts = exchange(parts.reshape(plane, rows, 2 * width), "tp")
    later_z = swap_chips(later)
    middle = kernel(add_first, ((plane, rows, 2 * width), bf16), ids, parts, got, got_z, scalars=1)
    middle = exchange(middle, "tp").reshape(plane // 2, 2, rows, 2 * width)

    parts = kernel(
        project,
        ((half, rows, 4 * dk + LANES), bf16),
        ids,
        middle,
        logits,
        *packs,
        scalars=1,
    )
    parts = exchange(parts, "zh")
    mixed = kernel(
        new_token,
        ((half, rows, dk), bf16),
        head,
        parts,
        state,
        new_extra,
        norm_gain,
        scalars=1,
        features=features,
    )
    mixed = exchange(mixed, "zh")
    parts = kernel(
        mixer_down, ((plane // 2, 2, rows, 2 * width), bf16), ids, mixed, *packs, scalars=1
    )
    parts, later_z = together(parts, later_z)
    parts = exchange(parts.reshape(plane, rows, 2 * width), "tp")
    later_zx = swap(later_z)
    parts, later_zx = together(parts, later_zx)
    laters = (later, later_x, later_z, later_zx)
    second = kernel(add_mixer, ((plane, rows, 2 * width), bf16), ids, parts, middle, scalars=1)
    second = exchange(second, "tp").reshape(plane // 2, 2, rows, 2 * width)

    sent = kernel(
        second_products,
        ((half, rows, 2 * hidden_units + LANES), bf16),
        ids,
        second,
        *packs,
        *laters,
        scalars=1,
    )
    parts = exchange(sent, "zh")
    hidden = kernel(activate, ((half, rows, hidden_units), bf16), parts, features=features)
    hidden = exchange(hidden, "zh")
    parts = kernel(
        last_down,
        ((2, 2, plane // 2, 2, rows, 2 * width), bf16),
        ids,
        hidden,
        second,
        *laters,
        scalars=1,
    )
    parts = exchange(parts.reshape(4 * plane, rows, 2 * width), ("za", "c", "tp"))
    parts = parts.reshape(2, 2, plane, rows, 2 * width)
    return kernel(finish, ((count, width), bf16), ids, parts, scalars=1)


def solution(mesh):
    kv, tp = mesh.shape["kv"], mesh.shape["tp"]
    split = Mesh(mesh.devices.reshape(kv // 4, 2, 2, tp), (*Z, "c", "tp"))
    kv = (*Z, "c")
    return jax.shard_map(
        layer,
        mesh=split,
        in_specs=(
            P("tp", kv),
            P(kv),
            P(kv, "tp"),
            P(kv, "tp"),
            P("tp", kv),
            P(kv),
            P(kv, "tp"),
            P(kv, "tp"),
            P(kv, "tp"),
            P(kv, "tp"),
            P(),
            P(),
            P("tp"),
            P("tp"),
            P(),
            P("tp", kv),
            P(kv),
            P(kv, "tp"),
            P(kv, "tp"),
            P("tp", kv),
            P(kv, "tp", None, None),
            P(kv, None, "tp"),
            P(kv, None, "tp"),
            P("tp", kv, None),
            P("tp", kv, None),
            P("tp", kv, None),
            P(kv),
        ),
        out_specs=P("tp", kv),
        check_vma=False,
    )
```

```python
import functools

import jax
import jax.numpy as jnp
from jax import lax
from jax.experimental import pallas as pl
from jax.experimental.pallas import tpu as pltpu
from jax.sharding import Mesh, PartitionSpec as P

HIGHEST = lax.Precision.HIGHEST
f32 = jnp.float32
bf16 = jnp.bfloat16
LANES = 128
Z = ("zh", "za")
EPS = 1e-06


def kernel(fn, out, *args, scalars=0, flops=1 << 20, limit=12 << 20, **static):
    outs = out if isinstance(out, list) else [out]
    smem = pl.BlockSpec(memory_space=pltpu.SMEM)
    vmem = pl.BlockSpec(memory_space=pltpu.VMEM)
    shapes = [jax.ShapeDtypeStruct(s, d) for s, d in outs]
    size = sum(a.size * a.dtype.itemsize for a in args)
    got = pl.pallas_call(
        functools.partial(fn, **static),
        out_shape=shapes,
        in_specs=[smem] * scalars + [vmem] * (len(args) - scalars),
        out_specs=[vmem] * len(outs),
        compiler_params=pltpu.CompilerParams(vmem_limit_bytes=limit),
        cost_estimate=pl.CostEstimate(flops=flops, bytes_accessed=size, transcendentals=0),
    )(*args)
    return got if isinstance(out, list) else got[0]


def dot(x, w):
    return jnp.dot(x, w, preferred_element_type=f32)


def dot_t(x, w):
    return lax.dot_general(x, w, (((1,), (1,)), ((), ())), preferred_element_type=f32)


def exact(x, y, contract=((1,), (0,))):
    return lax.dot_general(
        x, y, (contract, ((), ())), precision=HIGHEST, preferred_element_type=f32
    )


def flat(x):
    x = x.astype(f32)
    return x.reshape(-1, x.shape[-1])


def blocked(x, count):
    return x.reshape(count, -1, x.shape[-1])


def lane_tile(rows, columns):
    lane = lax.broadcasted_iota(jnp.int32, (rows, LANES), 1)
    tile = jnp.zeros((rows, LANES), f32)
    for i, column in enumerate(columns):
        high = column.astype(bf16).astype(f32)
        tile = jnp.where(lane == i, high, tile)
        tile = jnp.where(lane == i + len(columns), column - high, tile)
    return tile


def column_of(sums, start, i, count):
    at = start + i
    return sums[:, at : at + 1] + sums[:, at + count : at + count + 1]


def silu(x):
    return x * jax.nn.sigmoid(x)


def softplus(x):
    return jnp.maximum(x, 0.0) + jnp.log1p(jnp.exp(-jnp.abs(x)))


def spread(tokens, gain, out):
    raw = tokens[...].astype(f32)
    both = jnp.concatenate([raw, raw * gain[...]], 1)
    both = both.reshape(out.shape[0], 1, out.shape[2], out.shape[3])
    out[...] = jnp.broadcast_to(both, out.shape).astype(bf16)


def pack_first(gate, up, out):
    n = gate.shape[1]
    out[:, :n] = gate[...]
    out[:, n:] = up[...]


def lay(parts, out):
    rows, at = out.shape[0], 0
    for part in parts:
        for i in range(0, part.shape[0], rows):
            out[:, at : at + part.shape[1]] = part[i : i + rows]
            at += part.shape[1]
    return at


def pack(down, query, key, value, outer, mixer_out, gains, out):
    at = lay((down, query, key, value, outer, mixer_out), out)
    row = lax.broadcasted_iota(jnp.int32, (out.shape[0], LANES), 0)
    tile = jnp.zeros(row.shape, f32)
    for which in range(2):
        rest = gains[which : which + 1]
        for i in range(3):
            part = rest.astype(bf16).astype(f32)
            tile = jnp.where(row == 3 * which + i, part, tile)
            rest = rest - part
    out[:, at:] = tile.astype(bf16)


def pack_second(gate, up, down, out):
    lay((gate, up, down), out)


def packed_gain(packed, which):
    tile = packed[0:16, packed.shape[1] - LANES :].astype(f32)
    at = 3 * which
    return tile[at : at + 1] + tile[at + 1 : at + 2] + tile[at + 2 : at + 3]


def order(ids):
    core, side = ids[0], ids[2]
    return [(chip, half) for chip in (side, 1 - side) for half in (core, 1 - core)]


def gate_up(scaled, weights, square, out):
    n = (out.shape[2] - LANES) // 2
    count = out.shape[0]
    for i in range(2):
        part = sum(dot(x, w[:, i * n : (i + 1) * n]) for x, w in zip(scaled, weights))
        out[:, :, i * n : (i + 1) * n] = blocked(part, count).astype(bf16)
    out[:, :, 2 * n :] = blocked(lane_tile(square.shape[0], [square]), count).astype(bf16)


def row_sum(xs):
    return jnp.sum(sum(x * x for x in xs), -1, keepdims=True)


def first_products(ids, got, weights, weights_x, out):
    core = ids[0]
    wide = [flat(got[core]), flat(got[1 - core])]
    raw = [x[:, :LANES] for x in wide]
    scaled = [x[:, LANES:].astype(bf16) for x in wide]
    gate_up(scaled, (weights, weights_x), row_sum(raw), out)


def slices(ids, wide):
    out = []
    for chip in (ids[2], 1 - ids[2]):
        rows = flat(wide(chip))
        half = rows.shape[1] // 2
        out += [rows[:, :half], rows[:, half:]]
    return out


def second_products(ids, second, *refs):
    out, packs, weights = refs[-1], refs[:4], refs[4:8]
    raw = slices(ids, lambda chip: second[:, chip])
    scaled = [(x * packed_gain(p, 1)).astype(bf16) for x, p in zip(raw, packs)]
    gate_up(scaled, weights, row_sum(raw), out)


def activate(parts, out, *, features):
    sums = jnp.sum(parts[...].astype(f32), axis=0)
    n = (sums.shape[1] - LANES) // 2
    factor = lax.rsqrt(column_of(sums, 2 * n, 0, 1) / features + EPS)
    hidden = silu(sums[:, :n] * factor) * (sums[:, n : 2 * n] * factor)
    out[...] = jnp.broadcast_to(hidden[None], out.shape).astype(bf16)


def down_product(rows, packed, at):
    n = rows.shape[1]
    return sum(
        dot(rows[:, j : j + LANES], packed[:, at + j : at + j + LANES])
        for j in range(0, n, LANES)
    )


def first_down(ids, hidden, *refs):
    out = refs[-1]
    rows = flat(hidden[...]).astype(bf16)
    for i, ((chip, _), packed) in enumerate(zip(order(ids), refs[:-1])):
        at = i % 2 * LANES
        part = down_product(rows, packed, 0)
        out[:, chip, :, at : at + LANES] = blocked(part, out.shape[0]).astype(bf16)


def last_down(ids, hidden, second, *refs):
    out = refs[-1]
    side = ids[2]
    rows = flat(hidden[...]).astype(bf16)
    n = rows.shape[1]
    for i, ((chip, half), packed) in enumerate(zip(order(ids), refs[:-1])):
        part = down_product(rows, packed, 2 * n)
        out[chip, half, :, side, :, :LANES] = blocked(part, out.shape[2]).astype(bf16)
        at = i % 2 * LANES
        out[chip, half, :, side, :, LANES:] = second[:, chip, :, at : at + LANES]
        out[chip, half, :, 1 - side] = jnp.zeros((out.shape[2], *out.shape[4:]), bf16)


def mixer_down(ids, mixed, *refs):
    out = refs[-1]
    rows = flat(mixed[...]).astype(bf16)
    for i, ((chip, _), packed) in enumerate(zip(order(ids), refs[:-1])):
        weight = packed[:, packed.shape[1] - 2 * LANES : packed.shape[1] - LANES]
        at = i % 2 * LANES
        out[:, chip, :, at : at + LANES] = blocked(dot(rows, weight), out.shape[0]).astype(bf16)


def add_first(ids, parts, got, got_z, out):
    sums = jnp.sum(parts[...].astype(f32), axis=0)
    core, side, chip = ids[0], ids[2], ids[3]
    block = 2 * ids[4] + side
    halves = []
    for c in (core, 1 - core):
        mine, theirs = got[c, block].astype(f32), got_z[c, block].astype(f32)
        halves.append(jnp.where(chip == side, mine, theirs)[:, :LANES])
    rows = jnp.concatenate(halves, 1) + 0.5 * sums
    out[...] = jnp.broadcast_to(rows[None], out.shape).astype(bf16)


def add_mixer(ids, parts, middle, out):
    sums = jnp.sum(parts[...].astype(f32), axis=0)
    rows = middle[ids[4], ids[3]].astype(f32) + sums
    out[...] = jnp.broadcast_to(rows[None], out.shape).astype(bf16)


def project(ids, middle, logits, *refs):
    out, packs = refs[-1], refs[:-1]
    n, count = out.shape[2] - LANES, out.shape[0]
    raw = slices(ids, lambda chip: middle[:, chip])
    scaled = [(x * packed_gain(p, 0)).astype(bf16) for x, p in zip(raw, packs)]
    at = packs[0].shape[1] - 2 * LANES - n
    part = sum(dot(x, p[:, at : at + n]) for x, p in zip(scaled, packs))
    out[:, :, :n] = blocked(part, count).astype(bf16)
    heads = logits.shape[2]
    mine = lax.broadcasted_iota(jnp.int32, (part.shape[0], heads), 1) == ids[1]
    columns = []
    for i in range(2):
        logit = sum(
            dot_t(x, logits[i, chip * 2 + half]) for x, (chip, half) in zip(scaled, order(ids))
        )
        columns.append(jnp.sum(jnp.where(mine, logit, 0.0), -1, keepdims=True))
    columns.append(row_sum(raw))
    out[:, :, n:] = blocked(lane_tile(part.shape[0], columns), count).astype(bf16)


def earlier_state(
    lengths, head, recurrent, keys, values, strength, decay, extra, gain, state, new, gains
):
    count, span = strength.shape
    sequence = lax.broadcasted_iota(jnp.int32, (count, span), 0)
    lane = lax.broadcasted_iota(jnp.int32, (count, span), 1)
    latest = jnp.zeros((count, span), jnp.int32)
    for b in range(count):
        latest = jnp.where(sequence == b, lengths[b] - 1, latest)
    before = lane < latest
    beta = jnp.where(before, jax.nn.sigmoid(strength[...]), 0.0)
    amount = extra[...] - head[0] * softplus(decay[...] + head[1])
    amount = jnp.where(before, amount, 0.0)
    new_extra = jnp.sum(jnp.where(lane == latest, extra[...], 0.0), -1, keepdims=True)
    new[...] = jnp.broadcast_to(new_extra, new.shape)
    gains[...] = jnp.broadcast_to(gain[...], gains.shape)
    row = lax.broadcasted_iota(jnp.int32, (span, span), 0)
    col = lax.broadcasted_iota(jnp.int32, (span, span), 1)
    cumul = exact(amount, (row <= col).astype(f32))
    last = cumul[:, span - 1 : span]
    eye = (row == col).astype(f32)
    stacked = jnp.concatenate(
        [beta, cumul, jnp.exp(cumul), jnp.exp(last - cumul), before.astype(f32)], 0
    )
    upright = exact(eye, stacked, ((1,), (1,)))

    def upright_column(which, b):
        at = which * count + b
        return upright[:, at : at + 1]

    every = range(count)
    ks, couplings = [], []
    for b in every:
        k = keys[b].astype(f32) * upright_column(4, b)
        k = k * lax.rsqrt(jnp.sum(k * k, -1, keepdims=True) + EPS)
        gap = upright_column(1, b) - cumul[b : b + 1]
        gap = jnp.exp(jnp.where(row > col, gap, -jnp.inf))
        ks.append(k)
        couplings.append(upright_column(0, b) * exact(k, k, ((1,), (1,))) * gap)

    def same(size):
        return (row // size) == (col // size)

    first = [jnp.where(same(8), c, 0.0) for c in couplings]
    second = [exact(a, a) for a in first]
    fourth = [exact(a, a) for a in second]
    inverse = [exact(eye - a, eye + b) for a, b in zip(first, second)]
    inverse = [exact(a, eye + b) for a, b in zip(inverse, fourth)]
    size = 8
    while size < span:
        inside = same(2 * size) & ~same(size)
        right = [exact(jnp.where(inside, c, 0.0), a) for c, a in zip(couplings, inverse)]
        inverse = [a - exact(a, r) for a, r in zip(inverse, right)]
        size *= 2
    for b in every:
        carried = exact(ks[b], recurrent[b])
        value = values[b].astype(f32) * upright_column(4, b)
        side = upright_column(0, b) * (value - upright_column(2, b) * carried)
        update = exact(inverse[b], side) * upright_column(3, b)
        kept = jnp.exp(last[b : b + 1]) * recurrent[b]
        state[b] = kept + exact(ks[b], update, ((0,), (0,)))


def new_token(head, parts, state, new_extra, norm_gain, out, *, features):
    sums = jnp.sum(parts[...].astype(f32), axis=0)
    dk = (sums.shape[1] - LANES) // 4
    strength, decay, square = (column_of(sums, 4 * dk, i, 3) for i in range(3))
    factor = lax.rsqrt(square / features + EPS)
    query, key, value, gate = (sums[:, i * dk : (i + 1) * dk] * factor for i in range(4))
    beta = jax.nn.sigmoid(strength * factor)
    amount = new_extra[:, 0:1] - head[0] * softplus(decay * factor + head[1])
    query = query * lax.rsqrt(jnp.sum(query * query, -1, keepdims=True) + EPS) * dk**-0.5
    key = key * lax.rsqrt(jnp.sum(key * key, -1, keepdims=True) + EPS)
    score = jnp.sum(query * key, -1, keepdims=True)
    reduced = jnp.transpose(query - (score * beta) * key)
    sequence = lax.broadcasted_iota(jnp.int32, value.shape, 0)
    read = jnp.zeros(value.shape, f32)
    for b in range(value.shape[0]):
        one = jnp.sum(reduced[:, b : b + 1] * state[b], axis=0, keepdims=True)
        read = jnp.where(sequence == b, one, read)
    rows = jnp.exp(amount) * read + (score * beta) * value
    rows = rows * lax.rsqrt(jnp.mean(rows * rows, -1, keepdims=True) + EPS)
    rows = rows * norm_gain[...] * silu(gate)
    out[...] = jnp.broadcast_to(rows[None], out.shape).astype(bf16)


def finish(ids, parts, out):
    side = ids[3]
    sums = jnp.sum(parts[side].astype(f32), axis=1)
    half = out.shape[1]
    rows = []
    for c in range(2):
        rows.append(parts[side, c, 0].astype(f32)[:, half:] + 0.5 * sums[c][:, :half])
    out[...] = jnp.concatenate(rows, 0).astype(bf16)


def exchange(x, axis):
    return lax.all_to_all(x, axis, 0, 0, tiled=True)


def swap(x):
    return lax.ppermute(x, "c", [(0, 1), (1, 0)])


def swap_chips(x):
    return lax.ppermute(x, "za", [(0, 1), (1, 0)])


def together(*trees):
    return lax.optimization_barrier(trees)


def layer(
    tokens,
    first_norm_gain,
    first_gate_weight,
    first_up_weight,
    first_down_weight,
    mixer_norm_gain,
    query_weight_matrix,
    key_weight_matrix,
    value_weight_matrix,
    output_gate_weight,
    strength_weight,
    decay_weight,
    head_decay_speed,
    head_decay_offset,
    head_norm_gain,
    mixer_out_weight,
    second_norm_gain,
    second_gate_weight,
    second_up_weight,
    second_down_weight,
    recurrent,
    earlier_key_cache,
    earlier_value_cache,
    strength_logit_history,
    decay_input_history,
    position_decay_extra,
    lengths,
):
    core, tp, side = lax.axis_index("c"), lax.axis_index("tp"), lax.axis_index("za")
    plane, ring = lax.axis_size("tp"), lax.axis_size(Z)
    count, width = tokens.shape
    rows, half = count // 2, ring // 2
    features = 2 * ring * width
    hidden_units = first_gate_weight.shape[1]
    dk = query_weight_matrix.shape[1]
    ids = jnp.stack([core, tp, side, tp & 1, tp >> 1]).astype(jnp.int32)

    sent = kernel(
        spread, ((2, plane, rows, 2 * width), bf16), tokens, first_norm_gain[None]
    )
    got = exchange(sent.reshape(2 * plane, rows, 2 * width), ("c", "tp"))
    got = got.reshape(2, plane, rows, 2 * width)
    first = kernel(
        pack_first, ((width, 2 * hidden_units), bf16), first_gate_weight, first_up_weight
    )
    first_x = swap(first)
    packed = kernel(
        pack,
        ((width, hidden_units + 4 * dk + width + LANES), bf16),
        first_down_weight,
        query_weight_matrix,
        key_weight_matrix,
        value_weight_matrix,
        output_gate_weight,
        mixer_out_weight,
        jnp.stack([mixer_norm_gain, second_norm_gain]),
    )
    packed_z = swap_chips(packed)
    sent = kernel(
        first_products,
        ((ring, rows, 2 * hidden_units + LANES), bf16),
        ids,
        got,
        first,
        first_x,
        scalars=1,
    )

    sent, later = together(
        sent,
        (
            (second_gate_weight, second_up_weight, second_down_weight),
            (strength_weight, decay_weight),
            (head_decay_speed, head_decay_offset),
            (recurrent, earlier_key_cache, earlier_value_cache),
            (strength_logit_history, decay_input_history, position_decay_extra),
            (lengths, head_norm_gain),
        ),
    )
    branch, logits, decays, caches, histories, others = later
    parts = exchange(sent, Z)
    head = jnp.concatenate(decays)
    lengths, head_norm_gain = others
    local = lengths.shape[0]
    state, new_extra, norm_gain = kernel(
        earlier_state,
        [
            ((local, dk, recurrent.shape[-1]), f32),
            ((local, LANES), f32),
            ((local, recurrent.shape[-1]), f32),
        ],
        lengths,
        head,
        caches[0][:, 0],
        *caches[1:],
        *(h[0] for h in histories),
        head_norm_gain[None],
        scalars=2,
        flops=1 << 28,
    )
    got_z = swap_chips(got)
    start = lax.axis_index("zh") * 4 * width
    logits = [lax.dynamic_slice_in_dim(w.T, start, 4 * width, 1) for w in logits]
    logits = jnp.stack(logits).reshape(2, -1, 4, width).transpose(0, 2, 1, 3)
    parts, logits, state, new_extra, norm_gain, packed, branch = together(
        parts, logits, state, new_extra, norm_gain, packed, branch
    )

    hidden = kernel(activate, ((half, rows, hidden_units), bf16), parts, features=features)
    hidden, packed, branch = together(hidden, packed, branch)
    hidden = exchange(hidden, "zh")
    later = kernel(pack_second, ((width, 3 * hidden_units), bf16), *branch)
    packed_x = swap(packed)
    packed_zx = swap(packed_z)
    later_x = swap(later)
    hidden, packed_x, packed_z, packed_zx, got_z, later, later_x = together(
        hidden, packed_x, packed_z, packed_zx, got_z, later, later_x
    )
    packs = (packed, packed_x, packed_z, packed_zx)

    parts = kernel(
        first_down, ((plane // 2, 2, rows, 2 * width), bf16), ids, hidden, *packs, scalars=1
    )
    parts, later = together(parts, later)
    parts = exchange(parts.reshape(plane, rows, 2 * width), "tp")
    later_z = swap_chips(later)
    middle = kernel(add_first, ((plane, rows, 2 * width), bf16), ids, parts, got, got_z, scalars=1)
    middle = exchange(middle, "tp").reshape(plane // 2, 2, rows, 2 * width)

    parts = kernel(
        project,
        ((half, rows, 4 * dk + LANES), bf16),
        ids,
        middle,
        logits,
        *packs,
        scalars=1,
    )
    parts = exchange(parts, "zh")
    mixed = kernel(
        new_token,
        ((half, rows, dk), bf16),
        head,
        parts,
        state,
        new_extra,
        norm_gain,
        scalars=1,
        features=features,
    )
    mixed = exchange(mixed, "zh")
    parts = kernel(
        mixer_down, ((plane // 2, 2, rows, 2 * width), bf16), ids, mixed, *packs, scalars=1
    )
    parts, later_z = together(parts, later_z)
    parts = exchange(parts.reshape(plane, rows, 2 * width), "tp")
    later_zx = swap(later_z)
    parts, later_zx = together(parts, later_zx)
    laters = (later, later_x, later_z, later_zx)
    second = kernel(add_mixer, ((plane, rows, 2 * width), bf16), ids, parts, middle, scalars=1)
    second = exchange(second, "tp").reshape(plane // 2, 2, rows, 2 * width)

    sent = kernel(
        second_products,
        ((half, rows, 2 * hidden_units + LANES), bf16),
        ids,
        second,
        *packs,
        *laters,
        scalars=1,
    )
    parts = exchange(sent, "zh")
    hidden = kernel(activate, ((half, rows, hidden_units), bf16), parts, features=features)
    hidden = exchange(hidden, "zh")
    parts = kernel(
        last_down,
        ((2, 2, plane // 2, 2, rows, 2 * width), bf16),
        ids,
        hidden,
        second,
        *laters,
        scalars=1,
    )
    parts = exchange(parts.reshape(4 * plane, rows, 2 * width), ("za", "c", "tp"))
    parts = parts.reshape(2, 2, plane, rows, 2 * width)
    return kernel(finish, ((count, width), bf16), ids, parts, scalars=1)


def solution(mesh):
    kv, tp = mesh.shape["kv"], mesh.shape["tp"]
    split = Mesh(mesh.devices.reshape(kv // 4, 2, 2, tp), (*Z, "c", "tp"))
    kv = (*Z, "c")
    return jax.shard_map(
        layer,
        mesh=split,
        in_specs=(
            P("tp", kv),
            P(kv),
            P(kv, "tp"),
            P(kv, "tp"),
            P("tp", kv),
            P(kv),
            P(kv, "tp"),
            P(kv, "tp"),
            P(kv, "tp"),
            P(kv, "tp"),
            P(),
            P(),
            P("tp"),
            P("tp"),
            P(),
            P("tp", kv),
            P(kv),
            P(kv, "tp"),
            P(kv, "tp"),
            P("tp", kv),
            P(kv, "tp", None, None),
            P(kv, None, "tp"),
            P(kv, None, "tp"),
            P("tp", kv, None),
            P("tp", kv, None),
            P("tp", kv, None),
            P(kv),
        ),
        out_specs=P("tp", kv),
        check_vma=False,
    )
```
